32 devices in a mesh: sp: 8 (over z, core), tp: 4 (over y, x).
Axes of the slice: x: 2, y: 2, z: 4, core: 2. Of those that a mesh axis runs over, the one named last changes fastest.
Arguments:
- queries: bfloat16 [2048, 2048], P('sp', 'tp'), may hold values from -6 to 6
- keys: bfloat16 [2048, 1024], P('sp', 'tp'), may hold values from -6 to 6
- values: bfloat16 [2048, 1024], P('sp', 'tp'), may hold values from -6 to 6
- sink_logit: float32 [32], P('tp'), may hold values from -1 to 6
- out_weight: bfloat16 [2048, 2048], P(None, 'tp'), may hold values from -0.125 to 0.125
- residual: bfloat16 [2048, 2048], P(('sp', 'tp')), may hold values from -1.796875 to 1.796875
- norm_gain: float32 [2048], replicated, may hold values from 0.1 to 1.9
- routes: int32 [2048, 2], P(('sp', 'tp')), may hold values from 0 to 7, all different within a row; in each aligned block of 64 rows (0 to 63, 64 to 127, ...) at most 32 rows name the same one
- route_weights: float32 [2048, 2], P(('sp', 'tp')), may hold values from 0.2 to 1
- gate_weight: bfloat16 [8, 2048, 5120], P('sp', None, 'tp'), may hold values from -0.125 to 0.125
- up_weight: bfloat16 [8, 2048, 5120], P('sp', None, 'tp'), may hold values from -0.125 to 0.125
- down_weight: bfloat16 [8, 5120, 2048], P('sp', 'tp'), may hold values from -0.078125 to 0.078125
Outputs:
- mixed: bfloat16 [2048, 2048], P(('sp', 'tp'))
The draws below stay inside these ranges and needn't reach their ends.
Inputs may be any that keep to these rules, and one draw needn't show every extreme that they name: `routes`: each row names two different experts. Among the rows of one device no expert is named more than 32 times, and in every draw some expert is named exactly 32 times by the rows of some device.
All inputs are finite; a program needn't handle non-finite values.
Results may differ from the reference program's by a relative error of at most 0.018.
Values may be sent and summed in bfloat16 or wider, within the bound.
A program may use at most 64 MiB of HBM per device.

```python
import math
import jax
import jax.numpy as jnp
import numpy as np
from jax import lax

D = 2048
FF = 5120
HEADS = 32
KV_HEADS = 16
HEAD = 64
WINDOW = 128
TOK_DEV = 64
TOKENS = 2048
EXPERTS = 8
CAP = 32
N_SP = 8
N_TP = 4


def draw_queries(key, part):
    own_key = jax.random.fold_in(key, 17)
    drawn = jnp.clip(jax.random.normal(own_key, (TOKENS, HEADS * HEAD), jnp.float32), -6.0, 6.0)
    return drawn.astype(jnp.bfloat16)


def draw_keys(key, part):
    own_key = jax.random.fold_in(key, 29)
    drawn = jnp.clip(jax.random.normal(own_key, (TOKENS, KV_HEADS * HEAD), jnp.float32), -6.0, 6.0)
    return drawn.astype(jnp.bfloat16)


def shard_levels(stream_key, dims, cuts, smallest, top_value):
    level = 1.0
    for position, shards_of in cuts:
        steps = jax.random.uniform(jax.random.fold_in(jax.random.fold_in(stream_key, 6), position), (shards_of,), jnp.float32, smallest / len(cuts), top_value / len(cuts))
        level = level * jnp.repeat(jnp.exp(steps), dims[position] // shards_of).reshape((-1,) + (1,) * (len(dims) - 1 - position))
    return level


def deal_out(rng, own, number, rows, amount, top, limit, lean):
    order = jax.random.permutation(rng, amount)
    packed, ordinary = portions_of(amount, rows * top, limit, lean, True), portions_of(amount, rows * top, limit, lean, False)
    places = jnp.arange(amount)

    def named(tallies, rotation):
        used = int((tallies > 0).sum())
        fixed = max(1, used // 4)
        moved = fixed + (places - fixed + rotation * (used - fixed)) % max(1, amount - fixed)
        return jnp.zeros((amount,), jnp.int32).at[order[jnp.where(places < fixed, places, moved)]].set(jnp.asarray(tallies, jnp.int32))

    tallies = jnp.where(number % 4 == 0, named(packed, number // 4), named(ordinary, number - number // 4 - 1))
    mixed = jax.random.permutation(jax.random.fold_in(own, 3), amount)
    donor, taker = mixed[0:amount // 2 * 2:2], mixed[1:amount // 2 * 2:2]
    slack = jnp.minimum(tallies[donor] - 1, limit - tallies[taker]) // 2
    slack = jnp.where((donor == order[0]) | (taker == order[0]) | (tallies[taker] == 0), 0, jnp.maximum(slack, 0))
    moved = jax.random.randint(jax.random.fold_in(own, 4), (amount // 2,), 0, 1 << 20) % (slack + 1)
    tallies = tallies.at[donor].add(-moved).at[taker].add(moved)
    members = jnp.searchsorted(jnp.cumsum(tallies), jnp.arange(rows * top), side="right").astype(jnp.int32)
    listing = members.reshape(top, rows).T
    listing = listing[jax.random.permutation(jax.random.fold_in(own, 1), rows)]
    rotation = jax.random.randint(jax.random.fold_in(own, 2), (rows, 1), 0, top)
    return jnp.take_along_axis(listing, (jnp.arange(top)[None, :] + rotation) % top, axis=1)


def portions_of(amount, total, most, lean, full):
    loads = [(1 << 20) // math.isqrt(rank ** lean) + 1 for rank in range(1, amount + 1)]
    largest = most if full else min(most, max(-(-total // amount), total * loads[0] // sum(loads)))
    least = 1 if total - largest >= amount - 1 else 0
    counts, surplus = [largest] + [least] * (amount - 1), total - largest - least * (amount - 1)
    while surplus > 0:
        movable = [i for i in range(1, amount) if counts[i] < largest] or [i for i in range(1, amount) if counts[i] < most]
        pool, remaining = sum([loads[i] for i in movable]), surplus
        for i in movable:
            more = min(most - counts[i], max(1, remaining * loads[i] // pool), surplus)
            counts[i] = counts[i] + more
            surplus = surplus - more
    return np.array(counts)


def scatter_about(stream_key, extent, width, bound, shards=(), held_as=jnp.bfloat16):
    array = width * jax.random.normal(stream_key, extent, jnp.float32)
    if shards:
        array = array * shard_levels(stream_key, extent, shards, -0.22, 0.18)
    return jnp.clip(array, -bound, bound).astype(held_as)


def setup_inputs(seed: int = 0) -> dict:
    key_of = jax.random.split(jax.random.key(seed), 13)
    queries = draw_queries(jax.random.fold_in(key_of[12], 71), 0)
    keys = draw_keys(jax.random.fold_in(key_of[12], 71), 0)
    values = scatter_about(key_of[2], (TOKENS, KV_HEADS * HEAD), 1.0, 6.0, ((0, 8), (1, 4)))
    sink_logit = jnp.clip(-1.0 + 7.0 * jax.random.uniform(key_of[3], (HEADS,), jnp.float32) ** shard_levels(key_of[3], (HEADS,), ((0, 4),), -0.2, 0.2), -1.0, 6.0)
    out_weight = scatter_about(key_of[4], (HEADS * HEAD, D), (HEADS * HEAD) ** -0.5, 0.125, ((1, 4),))
    residual = scatter_about(key_of[5], (TOKENS, D), 0.3, 1.796875, ((0, 32),))
    norm_gain = jnp.clip(1.0 + 0.18 * jax.random.normal(key_of[6], (D,), jnp.float32), 0.1, 1.9)
    routes_keys = jax.random.split(jax.random.fold_in(key_of[7], 1), TOKENS // TOK_DEV)
    routes_turns = jax.random.permutation(jax.random.fold_in(key_of[7], 3), TOKENS // TOK_DEV)
    routes = jax.vmap(lambda own, number: deal_out(jax.random.fold_in(key_of[7], 2), own, number, TOK_DEV, EXPERTS, 2, CAP, 1))(routes_keys, routes_turns).reshape((TOKENS, 2))
    route_weights = jnp.clip(0.2 + 0.8 * jax.random.uniform(key_of[8], (TOKENS, 2), jnp.float32) ** shard_levels(key_of[8], (TOKENS, 2), ((0, 32),), -0.2, 0.2), 0.2, 1.0)
    gate_weight = scatter_about(key_of[9], (EXPERTS, D, FF), D ** -0.5, 0.125, ((0, 8), (2, 4)))
    up_weight = scatter_about(key_of[10], (EXPERTS, D, FF), D ** -0.5, 0.125, ((0, 8), (2, 4)))
    down_weight = scatter_about(key_of[11], (EXPERTS, FF, D), FF ** -0.5, 0.078125, ((0, 8), (1, 4)))
    return {"queries": queries, "keys": keys, "values": values, "sink_logit": sink_logit, "out_weight": out_weight, "residual": residual, "norm_gain": norm_gain, "routes": routes, "route_weights": route_weights, "gate_weight": gate_weight, "up_weight": up_weight, "down_weight": down_weight}


EPS = 1e-06
NEGATIVE = -1e+30

def make_band(tensor):
    length = tensor.shape[0]
    blocks = length // WINDOW
    padded = jnp.pad(tensor, ((WINDOW, WINDOW), (0, 0)))
    pieces = [padded[offset * WINDOW:offset * WINDOW + length].reshape(blocks, WINDOW, -1) for offset in range(3)]
    return jnp.concatenate(pieces, axis=1)

def attend(queries, keys, values, sink_logit):
    tokens = queries.shape[0]
    blocks = tokens // WINDOW
    repeat = HEADS // KV_HEADS
    scale = HEAD ** (-0.5)
    near = jnp.abs(jnp.arange(WINDOW)[:, None] + WINDOW - jnp.arange(3 * WINDOW)[None, :]) <= WINDOW
    key_pos = (jnp.arange(blocks)[:, None] - 1) * WINDOW + jnp.arange(3 * WINDOW)[None, :]
    inside = (key_pos >= 0) & (key_pos < tokens)
    valid = near[None, None, :, :] & inside[:, None, None, :]
    query_groups = queries.reshape(tokens, KV_HEADS, repeat, HEAD).transpose(1, 0, 2, 3)
    key_groups = keys.reshape(tokens, KV_HEADS, HEAD).transpose(1, 0, 2)
    value_groups = values.reshape(tokens, KV_HEADS, HEAD).transpose(1, 0, 2)
    sink_groups = sink_logit.reshape(KV_HEADS, repeat)

    def one_group(inputs):
        query_rows, key_rows, value_rows, sinks = inputs
        query_blocks = query_rows.reshape(blocks, WINDOW, repeat, HEAD).astype(jnp.float32)
        key_band = make_band(key_rows).astype(jnp.float32)
        value_band = make_band(value_rows).astype(jnp.float32)
        scores = jnp.einsum('nqrd,nkd->nrqk', query_blocks, key_band) * scale
        sink = sinks.astype(jnp.float32)[None, :, None, None]
        masked = jnp.where(valid, scores, NEGATIVE)
        top = jnp.maximum(lax.optimization_barrier(jnp.max(masked, axis=-1, keepdims=True)), sink)
        probs = jnp.exp(masked - top)
        denom = lax.optimization_barrier(jnp.sum(probs, axis=-1, keepdims=True)) + jnp.exp(sink - top)
        weights = (probs / denom).astype(jnp.bfloat16)
        output = jnp.einsum('nrqk,nkd->nqrd', weights.astype(jnp.float32), value_band)
        return output.astype(jnp.bfloat16).reshape(tokens, repeat * HEAD)
    outputs = lax.map(one_group, (query_groups, key_groups, value_groups, sink_groups))
    return outputs.transpose(1, 0, 2).reshape(tokens, HEADS * HEAD)

def one_expert(inputs):
    rows, gate_matrix, up_matrix, down_matrix = inputs
    gate = jnp.dot(rows, gate_matrix, preferred_element_type=jnp.float32)
    upward = jnp.dot(rows, up_matrix, preferred_element_type=jnp.float32)
    hidden = (jax.nn.silu(gate) * upward).astype(jnp.bfloat16)
    block_width = FF // N_TP
    shares = jnp.einsum('rjf,jfd->jrd', hidden.reshape(-1, N_TP, block_width).astype(jnp.float32), down_matrix.reshape(N_TP, block_width, D).astype(jnp.float32))
    return lax.optimization_barrier(jnp.sum(shares.astype(jnp.bfloat16).astype(jnp.float32), axis=0)).astype(jnp.bfloat16)

def reference(queries, keys, values, sink_logit, out_weight, residual, norm_gain, routes, route_weights, gate_weight, up_weight, down_weight):
    attention = attend(queries, keys, values, sink_logit)
    projected = jnp.dot(attention, out_weight, preferred_element_type=jnp.float32).astype(jnp.bfloat16)
    hidden_state = residual.astype(jnp.float32) + projected.astype(jnp.float32)
    inverse = lax.rsqrt(lax.optimization_barrier(jnp.mean(hidden_state * hidden_state, axis=-1, keepdims=True)) + EPS)
    normed = (hidden_state * inverse * norm_gain).astype(jnp.bfloat16)
    devices = N_SP * N_TP
    expert_ids = routes.reshape(devices, 2 * TOK_DEV).astype(jnp.int32)
    onehot = (expert_ids[..., None] == jnp.arange(EXPERTS, dtype=jnp.int32)).astype(jnp.int32)
    earlier = jnp.cumsum(onehot, axis=1) - onehot
    rank = lax.optimization_barrier(jnp.sum(earlier * onehot, axis=-1))
    slots = (jnp.arange(devices, dtype=jnp.int32)[:, None] * CAP + rank).reshape(-1).astype(jnp.int32)
    flat_ids = expert_ids.reshape(-1)
    pair_rows = jnp.repeat(normed, 2, axis=0)
    buffer = jnp.zeros((EXPERTS, devices * CAP, D), jnp.bfloat16).at[flat_ids, slots].set(pair_rows)
    expert_out = lax.map(one_expert, (buffer, gate_weight, up_weight, down_weight))
    picked = expert_out[flat_ids, slots].reshape(TOKENS, 2, D).astype(jnp.float32)
    mixture = lax.optimization_barrier(jnp.sum(route_weights[..., None] * picked, axis=1))
    return (hidden_state + mixture).astype(jnp.bfloat16)
```

```python
import functools

import jax
import jax.numpy as jnp
from jax import lax
from jax.experimental import pallas as pl
from jax.experimental.pallas import tpu as pltpu
from jax.sharding import PartitionSpec as P

HEADS = 32
KV_HEADS = 16
HEAD = 64
WINDOW = 128


EPS = 1e-06
NEGATIVE = -1e30
MESH = pl.DeviceIdType.MESH


def plane():
    t = lax.axis_index("tp")
    tx = t + 1 - 2 * lax.rem(t, 2)
    ty = lax.rem(t + 2, 4)
    return t, tx, ty, 3 - t


def greet(devices):
    barrier = pltpu.get_barrier_semaphore()
    for device in devices:
        pl.semaphore_signal(barrier, inc=1, device_id=device, device_id_type=MESH)
    pl.semaphore_wait(barrier, len(devices))


def remote(src, dst, send, recv, device):
    return pltpu.make_async_remote_copy(
        src_ref=src,
        dst_ref=dst,
        send_sem=send,
        recv_sem=recv,
        device_id=device,
        device_id_type=MESH,
    )


def flipped(index, mask):
    result = index
    bit = 1
    while bit <= mask:
        if mask & bit:
            result = result + bit * (1 - 2 * lax.rem(index // bit, 2))
        bit *= 2
    return result


def expert_kernel(
    send_ref, gate_hbm, up_hbm, down_hbm, out_ref,
    gate, up, down, piece, hidden, part, bx1, by1, bx2, by2, acc, fin, load,
    zs, zr, xs, xr, ys, yr, xhs, xhr, yhs, yhr,
    x1s, x1r, y1s, y1r, x2s, x2r, y2s, y2r, zls, zlr, zhs, zhr,
):
    n, capacity, width = send_ref.shape
    s = lax.axis_index("sp")
    t, tx, ty, td = plane()
    half = capacity // 2
    low, high = pl.ds(0, half), pl.ds(half, half)
    x_dev, y_dev = (s, tx), (s, ty)
    loads = [
        pltpu.make_async_copy(source, target, load.at[k])
        for k, (source, target) in enumerate(((gate_hbm, gate), (up_hbm, up), (down_hbm, down)))
    ]
    for copy in loads:
        copy.start()
    greet([(flipped(s, m), t) for m in range(1, n)] + [x_dev, y_dev])
    copies = []

    def go(*args):
        copy = remote(*args)
        copy.start()
        copies.append(copy)
        return copy

    def total(a, b):
        return (a.astype(jnp.float32) + b.astype(jnp.float32)).astype(jnp.bfloat16)

    gray = [k ^ (k >> 1) for k in range(n // 2)]
    z_copies, full, halves, first, second, back = {}, {}, {}, {}, {}, []

    def members(q):
        return (2 * q, 2 * q + 1)

    def stage_a(q):
        for m in members(q):
            source = flipped(s, m)
            if m:
                z_copies[m].wait_recv()
            src = piece.at[t, source] if m else send_ref.at[source]
            full[m] = (
                go(src, piece.at[t, source], xs.at[m], xr.at[m], x_dev),
                go(src, piece.at[t, source], ys.at[m], yr.at[m], y_dev),
            )

    def stage_b(q):
        for m in members(q):
            source = flipped(s, m)
            full[m][0].wait_recv()
            block = piece.at[tx, source, low]
            to_y = go(block, block, yhs.at[m], yhr.at[m], y_dev)
            full[m][1].wait_recv()
            block = piece.at[ty, source, high]
            halves[m] = (to_y, go(block, block, xhs.at[m], xhr.at[m], x_dev))

    def compute(q):
        for m in members(q):
            for copy in halves[m]:
                copy.wait_recv()
        base = flipped(s // 2, q) * 2
        rows = 8 * capacity
        step = 256

        @pl.loop(0, gate.shape[1] // step)
        def _(k):
            columns = pl.ds(pl.multiple_of(k * step, step), step)
            x = piece[:, pl.ds(base, 2)].reshape(rows, width)
            g = jnp.dot(x, gate[:, columns], preferred_element_type=jnp.float32)
            u = jnp.dot(x, up[:, columns], preferred_element_type=jnp.float32)
            hidden[:, columns] = (jax.nn.silu(g) * u).astype(hidden.dtype)

        wide = 512

        @pl.loop(0, width // wide)
        def _(k):
            columns = pl.ds(pl.multiple_of(k * wide, wide), wide)
            share = jnp.dot(hidden[...], down[:, columns], preferred_element_type=jnp.float32)
            part[:, pl.ds(base, 2), :, columns] = share.astype(part.dtype).reshape(
                4, 2, capacity, wide
            )

    def begin(q):
        for m in members(q):
            owner = flipped(s, m)
            first[m] = (
                go(part.at[td, owner, low], bx1.at[m, 1], x1s.at[m, 1], x1r.at[m, 1], x_dev),
                go(part.at[td, owner, high], by1.at[m, 1], y1s.at[m, 1], y1r.at[m, 1], y_dev),
                go(part.at[tx, owner, low], bx1.at[m, 0], x1s.at[m, 0], x1r.at[m, 0], x_dev),
                go(part.at[ty, owner, high], by1.at[m, 0], y1s.at[m, 0], y1r.at[m, 0], y_dev),
            )

    def middle(q):
        for m in members(q):
            owner = flipped(s, m)
            first[m][0].wait_recv()
            acc[m, 0] = total(part[ty, owner, low], bx1[m, 1])
            to_y = go(acc.at[m, 0], by2.at[m], y2s.at[m], y2r.at[m], y_dev)
            first[m][1].wait_recv()
            acc[m, 1] = total(part[tx, owner, high], by1[m, 1])
            second[m] = (to_y, go(acc.at[m, 1], bx2.at[m], x2s.at[m], x2r.at[m], x_dev))

    def last(q):
        for m in members(q):
            owner = flipped(s, m)
            first[m][2].wait_recv()
            second[m][0].wait_recv()
            lower = total(
                part[t, owner, low].astype(jnp.float32) + bx1[m, 0].astype(jnp.float32), by2[m]
            )
            first[m][3].wait_recv()
            second[m][1].wait_recv()
            upper = total(
                part[t, owner, high].astype(jnp.float32) + by1[m, 0].astype(jnp.float32), bx2[m]
            )
            if m:
                away = (owner, t)
                fin[m, low] = lower
                back.append(go(fin.at[m, low], out_ref.at[s, low], zls.at[m], zlr.at[m], away))
                fin[m, high] = upper
                back.append(go(fin.at[m, high], out_ref.at[s, high], zhs.at[m], zhr.at[m], away))
            else:
                out_ref[s, low] = lower
                out_ref[s, high] = upper

    for q in gray:
        for m in members(q):
            if m:
                target = flipped(s, m)
                z_copies[m] = go(
                    send_ref.at[target], piece.at[t, s], zs.at[m], zr.at[m], (target, t)
                )
    stage_a(0)
    piece[t, s] = send_ref[s]
    order = gray[1:] + [0]
    count = len(gray)
    for k in range(count + 4):
        if k + 1 < count:
            stage_a(gray[k + 1])
        if k < count:
            stage_b(gray[k])
        if k == 2:
            for copy in loads:
                copy.wait()
        if 0 <= k - 2 < count:
            compute(order[k - 2])
            begin(order[k - 2])
        if 0 <= k - 3 < count:
            middle(order[k - 3])
        if 0 <= k - 4 < count:
            last(order[k - 4])
    for copy in back:
        copy.wait_recv()
    for copy in copies:
        copy.wait_send()


def experts(sending, gate_weight, up_weight, down_weight):
    n, capacity, width = sending.shape
    half = capacity // 2
    kind = sending.dtype
    one = pltpu.SemaphoreType.DMA((n,))
    two = pltpu.SemaphoreType.DMA((n, 2))
    anywhere = pl.BlockSpec(memory_space=pl.ANY)
    return pl.pallas_call(
        expert_kernel,
        out_shape=jax.ShapeDtypeStruct((n, capacity, width), kind),
        in_specs=[pl.BlockSpec(memory_space=pltpu.VMEM), anywhere, anywhere, anywhere],
        out_specs=pl.BlockSpec(memory_space=pltpu.VMEM),
        scratch_shapes=[
            pltpu.VMEM(gate_weight.shape, kind),
            pltpu.VMEM(up_weight.shape, kind),
            pltpu.VMEM(down_weight.shape, kind),
            pltpu.VMEM((4, n, capacity, width), kind),
            pltpu.VMEM((8 * capacity, gate_weight.shape[1]), kind),
            pltpu.VMEM((4, n, capacity, width), kind),
            pltpu.VMEM((n, 2, half, width), kind),
            pltpu.VMEM((n, 2, half, width), kind),
            pltpu.VMEM((n, half, width), kind),
            pltpu.VMEM((n, half, width), kind),
            pltpu.VMEM((n, 2, half, width), kind),
            pltpu.VMEM((n, capacity, width), kind),
            pltpu.SemaphoreType.DMA((3,)),
        ]
        + [one] * 10
        + [two] * 4
        + [one] * 8,
        compiler_params=pltpu.CompilerParams(
            collective_id=0, has_side_effects=True, vmem_limit_bytes=56 * 1024 * 1024
        ),
    )(sending, gate_weight, up_weight, down_weight)


def attend_kernel(
    q_hbm, k_hbm, v_hbm, sink_ref, w_hbm, res_hbm, gain_ref, hidden_ref, normed_ref,
    q, kv, w, res, buf, acc, cols, got,
    load, hs, hr, gs, gr, as_, ar,
):
    s = lax.axis_index("sp")
    t, tx, ty, td = plane()
    last = lax.axis_size("sp") - 1
    rows, depth = q.shape
    half = rows // 2
    groups = k_hbm.shape[1] // HEAD
    kept = groups * HEAD
    odd = lax.rem(s, 2)
    near = s + 1 - 2 * odd
    has_far = jnp.logical_and(s != 0, s != last)
    far = jnp.where(has_far, s - 1 + 2 * odd, near)
    x_dev, y_dev, d_dev, n_dev, f_dev = (s, tx), (s, ty), (s, td), (near, t), (far, t)
    middle = pl.ds(half, rows)
    loads = [
        pltpu.make_async_copy(source, target, load.at[k])
        for k, (source, target) in enumerate(
            (
                (k_hbm, kv.at[middle, pl.ds(0, kept)]),
                (v_hbm, kv.at[middle, pl.ds(kept, kept)]),
                (q_hbm, q),
                (w_hbm, w),
                (res_hbm, res),
            )
        )
    ]
    for copy in loads:
        copy.start()
    barrier = pltpu.get_barrier_semaphore()
    for device in (x_dev, y_dev, d_dev, n_dev):
        pl.semaphore_signal(barrier, inc=1, device_id=device, device_id_type=MESH)

    @pl.when(has_far)
    def _():
        pl.semaphore_signal(barrier, inc=1, device_id=f_dev, device_id_type=MESH)
        pl.semaphore_wait(barrier, 5)

    @pl.when(jnp.logical_not(has_far))
    def _():
        pl.semaphore_wait(barrier, 4)

    def aligned(value, size):
        return pl.ds(pl.multiple_of(value, size), size)

    near_src = aligned(2 * half - half * odd, half)
    near_dst = aligned(3 * half * odd, half)
    far_src = aligned(half + half * odd, half)
    far_dst = aligned(3 * half * (1 - odd), half)
    near_copy = remote(kv.at[near_src], kv.at[near_dst], hs.at[0], hr.at[0], n_dev)
    far_copy = remote(kv.at[far_src], kv.at[far_dst], hs.at[1], hr.at[1], f_dev)
    loads[0].wait()
    loads[1].wait()

    @pl.when(has_far)
    def _():
        far_copy.start()

    near_copy.start()

    @pl.when(jnp.logical_not(has_far))
    def _():
        kv[aligned(3 * half * odd, half)] = jnp.zeros((half, kv.shape[1]), kv.dtype)

    loads[2].wait()
    span = 3 * half
    query = lax.broadcasted_iota(jnp.int32, (2 * half, span), 0)
    query = jnp.where(query >= half, query - half, query)
    key = lax.broadcasted_iota(jnp.int32, (2 * half, span), 1)
    band = jnp.abs(query + half - key) <= WINDOW
    upper = lax.broadcasted_iota(jnp.int32, (2 * half, 1), 0) < half

    def attend(b):
        valid = jnp.logical_and(
            band,
            jnp.logical_and(
                key >= jnp.where(2 * s + b == 0, half, 0),
                key < jnp.where(2 * s + b == 2 * last + 1, 2 * half, span),
            ),
        )
        keys_at = pl.ds(pl.multiple_of(b * half, half), span)
        mine = aligned(b * half, half)
        for g in range(groups):
            pair = q[mine, 2 * g * HEAD : 2 * (g + 1) * HEAD]
            stacked = jnp.concatenate([pair[:, :HEAD], pair[:, HEAD:]], axis=0)
            scores = lax.dot_general(
                stacked,
                kv[keys_at, g * HEAD : (g + 1) * HEAD],
                (((1,), (1,)), ((), ())),
                preferred_element_type=jnp.float32,
            ) * HEAD ** (-0.5)
            sink = jnp.where(upper, sink_ref[2 * g], sink_ref[2 * g + 1])
            masked = jnp.where(valid, scores, NEGATIVE)
            top = jnp.maximum(jnp.max(masked, axis=-1, keepdims=True), sink)
            probs = jnp.exp(masked - top)
            denom = jnp.sum(probs, axis=-1, keepdims=True) + jnp.exp(sink - top)
            weights = (probs * (1.0 / denom)).astype(jnp.bfloat16)
            output = jnp.dot(
                weights,
                kv[keys_at, kept + g * HEAD : kept + (g + 1) * HEAD],
                preferred_element_type=jnp.float32,
            )
            joined = jnp.concatenate([output[:half], output[half:]], axis=1)
            buf[t, mine, 2 * g * HEAD : 2 * (g + 1) * HEAD] = joined.astype(buf.dtype)

    first_block, second_block = 1 - odd, odd
    copies = []

    def go(*args):
        copy = remote(*args)
        copy.start()
        copies.append(copy)
        return copy

    def spread(b, k):
        piece = buf.at[t, aligned(b * half, half)]
        return (
            go(piece, piece, gs.at[k], gr.at[k], x_dev),
            go(piece, piece, gs.at[k + 1], gr.at[k + 1], y_dev),
        )

    near_copy.wait_recv()
    attend(first_block)
    x_one, y_one = spread(first_block, 0)

    @pl.when(has_far)
    def _():
        far_copy.wait_recv()

    attend(second_block)
    x_two, y_two = spread(second_block, 2)
    loads[3].wait()

    def product(b, owner):
        weight = w[pl.ds(pl.multiple_of(owner * depth, depth), depth)]
        piece = buf[owner, aligned(b * half, half)]
        return jnp.dot(piece, weight, preferred_element_type=jnp.float32)

    x_one.wait_recv()
    piece = buf.at[tx, aligned(first_block * half, half)]
    d_one = go(piece, piece, gs.at[4], gr.at[4], y_dev)
    acc[0] = product(first_block, t)
    acc[0] += product(first_block, tx)
    y_one.wait_recv()
    acc[0] += product(first_block, ty)
    y_two.wait_recv()
    piece = buf.at[ty, aligned(second_block * half, half)]
    d_two = go(piece, piece, gs.at[5], gr.at[5], x_dev)
    acc[1] = product(second_block, t)
    acc[1] += product(second_block, ty)
    own = rows // 4
    to_x = remote(
        cols.at[aligned(tx * own, own)], got.at[t], as_.at[0], ar.at[0], x_dev
    )
    to_y = remote(
        cols.at[aligned(ty * own, own)], got.at[t], as_.at[1], ar.at[1], y_dev
    )
    to_d = remote(
        cols.at[aligned(td * own, own)], got.at[t], as_.at[2], ar.at[2], d_dev
    )
    home = t // 2

    def finish(b, k):
        total = acc[k] + product(b, td)
        cols[aligned(b * half, half)] = total.astype(cols.dtype)

        @pl.when(home == b)
        def _():
            to_x.start()

        @pl.when(home != b)
        def _():
            to_d.start()
            to_y.start()

    d_one.wait_recv()
    finish(first_block, 0)
    x_two.wait_recv()
    acc[1] += product(second_block, tx)
    d_two.wait_recv()
    finish(second_block, 1)
    got[t] = cols[aligned(t * own, own)]
    loads[4].wait()
    to_x.wait_recv()
    to_y.wait_recv()
    to_d.wait_recv()
    squares = jnp.zeros((own, 1), jnp.float32)
    width = w.shape[1]
    for k in range(4):
        columns = slice(k * width, (k + 1) * width)
        state = res[:, columns].astype(jnp.float32) + got[k].astype(jnp.float32)
        hidden_ref[:, columns] = state
        squares += jnp.sum(state * state, axis=-1, keepdims=True)
    inverse = lax.rsqrt(squares * (1.0 / (4 * width)) + EPS)
    for k in range(4):
        columns = slice(k * width, (k + 1) * width)
        normed_ref[:, columns] = (
            hidden_ref[:, columns] * inverse * gain_ref[:, columns]
        ).astype(normed_ref.dtype)
    for copy in copies:
        copy.wait_send()
    near_copy.wait_send()
    to_x.wait_send()
    to_y.wait_send()
    to_d.wait_send()

    @pl.when(has_far)
    def _():
        far_copy.wait_send()


def attend_project(queries, keys, values, sink_logit, out_weight, residual, norm_gain):
    rows, depth = queries.shape
    kind = queries.dtype
    width = out_weight.shape[1]
    anywhere = pl.BlockSpec(memory_space=pl.ANY)
    vmem = pl.BlockSpec(memory_space=pltpu.VMEM)
    dma = pltpu.SemaphoreType.DMA
    return pl.pallas_call(
        attend_kernel,
        out_shape=(
            jax.ShapeDtypeStruct(residual.shape, jnp.float32),
            jax.ShapeDtypeStruct(residual.shape, kind),
        ),
        in_specs=[anywhere] * 3
        + [pl.BlockSpec(memory_space=pltpu.SMEM), anywhere, anywhere, vmem],
        out_specs=(vmem, vmem),
        scratch_shapes=[
            pltpu.VMEM(queries.shape, kind),
            pltpu.VMEM((2 * rows, 2 * keys.shape[1]), kind),
            pltpu.VMEM(out_weight.shape, kind),
            pltpu.VMEM(residual.shape, kind),
            pltpu.VMEM((4, rows, depth), kind),
            pltpu.VMEM((2, rows // 2, width), jnp.float32),
            pltpu.VMEM((rows, width), kind),
            pltpu.VMEM((4, rows // 4, width), kind),
            dma((5,)),
            dma((2,)),
            dma((2,)),
            dma((6,)),
            dma((6,)),
            dma((3,)),
            dma((3,)),
        ],
        compiler_params=pltpu.CompilerParams(collective_id=2, has_side_effects=True),
    )(queries, keys, values, sink_logit, out_weight, residual, norm_gain.reshape(1, -1))


def with_halo(block, sides, width):
    for axis, dim in sides:
        count = lax.axis_size(axis)
        forward = [(i, i + 1) for i in range(count - 1)]
        backward = [(target, source) for source, target in forward]
        low = lax.ppermute(
            lax.slice_in_dim(block, block.shape[dim] - width, None, axis=dim), axis, forward
        )
        high = lax.ppermute(lax.slice_in_dim(block, 0, width, axis=dim), axis, backward)
        block = jnp.concatenate([low, block, high], axis=dim)
    return block


def make_band(extended, length):
    blocks = length // WINDOW
    pieces = [
        lax.slice_in_dim(extended, offset * WINDOW, offset * WINDOW + length, axis=0).reshape(
            blocks, WINDOW, -1
        )
        for offset in range(3)
    ]
    return jnp.concatenate(pieces, axis=1)


def attend_local(queries, keys, values, sink_logit):
    length = queries.shape[0]
    groups = keys.shape[1] // HEAD
    repeat = HEADS // KV_HEADS
    blocks = length // WINDOW
    joined = jnp.concatenate([keys, values], axis=1)
    extended = with_halo(joined, (("sp", 0),), WINDOW)
    banded = make_band(extended, length)
    key_band = banded[..., : groups * HEAD].reshape(blocks, 3 * WINDOW, groups, HEAD)
    value_band = banded[..., groups * HEAD :].reshape(blocks, 3 * WINDOW, groups, HEAD)
    query_blocks = queries.reshape(blocks, WINDOW, groups, repeat, HEAD)
    scores = jnp.einsum(
        "nqgrd,nkgd->ngrqk", query_blocks, key_band, preferred_element_type=jnp.float32
    ) * HEAD ** (-0.5)
    near = jnp.abs(jnp.arange(WINDOW)[:, None] + WINDOW - jnp.arange(3 * WINDOW)[None, :]) <= WINDOW
    first_token = lax.axis_index("sp") * length
    key_pos = (
        first_token + (jnp.arange(blocks)[:, None] - 1) * WINDOW + jnp.arange(3 * WINDOW)[None, :]
    )
    inside = (key_pos >= 0) & (key_pos < length * lax.axis_size("sp"))
    valid = near[None, None, None, :, :] & inside[:, None, None, None, :]
    sinks = sink_logit.reshape(1, groups, repeat, 1, 1)
    masked = jnp.where(valid, scores, NEGATIVE)
    top = jnp.maximum(jnp.max(masked, axis=-1, keepdims=True), sinks)
    probs = jnp.exp(masked - top)
    denom = jnp.sum(probs, axis=-1, keepdims=True) + jnp.exp(sinks - top)
    weights = (probs / denom).astype(jnp.bfloat16)
    output = jnp.einsum(
        "ngrqk,nkgd->nqgrd", weights, value_band, preferred_element_type=jnp.float32
    )
    return output.astype(jnp.bfloat16).reshape(length, groups * repeat * HEAD)


def local(
    queries,
    keys,
    values,
    sink_logit,
    out_weight,
    residual,
    norm_gain,
    routes,
    route_weights,
    gate_weight,
    up_weight,
    down_weight,
):
    capacity = max(2, 4 * residual.shape[0] // lax.axis_size("sp"))
    in_plane = (
        lax.axis_size("tp") == 4
        and lax.axis_size("sp") == 8
        and capacity % 32 == 0
        and gate_weight.shape[2] % 256 == 0
        and queries.shape[0] == 2 * WINDOW
    )
    if in_plane:
        hidden_state, normed = attend_project(
            queries, keys, values, sink_logit, out_weight, residual, norm_gain
        )
    else:
        attention = attend_local(queries, keys, values, sink_logit)
        columns = jnp.dot(
            lax.all_gather(attention, "tp", axis=1, tiled=True),
            out_weight,
            preferred_element_type=jnp.float32,
        )
        projected = lax.all_to_all(
            columns.astype(jnp.bfloat16), "tp", split_axis=0, concat_axis=1, tiled=True
        )
        hidden_state = residual.astype(jnp.float32) + projected.astype(jnp.float32)
        inverse = lax.rsqrt(jnp.mean(hidden_state * hidden_state, axis=-1, keepdims=True) + EPS)
        normed = (hidden_state * inverse * norm_gain).astype(jnp.bfloat16)
    sp_count = lax.axis_size("sp")
    tok_rows = residual.shape[0]
    width = residual.shape[1]
    slot_total = sp_count * capacity
    expert_ids = routes.reshape(-1)
    onehot = (expert_ids[:, None] == jnp.arange(sp_count, dtype=jnp.int32)[None, :]).astype(
        jnp.int32
    )
    earlier = jnp.cumsum(onehot, axis=0) - onehot
    rank = jnp.sum(earlier * onehot, axis=1)
    slots = expert_ids * capacity + rank
    placing = (slots[:, None] == jnp.arange(slot_total, dtype=jnp.int32)[None, :]).astype(
        jnp.bfloat16
    )
    placing = placing.reshape(tok_rows, 2, slot_total)
    first_place = placing[:, 0]
    second_place = placing[:, 1]
    sending = jnp.einsum(
        "ts,td->sd", first_place + second_place, normed, preferred_element_type=jnp.float32
    )
    sending = sending.astype(jnp.bfloat16).reshape(sp_count, capacity, width)
    if in_plane:
        returned = experts(sending, gate_weight[0], up_weight[0], down_weight[0])
    else:
        piece = lax.all_gather(
            lax.all_to_all(sending, "sp", split_axis=0, concat_axis=0, tiled=True),
            "tp",
            axis=0,
            tiled=True,
        )
        flat = piece.reshape(-1, piece.shape[-1])
        gate = jnp.dot(flat, gate_weight[0], preferred_element_type=jnp.float32)
        upward = jnp.dot(flat, up_weight[0], preferred_element_type=jnp.float32)
        hidden = (jax.nn.silu(gate) * upward).astype(jnp.bfloat16)
        partial_value = jnp.dot(hidden, down_weight[0], preferred_element_type=jnp.float32)
        partial_value = partial_value.reshape(piece.shape[:-1] + (down_weight.shape[-1],))
        returned = lax.all_to_all(
            lax.psum_scatter(
                partial_value.astype(jnp.bfloat16), "tp", scatter_dimension=0, tiled=True
            ),
            "sp",
            split_axis=0,
            concat_axis=0,
            tiled=True,
        )
    gathered_back = returned.reshape(slot_total, width)
    first_pick = jnp.dot(first_place, gathered_back, preferred_element_type=jnp.float32)
    second_pick = jnp.dot(second_place, gathered_back, preferred_element_type=jnp.float32)
    mixture = route_weights[:, 0:1] * first_pick + route_weights[:, 1:2] * second_pick
    return (hidden_state + mixture).astype(jnp.bfloat16)


def solution(mesh):
    in_specs = (
        P("sp", "tp"),
        P("sp", "tp"),
        P("sp", "tp"),
        P("tp"),
        P(None, "tp"),
        P(("sp", "tp"), None),
        P(),
        P(("sp", "tp"), None),
        P(("sp", "tp"), None),
        P("sp", None, "tp"),
        P("sp", None, "tp"),
        P("sp", "tp", None),
    )
    out_specs = P(("sp", "tp"), None)
    return jax.shard_map(local, mesh=mesh, in_specs=in_specs, out_specs=out_specs, check_vma=False)
```

```python
import functools

import jax
import jax.numpy as jnp
from jax import lax
from jax.experimental import pallas as pl
from jax.experimental.pallas import tpu as pltpu
from jax.sharding import PartitionSpec as P

HEADS = 32
KV_HEADS = 16
HEAD = 64
WINDOW = 128


EPS = 1e-06
NEGATIVE = -1e30
MESH = pl.DeviceIdType.MESH


def plane():
    t = lax.axis_index("tp")
    tx = t + 1 - 2 * lax.rem(t, 2)
    ty = lax.rem(t + 2, 4)
    return t, tx, ty, 3 - t


def remote(src, dst, send, recv, device):
    return pltpu.make_async_remote_copy(
        src_ref=src,
        dst_ref=dst,
        send_sem=send,
        recv_sem=recv,
        device_id=device,
        device_id_type=MESH,
    )


def flipped(index, mask):
    result = index
    bit = 1
    while bit <= mask:
        if mask & bit:
            result = result + bit * (1 - 2 * lax.rem(index // bit, 2))
        bit *= 2
    return result


def layer_kernel(
    q_hbm, k_hbm, v_hbm, sink_ref, w_hbm, res_hbm, gain_ref, routes_ref, route_weights_ref,
    gate_hbm, up_hbm, down_hbm, out_ref,
    q, kv, w, res, buf, acc, cols, got, state, gate, up, down,
    meta, meta_in, meta_z, meta_p, tok, xs, xo, hidden, po, ps, rt,
    bx1, by1, bx2, by2, mid, sz, zin, home_sum,
    load, hs, hr, gs, gr, as_, ar, ms, mr, zs, zr, ds_, dr, xs_s, xs_r, ps_s, ps_r,
    rs, rr, zbs, zbr,
):
    s = lax.axis_index("sp")
    t, tx, ty, td = plane()
    last = lax.axis_size("sp") - 1
    rows, depth = q.shape
    half = rows // 2
    groups = k_hbm.shape[1] // HEAD
    kept = groups * HEAD
    odd = lax.rem(s, 2)
    near = s + 1 - 2 * odd
    has_far = jnp.logical_and(s != 0, s != last)
    far = jnp.where(has_far, s - 1 + 2 * odd, near)
    x_dev, y_dev, d_dev, n_dev, f_dev = (s, tx), (s, ty), (s, td), (near, t), (far, t)
    z = s // 2
    planes = [flipped(z, m) for m in range(4)]
    z_devs = [(2 * planes[m] + odd, t) for m in range(4)]
    middle = pl.ds(half, rows)
    loads = [
        pltpu.make_async_copy(source, target, load.at[k])
        for k, (source, target) in enumerate(
            (
                (k_hbm, kv.at[middle, pl.ds(0, kept)]),
                (v_hbm, kv.at[middle, pl.ds(kept, kept)]),
                (q_hbm, q),
                (w_hbm, w),
                (res_hbm, res),
                (gate_hbm, gate),
                (up_hbm, up),
                (down_hbm, down),
            )
        )
    ]
    for copy in loads[:5]:
        copy.start()
    barrier = pltpu.get_barrier_semaphore()
    for device in [x_dev, y_dev, d_dev, n_dev] + z_devs[1:]:
        pl.semaphore_signal(barrier, inc=1, device_id=device, device_id_type=MESH)

    @pl.when(has_far)
    def _():
        pl.semaphore_signal(barrier, inc=1, device_id=f_dev, device_id_type=MESH)
        pl.semaphore_wait(barrier, 8)

    @pl.when(jnp.logical_not(has_far))
    def _():
        pl.semaphore_wait(barrier, 7)

    def aligned(value, size):
        return pl.ds(pl.multiple_of(value, size), size)

    near_src = aligned(2 * half - half * odd, half)
    near_dst = aligned(3 * half * odd, half)
    far_src = aligned(half + half * odd, half)
    far_dst = aligned(3 * half * (1 - odd), half)
    near_copy = remote(kv.at[near_src], kv.at[near_dst], hs.at[0], hr.at[0], n_dev)
    far_copy = remote(kv.at[far_src], kv.at[far_dst], hs.at[1], hr.at[1], f_dev)
    loads[0].wait()
    loads[1].wait()

    @pl.when(has_far)
    def _():
        far_copy.start()

    near_copy.start()
    copies = []

    def go(*args):
        copy = remote(*args)
        copy.start()
        copies.append(copy)
        return copy

    count, lanes = meta.shape[0] // 2, meta.shape[1]
    tokens = lanes // 4
    expert = lax.broadcasted_iota(jnp.int32, (count, lanes), 0)
    lane = lax.broadcasted_iota(jnp.int32, (count, lanes), 1)
    mine_lane = jnp.logical_and(lane >= t * tokens, lane < (t + 1) * tokens)
    hit_one = routes_ref[0:1, :] == expert
    hit = jnp.logical_and(mine_lane, jnp.logical_or(hit_one, routes_ref[1:2, :] == expert))
    chosen = jnp.where(hit, 1.0, 0.0)
    before = lax.broadcasted_iota(jnp.int32, (lanes, lanes), 0) <= lax.broadcasted_iota(
        jnp.int32, (lanes, lanes), 1
    )
    rank = jnp.dot(
        chosen.astype(jnp.bfloat16),
        jnp.where(before, 1.0, 0.0).astype(jnp.bfloat16),
        preferred_element_type=jnp.float32,
    )
    meta[0:count] = chosen * rank
    meta[count : 2 * count] = chosen * jnp.where(
        hit_one, route_weights_ref[0:1, :], route_weights_ref[1:2, :]
    )
    meta_copies = [
        go(meta, meta_in.at[t], ms.at[k], mr.at[k], device)
        for k, device in enumerate((x_dev, y_dev, d_dev))
    ]

    for copy in loads[5:]:
        copy.start()

    @pl.when(jnp.logical_not(has_far))
    def _():
        kv[aligned(3 * half * odd, half)] = jnp.zeros((half, kv.shape[1]), kv.dtype)

    loads[2].wait()
    span = 3 * half
    query = lax.broadcasted_iota(jnp.int32, (2 * half, span), 0)
    query = jnp.where(query >= half, query - half, query)
    key = lax.broadcasted_iota(jnp.int32, (2 * half, span), 1)
    band = jnp.abs(query + half - key) <= WINDOW
    upper = lax.broadcasted_iota(jnp.int32, (2 * half, 1), 0) < half

    def attend(b):
        valid = jnp.logical_and(
            band,
            jnp.logical_and(
                key >= jnp.where(2 * s + b == 0, half, 0),
                key < jnp.where(2 * s + b == 2 * last + 1, 2 * half, span),
            ),
        )
        keys_at = pl.ds(pl.multiple_of(b * half, half), span)
        mine = aligned(b * half, half)
        for g in range(groups):
            pair = q[mine, 2 * g * HEAD : 2 * (g + 1) * HEAD]
            stacked = jnp.concatenate([pair[:, :HEAD], pair[:, HEAD:]], axis=0)
            scores = lax.dot_general(
                stacked,
                kv[keys_at, g * HEAD : (g + 1) * HEAD],
                (((1,), (1,)), ((), ())),
                preferred_element_type=jnp.float32,
            ) * HEAD ** (-0.5)
            sink = jnp.where(upper, sink_ref[2 * g], sink_ref[2 * g + 1])
            masked = jnp.where(valid, scores, NEGATIVE)
            top = jnp.maximum(jnp.max(masked, axis=-1, keepdims=True), sink)
            probs = jnp.exp(masked - top)
            denom = jnp.sum(probs, axis=-1, keepdims=True) + jnp.exp(sink - top)
            weights = (probs * (1.0 / denom)).astype(jnp.bfloat16)
            output = jnp.dot(
                weights,
                kv[keys_at, kept + g * HEAD : kept + (g + 1) * HEAD],
                preferred_element_type=jnp.float32,
            )
            joined = jnp.concatenate([output[:half], output[half:]], axis=1)
            buf[t, mine, 2 * g * HEAD : 2 * (g + 1) * HEAD] = joined.astype(buf.dtype)

    first_block, second_block = 1 - odd, odd
    def spread(b, k):
        piece = buf.at[t, aligned(b * half, half)]
        return (
            go(piece, piece, gs.at[k], gr.at[k], x_dev),
            go(piece, piece, gs.at[k + 1], gr.at[k + 1], y_dev),
        )

    near_copy.wait_recv()
    attend(first_block)
    x_one, y_one = spread(first_block, 0)

    @pl.when(has_far)
    def _():
        far_copy.wait_recv()

    attend(second_block)
    x_two, y_two = spread(second_block, 2)
    for copy in meta_copies:
        copy.wait_recv()
    meta_z[z] = (meta[...] + meta_in[tx]) + (meta_in[ty] + meta_in[td])
    meta_z_copies = [
        go(meta_z.at[z], meta_z.at[z], ms.at[2 + m], mr.at[2 + m], z_devs[m]) for m in (1, 2, 3)
    ]
    loads[3].wait()

    def product(b, owner):
        weight = w[pl.ds(pl.multiple_of(owner * depth, depth), depth)]
        piece = buf[owner, aligned(b * half, half)]
        return jnp.dot(piece, weight, preferred_element_type=jnp.float32)

    x_one.wait_recv()
    piece = buf.at[tx, aligned(first_block * half, half)]
    d_one = go(piece, piece, gs.at[4], gr.at[4], y_dev)
    acc[0] = product(first_block, t)
    acc[0] += product(first_block, tx)
    y_one.wait_recv()
    acc[0] += product(first_block, ty)
    y_two.wait_recv()
    piece = buf.at[ty, aligned(second_block * half, half)]
    d_two = go(piece, piece, gs.at[5], gr.at[5], x_dev)
    acc[1] = product(second_block, t)
    acc[1] += product(second_block, ty)
    own = rows // 4
    to_x = remote(
        cols.at[aligned(tx * own, own)], got.at[t], as_.at[0], ar.at[0], x_dev
    )
    to_y = remote(
        cols.at[aligned(ty * own, own)], got.at[t], as_.at[1], ar.at[1], y_dev
    )
    to_d = remote(
        cols.at[aligned(td * own, own)], got.at[t], as_.at[2], ar.at[2], d_dev
    )
    home = t // 2

    def finish(b, k):
        total = acc[k] + product(b, td)
        cols[aligned(b * half, half)] = total.astype(cols.dtype)

        @pl.when(home == b)
        def _():
            to_x.start()

        @pl.when(home != b)
        def _():
            to_d.start()
            to_y.start()

    d_one.wait_recv()
    finish(first_block, 0)
    x_two.wait_recv()
    acc[1] += product(second_block, tx)
    d_two.wait_recv()
    finish(second_block, 1)
    got[t] = cols[aligned(t * own, own)]
    loads[4].wait()
    to_x.wait_recv()
    to_y.wait_recv()
    to_d.wait_recv()
    squares = jnp.zeros((own, 1), jnp.float32)
    width = w.shape[1]
    for k in range(4):
        columns = slice(k * width, (k + 1) * width)
        value = res[:, columns].astype(jnp.float32) + got[k].astype(jnp.float32)
        state[:, columns] = value
        squares += jnp.sum(value * value, axis=-1, keepdims=True)
    inverse = lax.rsqrt(squares * (1.0 / (4 * width)) + EPS)
    for k in range(4):
        columns = slice(k * width, (k + 1) * width)
        tok[t, z, :, columns] = (state[:, columns] * inverse * gain_ref[:, columns]).astype(
            tok.dtype
        )
    low, high = pl.ds(0, own // 2), pl.ds(own // 2, own // 2)
    z_copies = {
        m: go(tok.at[t, z], tok.at[t, z], zs.at[m], zr.at[m], z_devs[m]) for m in (1, 3, 2)
    }
    sent, forwarded, picks, parts, firsts, seconds, homes = {}, {}, {}, {}, {}, {}, {}

    def send(m):
        if m:
            z_copies[m].wait_recv()
        lower, upper = tok.at[t, planes[m], low], tok.at[t, planes[m], high]
        sent[m] = (
            go(lower, lower, ds_.at[m, 0], dr.at[m, 0], x_dev),
            go(upper, upper, ds_.at[m, 1], dr.at[m, 1], y_dev),
            go(upper, upper, ds_.at[m, 2], dr.at[m, 2], x_dev),
            go(lower, lower, ds_.at[m, 3], dr.at[m, 3], y_dev),
        )

    def forward(m):
        sent[m][0].wait_recv()
        block = tok.at[tx, planes[m], low]
        to_side = go(block, block, ds_.at[m, 4], dr.at[m, 4], y_dev)
        sent[m][1].wait_recv()
        block = tok.at[ty, planes[m], high]
        forwarded[m] = (to_side, go(block, block, ds_.at[m, 5], dr.at[m, 5], x_dev))

    slots = xo.shape[1]
    capacity = slots // 4
    step = 256
    model = tok.shape[3]
    row = lax.broadcasted_iota(jnp.int32, (slots, lanes), 0).astype(jnp.float32)
    shift = (lax.broadcasted_iota(jnp.int32, (1, lanes), 1) // tokens * capacity).astype(
        jnp.float32
    )
    mine_expert, near_expert = s, near

    def place(source, m, which):
        ranks = source[planes[m], pl.ds(which, 1), :]
        target = jnp.where(ranks > 0.5, ranks + (shift - 1.0), -1.0)
        return row == target

    def scale(source, m, which):
        weights = source[planes[m], pl.ds(count + which, 1), :]
        return jnp.sum(
            jnp.where(place(source, m, which), weights, 0.0), axis=1, keepdims=True
        )

    def picking(m):
        return jnp.concatenate(
            [
                jnp.where(place(meta_z, m, which), 1.0, 0.0)
                for which in (mine_expert, near_expert)
            ],
            axis=0,
        )

    def pick(m):
        for copy in sent[m][2:] + forwarded[m]:
            copy.wait_recv()
        chooser = picking(m).astype(jnp.bfloat16)
        for k in range(model // step):
            columns = slice(k * step, (k + 1) * step)
            rows_in = tok[:, planes[m], :, columns].reshape(lanes, step)
            found = jnp.dot(chooser, rows_in, preferred_element_type=jnp.float32)
            found = found.astype(xs.dtype)
            xs[m, 0:slots, columns] = found[:slots]
            xo[m, :, columns] = found[slots:]
        picks[m] = go(
            xo.at[m], xs.at[m, pl.ds(slots, slots)], xs_s.at[m], xs_r.at[m], n_dev
        )

    def rise(m, begin, end):
        @pl.loop(begin, end)
        def _(k):
            columns = pl.ds(pl.multiple_of(k * step, step), step)
            x = xs[m]
            g = jnp.dot(x, gate[:, columns], preferred_element_type=jnp.float32)
            u = jnp.dot(x, up[:, columns], preferred_element_type=jnp.float32)
            hidden[:, columns] = (jax.nn.silu(g) * u).astype(hidden.dtype)

    total_steps = gate.shape[1] // step
    first_steps = (total_steps + 1) // 2

    def fall(m):
        factor_mine = scale(meta_z, m, mine_expert)
        factor_near = scale(meta_p, m, mine_expert)
        wide = 512

        @pl.loop(0, model // wide)
        def _(k):
            columns = pl.ds(pl.multiple_of(k * wide, wide), wide)
            share = jnp.dot(hidden[...], down[:, columns], preferred_element_type=jnp.float32)
            po[m, 0:slots, columns] = (share[:slots] * factor_mine).astype(po.dtype)
            ps[m, :, columns] = (share[slots:] * factor_near).astype(ps.dtype)

        parts[m] = go(
            ps.at[m], po.at[m, pl.ds(slots, slots)], ps_s.at[m], ps_r.at[m], n_dev
        )

    def expand(m):
        parts[m].wait_recv()
        spreader = picking(m).T.astype(jnp.bfloat16)
        for k in range(model // step):
            columns = slice(k * step, (k + 1) * step)
            found = jnp.dot(spreader, po[m, :, columns], preferred_element_type=jnp.float32)
            rt[m, :, :, columns] = found.astype(rt.dtype).reshape(4, tokens, step)

    def reduce_one(m):
        firsts[m] = (
            go(rt.at[m, td, low], bx1.at[m, 1], rs.at[m, 0], rr.at[m, 0], x_dev),
            go(rt.at[m, td, high], by1.at[m, 1], rs.at[m, 1], rr.at[m, 1], y_dev),
            go(rt.at[m, tx, low], bx1.at[m, 0], rs.at[m, 2], rr.at[m, 2], x_dev),
            go(rt.at[m, ty, high], by1.at[m, 0], rs.at[m, 3], rr.at[m, 3], y_dev),
        )

    def wide_sum(*pieces):
        result = pieces[0].astype(jnp.float32)
        for piece in pieces[1:]:
            result = result + piece.astype(jnp.float32)
        return result

    def reduce_two(m):
        firsts[m][0].wait_recv()
        mid[m, 0] = wide_sum(rt[m, ty, low], bx1[m, 1]).astype(mid.dtype)
        to_side = go(mid.at[m, 0], by2.at[m], rs.at[m, 4], rr.at[m, 4], y_dev)
        firsts[m][1].wait_recv()
        mid[m, 1] = wide_sum(rt[m, tx, high], by1[m, 1]).astype(mid.dtype)
        seconds[m] = (
            to_side,
            go(mid.at[m, 1], bx2.at[m], rs.at[m, 5], rr.at[m, 5], x_dev),
        )

    def reduce_three(m):
        firsts[m][2].wait_recv()
        seconds[m][0].wait_recv()
        lower = wide_sum(rt[m, t, low], bx1[m, 0], by2[m])
        firsts[m][3].wait_recv()
        seconds[m][1].wait_recv()
        upper = wide_sum(rt[m, t, high], by1[m, 0], bx2[m])
        if m:
            sz[m, low] = lower.astype(sz.dtype)
            sz[m, high] = upper.astype(sz.dtype)
            homes[m] = go(sz.at[m], zin.at[m], zbs.at[m], zbr.at[m], z_devs[m])
        else:
            home_sum[low] = lower
            home_sum[high] = upper

    send(0)
    forward(0)
    for copy in meta_z_copies:
        copy.wait_recv()
    meta_near = go(meta_z, meta_p, ms.at[6], mr.at[6], n_dev)
    send(1)
    pick(0)
    for copy in loads[5:]:
        copy.wait()
    picks[0].wait_recv()
    rise(0, 0, first_steps)
    forward(1)
    send(3)
    rise(0, first_steps, total_steps)
    meta_near.wait_recv()
    fall(0)
    pick(1)
    picks[1].wait_recv()
    rise(1, 0, first_steps)
    forward(3)
    send(2)
    rise(1, first_steps, total_steps)
    fall(1)
    pick(3)
    picks[3].wait_recv()
    rise(3, 0, first_steps)
    forward(2)
    rise(3, first_steps, total_steps)
    fall(3)
    expand(3)
    reduce_one(3)
    pick(2)
    picks[2].wait_recv()
    rise(2, 0, first_steps)
    reduce_two(3)
    rise(2, first_steps, total_steps)
    fall(2)
    expand(2)
    reduce_one(2)
    reduce_three(3)
    expand(1)
    reduce_one(1)
    reduce_two(2)
    expand(0)
    reduce_one(0)
    reduce_three(2)
    reduce_two(1)
    reduce_three(1)
    reduce_two(0)
    reduce_three(0)
    for m in (3, 2, 1):
        homes[m].wait_recv()
    out_ref[...] = (
        state[...] + (home_sum[...] + wide_sum(zin[1], zin[2], zin[3]))
    ).astype(out_ref.dtype)
    for copy in copies:
        copy.wait_send()
    near_copy.wait_send()
    to_x.wait_send()
    to_y.wait_send()
    to_d.wait_send()

    @pl.when(has_far)
    def _():
        far_copy.wait_send()


def layer(
    queries, keys, values, sink_logit, out_weight, residual, norm_gain, routes, route_weights,
    gate_weight, up_weight, down_weight, capacity,
):
    rows, depth = queries.shape
    kind = queries.dtype
    width = out_weight.shape[1]
    tokens, model = residual.shape
    count = lax.axis_size("sp")
    slots = 4 * capacity
    anywhere = pl.BlockSpec(memory_space=pl.ANY)
    vmem = pl.BlockSpec(memory_space=pltpu.VMEM)
    dma = pltpu.SemaphoreType.DMA
    one, six = dma((4,)), dma((4, 6))
    lanes = 4 * tokens
    return pl.pallas_call(
        layer_kernel,
        out_shape=jax.ShapeDtypeStruct(residual.shape, kind),
        in_specs=[anywhere] * 3
        + [pl.BlockSpec(memory_space=pltpu.SMEM), anywhere, anywhere, vmem, vmem, vmem]
        + [anywhere] * 3,
        out_specs=vmem,
        scratch_shapes=[
            pltpu.VMEM(queries.shape, kind),
            pltpu.VMEM((2 * rows, 2 * keys.shape[1]), kind),
            pltpu.VMEM(out_weight.shape, kind),
            pltpu.VMEM(residual.shape, kind),
            pltpu.VMEM((4, rows, depth), kind),
            pltpu.VMEM((2, rows // 2, width), jnp.float32),
            pltpu.VMEM((rows, width), kind),
            pltpu.VMEM((4, rows // 4, width), kind),
            pltpu.VMEM(residual.shape, jnp.float32),
            pltpu.VMEM(gate_weight.shape, kind),
            pltpu.VMEM(up_weight.shape, kind),
            pltpu.VMEM(down_weight.shape, kind),
            pltpu.VMEM((2 * count, lanes), jnp.float32),
            pltpu.VMEM((4, 2 * count, lanes), jnp.float32),
            pltpu.VMEM((4, 2 * count, lanes), jnp.float32),
            pltpu.VMEM((4, 2 * count, lanes), jnp.float32),
            pltpu.VMEM((4, 4, tokens, model), kind),
            pltpu.VMEM((4, 2 * slots, model), kind),
            pltpu.VMEM((4, slots, model), kind),
            pltpu.VMEM((2 * slots, gate_weight.shape[1]), kind),
            pltpu.VMEM((4, 2 * slots, model), kind),
            pltpu.VMEM((4, slots, model), kind),
            pltpu.VMEM((4, 4, tokens, model), kind),
            pltpu.VMEM((4, 2, tokens // 2, model), kind),
            pltpu.VMEM((4, 2, tokens // 2, model), kind),
            pltpu.VMEM((4, tokens // 2, model), kind),
            pltpu.VMEM((4, tokens // 2, model), kind),
            pltpu.VMEM((4, 2, tokens // 2, model), kind),
            pltpu.VMEM((4, tokens, model), kind),
            pltpu.VMEM((4, tokens, model), kind),
            pltpu.VMEM(residual.shape, jnp.float32),
            dma((8,)),
            dma((2,)),
            dma((2,)),
            dma((6,)),
            dma((6,)),
            dma((3,)),
            dma((3,)),
            dma((7,)),
            dma((7,)),
            one, one, six, six, one, one, one, one, six, six, one, one,
        ],
        compiler_params=pltpu.CompilerParams(
            collective_id=0, has_side_effects=True, vmem_limit_bytes=60 * 1024 * 1024
        ),
    )(
        queries, keys, values, sink_logit, out_weight, residual, norm_gain.reshape(1, -1),
        jnp.tile(routes.T, (1, 4)), jnp.tile(route_weights.T, (1, 4)),
        gate_weight, up_weight, down_weight,
    )


def with_halo(block, sides, width):
    for axis, dim in sides:
        count = lax.axis_size(axis)
        forward = [(i, i + 1) for i in range(count - 1)]
        backward = [(target, source) for source, target in forward]
        low = lax.ppermute(
            lax.slice_in_dim(block, block.shape[dim] - width, None, axis=dim), axis, forward
        )
        high = lax.ppermute(lax.slice_in_dim(block, 0, width, axis=dim), axis, backward)
        block = jnp.concatenate([low, block, high], axis=dim)
    return block


def make_band(extended, length):
    blocks = length // WINDOW
    pieces = [
        lax.slice_in_dim(extended, offset * WINDOW, offset * WINDOW + length, axis=0).reshape(
            blocks, WINDOW, -1
        )
        for offset in range(3)
    ]
    return jnp.concatenate(pieces, axis=1)


def attend_local(queries, keys, values, sink_logit):
    length = queries.shape[0]
    groups = keys.shape[1] // HEAD
    repeat = HEADS // KV_HEADS
    blocks = length // WINDOW
    joined = jnp.concatenate([keys, values], axis=1)
    extended = with_halo(joined, (("sp", 0),), WINDOW)
    banded = make_band(extended, length)
    key_band = banded[..., : groups * HEAD].reshape(blocks, 3 * WINDOW, groups, HEAD)
    value_band = banded[..., groups * HEAD :].reshape(blocks, 3 * WINDOW, groups, HEAD)
    query_blocks = queries.reshape(blocks, WINDOW, groups, repeat, HEAD)
    scores = jnp.einsum(
        "nqgrd,nkgd->ngrqk", query_blocks, key_band, preferred_element_type=jnp.float32
    ) * HEAD ** (-0.5)
    near = jnp.abs(jnp.arange(WINDOW)[:, None] + WINDOW - jnp.arange(3 * WINDOW)[None, :]) <= WINDOW
    first_token = lax.axis_index("sp") * length
    key_pos = (
        first_token + (jnp.arange(blocks)[:, None] - 1) * WINDOW + jnp.arange(3 * WINDOW)[None, :]
    )
    inside = (key_pos >= 0) & (key_pos < length * lax.axis_size("sp"))
    valid = near[None, None, None, :, :] & inside[:, None, None, None, :]
    sinks = sink_logit.reshape(1, groups, repeat, 1, 1)
    masked = jnp.where(valid, scores, NEGATIVE)
    top = jnp.maximum(jnp.max(masked, axis=-1, keepdims=True), sinks)
    probs = jnp.exp(masked - top)
    denom = jnp.sum(probs, axis=-1, keepdims=True) + jnp.exp(sinks - top)
    weights = (probs / denom).astype(jnp.bfloat16)
    output = jnp.einsum(
        "ngrqk,nkgd->nqgrd", weights, value_band, preferred_element_type=jnp.float32
    )
    return output.astype(jnp.bfloat16).reshape(length, groups * repeat * HEAD)


def local(
    queries,
    keys,
    values,
    sink_logit,
    out_weight,
    residual,
    norm_gain,
    routes,
    route_weights,
    gate_weight,
    up_weight,
    down_weight,
):
    capacity = max(2, 4 * residual.shape[0] // lax.axis_size("sp"))
    in_plane = (
        lax.axis_size("tp") == 4
        and lax.axis_size("sp") == 8
        and capacity % 32 == 0
        and gate_weight.shape[2] % 256 == 0
        and queries.shape[0] == 2 * WINDOW
        and residual.shape[0] == 64
    )
    if in_plane:
        return layer(
            queries, keys, values, sink_logit, out_weight, residual, norm_gain, routes,
            route_weights, gate_weight[0], up_weight[0], down_weight[0], capacity,
        )
    attention = attend_local(queries, keys, values, sink_logit)
    columns = jnp.dot(
        lax.all_gather(attention, "tp", axis=1, tiled=True),
        out_weight,
        preferred_element_type=jnp.float32,
    )
    projected = lax.all_to_all(
        columns.astype(jnp.bfloat16), "tp", split_axis=0, concat_axis=1, tiled=True
    )
    hidden_state = residual.astype(jnp.float32) + projected.astype(jnp.float32)
    inverse = lax.rsqrt(jnp.mean(hidden_state * hidden_state, axis=-1, keepdims=True) + EPS)
    normed = (hidden_state * inverse * norm_gain).astype(jnp.bfloat16)
    sp_count = lax.axis_size("sp")
    tok_rows = residual.shape[0]
    width = residual.shape[1]
    slot_total = sp_count * capacity
    expert_ids = routes.reshape(-1)
    onehot = (expert_ids[:, None] == jnp.arange(sp_count, dtype=jnp.int32)[None, :]).astype(
        jnp.int32
    )
    earlier = jnp.cumsum(onehot, axis=0) - onehot
    rank = jnp.sum(earlier * onehot, axis=1)
    slots = expert_ids * capacity + rank
    placing = (slots[:, None] == jnp.arange(slot_total, dtype=jnp.int32)[None, :]).astype(
        jnp.bfloat16
    )
    placing = placing.reshape(tok_rows, 2, slot_total)
    first_place = placing[:, 0]
    second_place = placing[:, 1]
    sending = jnp.einsum(
        "ts,td->sd", first_place + second_place, normed, preferred_element_type=jnp.float32
    )
    sending = sending.astype(jnp.bfloat16).reshape(sp_count, capacity, width)
    piece = lax.all_gather(
        lax.all_to_all(sending, "sp", split_axis=0, concat_axis=0, tiled=True),
        "tp",
        axis=0,
        tiled=True,
    )
    flat = piece.reshape(-1, piece.shape[-1])
    gate = jnp.dot(flat, gate_weight[0], preferred_element_type=jnp.float32)
    upward = jnp.dot(flat, up_weight[0], preferred_element_type=jnp.float32)
    hidden = (jax.nn.silu(gate) * upward).astype(jnp.bfloat16)
    partial_value = jnp.dot(hidden, down_weight[0], preferred_element_type=jnp.float32)
    partial_value = partial_value.reshape(piece.shape[:-1] + (down_weight.shape[-1],))
    returned = lax.all_to_all(
        lax.psum_scatter(
            partial_value.astype(jnp.bfloat16), "tp", scatter_dimension=0, tiled=True
        ),
        "sp",
        split_axis=0,
        concat_axis=0,
        tiled=True,
    )
    gathered_back = returned.reshape(slot_total, width)
    first_pick = jnp.dot(first_place, gathered_back, preferred_element_type=jnp.float32)
    second_pick = jnp.dot(second_place, gathered_back, preferred_element_type=jnp.float32)
    mixture = route_weights[:, 0:1] * first_pick + route_weights[:, 1:2] * second_pick
    return (hidden_state + mixture).astype(jnp.bfloat16)


def solution(mesh):
    in_specs = (
        P("sp", "tp"),
        P("sp", "tp"),
        P("sp", "tp"),
        P("tp"),
        P(None, "tp"),
        P(("sp", "tp"), None),
        P(),
        P(("sp", "tp"), None),
        P(("sp", "tp"), None),
        P("sp", None, "tp"),
        P("sp", None, "tp"),
        P("sp", "tp", None),
    )
    out_specs = P(("sp", "tp"), None)
    return jax.shard_map(local, mesh=mesh, in_specs=in_specs, out_specs=out_specs, check_vma=False)
```

```python
import functools

import jax
import jax.numpy as jnp
from jax import lax
from jax.experimental import pallas as pl
from jax.experimental.pallas import tpu as pltpu
from jax.sharding import PartitionSpec as P

HEADS = 32
KV_HEADS = 16
HEAD = 64
WINDOW = 128


EPS = 1e-06
NEGATIVE = -1e30
MESH = pl.DeviceIdType.MESH


def plane():
    t = lax.axis_index("tp")
    tx = t + 1 - 2 * lax.rem(t, 2)
    ty = lax.rem(t + 2, 4)
    return t, tx, ty, 3 - t


def remote(src, dst, send, recv, device):
    return pltpu.make_async_remote_copy(
        src_ref=src,
        dst_ref=dst,
        send_sem=send,
        recv_sem=recv,
        device_id=device,
        device_id_type=MESH,
    )


def flipped(index, mask):
    result = index
    bit = 1
    while bit <= mask:
        if mask & bit:
            result = result + bit * (1 - 2 * lax.rem(index // bit, 2))
        bit *= 2
    return result


def layer_kernel(
    q_hbm, k_hbm, v_hbm, sink_ref, w_hbm, res_hbm, gain_ref, routes_ref, route_weights_ref,
    gate_hbm, up_hbm, down_hbm, out_ref,
    q, kv, w, res, res_in, buf, acc, proj, gate, up, down,
    meta, meta_in, meta_z, meta_p, squares, squares_in, inverse, tok, xs, xo, hidden, po, ps, rt,
    bx1, by1, bx2, by2, mid, sz, zin, home_sum,
    load, hs, hr, gs, gr, as_, ar, ms, mr, qs, qr, zs, zr, ds_, dr, xs_s, xs_r, ps_s, ps_r,
    rs, rr, zbs, zbr,
):
    s = lax.axis_index("sp")
    t, tx, ty, td = plane()
    last = lax.axis_size("sp") - 1
    rows, depth = q.shape
    half = rows // 2
    groups = k_hbm.shape[1] // HEAD
    kept = groups * HEAD
    odd = lax.rem(s, 2)
    near = s + 1 - 2 * odd
    has_far = jnp.logical_and(s != 0, s != last)
    far = jnp.where(has_far, s - 1 + 2 * odd, near)
    x_dev, y_dev, d_dev, n_dev, f_dev = (s, tx), (s, ty), (s, td), (near, t), (far, t)
    z = s // 2
    planes = [flipped(z, m) for m in range(4)]
    z_devs = [(2 * planes[m] + odd, t) for m in range(4)]
    inner = jnp.logical_or(z == 1, z == 2)
    outer = jnp.logical_not(inner)
    middle = pl.ds(half, rows)
    loads = [
        pltpu.make_async_copy(source, target, load.at[k])
        for k, (source, target) in enumerate(
            (
                (k_hbm, kv.at[middle, pl.ds(0, kept)]),
                (v_hbm, kv.at[middle, pl.ds(kept, kept)]),
                (q_hbm, q),
                (w_hbm, w),
                (res_hbm, res),
                (gate_hbm, gate),
                (up_hbm, up),
                (down_hbm, down),
            )
        )
    ]
    for copy in loads[:5]:
        copy.start()
    barrier = pltpu.get_barrier_semaphore()
    for device in [x_dev, y_dev, d_dev, n_dev] + z_devs[1:]:
        pl.semaphore_signal(barrier, inc=1, device_id=device, device_id_type=MESH)

    @pl.when(has_far)
    def _():
        pl.semaphore_signal(barrier, inc=1, device_id=f_dev, device_id_type=MESH)
        pl.semaphore_wait(barrier, 8)

    @pl.when(jnp.logical_not(has_far))
    def _():
        pl.semaphore_wait(barrier, 7)

    def aligned(value, size):
        return pl.ds(pl.multiple_of(value, size), size)

    near_src = aligned(2 * half - half * odd, half)
    near_dst = aligned(3 * half * odd, half)
    far_src = aligned(half + half * odd, half)
    far_dst = aligned(3 * half * (1 - odd), half)
    near_copy = remote(kv.at[near_src], kv.at[near_dst], hs.at[0], hr.at[0], n_dev)
    far_copy = remote(kv.at[far_src], kv.at[far_dst], hs.at[1], hr.at[1], f_dev)
    loads[0].wait()
    loads[1].wait()

    @pl.when(has_far)
    def _():
        far_copy.start()

    near_copy.start()
    copies = []

    def go(*args):
        copy = remote(*args)
        copy.start()
        copies.append(copy)
        return copy

    own, model = res.shape
    width = w.shape[1]
    loads[4].wait()
    res_copies = [
        go(
            res.at[:, aligned(owner * width, width)],
            res_in.at[t],
            as_.at[k],
            ar.at[k],
            device,
        )
        for k, (owner, device) in enumerate(((tx, x_dev), (ty, y_dev), (td, d_dev)))
    ]
    res_in[t] = res[:, aligned(t * width, width)]
    count, lanes = meta.shape[0] // 2, meta.shape[1]
    tokens = lanes // 4
    expert = lax.broadcasted_iota(jnp.int32, (count, lanes), 0)
    lane = lax.broadcasted_iota(jnp.int32, (count, lanes), 1)
    mine_lane = jnp.logical_and(lane >= t * tokens, lane < (t + 1) * tokens)
    routes = jnp.concatenate([routes_ref[...]] * 4, axis=1)
    route_weights = jnp.concatenate([route_weights_ref[...]] * 4, axis=1)
    hit_one = routes[0:1, :] == expert
    hit = jnp.logical_and(mine_lane, jnp.logical_or(hit_one, routes[1:2, :] == expert))
    chosen = jnp.where(hit, 1.0, 0.0)
    before = lax.broadcasted_iota(jnp.int32, (lanes, lanes), 0) <= lax.broadcasted_iota(
        jnp.int32, (lanes, lanes), 1
    )
    rank = jnp.dot(
        chosen.astype(jnp.bfloat16),
        jnp.where(before, 1.0, 0.0).astype(jnp.bfloat16),
        preferred_element_type=jnp.float32,
    )
    meta[0:count] = chosen * rank
    meta[count : 2 * count] = chosen * jnp.where(
        hit_one, route_weights[0:1, :], route_weights[1:2, :]
    )
    meta_copies = [
        go(meta, meta_in.at[t], ms.at[k], mr.at[k], device)
        for k, device in enumerate((x_dev, y_dev, d_dev))
    ]

    for copy in loads[5:]:
        copy.start()

    @pl.when(jnp.logical_not(has_far))
    def _():
        kv[aligned(3 * half * odd, half)] = jnp.zeros((half, kv.shape[1]), kv.dtype)

    loads[2].wait()
    span = 3 * half
    query = lax.broadcasted_iota(jnp.int32, (2 * half, span), 0)
    query = jnp.where(query >= half, query - half, query)
    key = lax.broadcasted_iota(jnp.int32, (2 * half, span), 1)
    band = jnp.abs(query + half - key) <= WINDOW
    upper = lax.broadcasted_iota(jnp.int32, (2 * half, 1), 0) < half

    def attend(b):
        valid = jnp.logical_and(
            band,
            jnp.logical_and(
                key >= jnp.where(2 * s + b == 0, half, 0),
                key < jnp.where(2 * s + b == 2 * last + 1, 2 * half, span),
            ),
        )
        keys_at = pl.ds(pl.multiple_of(b * half, half), span)
        mine = aligned(b * half, half)
        for g in range(groups):
            pair = q[mine, 2 * g * HEAD : 2 * (g + 1) * HEAD]
            stacked = jnp.concatenate([pair[:, :HEAD], pair[:, HEAD:]], axis=0)
            scores = lax.dot_general(
                stacked,
                kv[keys_at, g * HEAD : (g + 1) * HEAD],
                (((1,), (1,)), ((), ())),
                preferred_element_type=jnp.float32,
            ) * HEAD ** (-0.5)
            sink = jnp.where(upper, sink_ref[2 * g], sink_ref[2 * g + 1])
            masked = jnp.where(valid, scores, NEGATIVE)
            top = jnp.maximum(jnp.max(masked, axis=-1, keepdims=True), sink)
            probs = jnp.exp(masked - top)
            denom = jnp.sum(probs, axis=-1, keepdims=True) + jnp.exp(sink - top)
            weights = (probs * (1.0 / denom)).astype(jnp.bfloat16)
            output = jnp.dot(
                weights,
                kv[keys_at, kept + g * HEAD : kept + (g + 1) * HEAD],
                preferred_element_type=jnp.float32,
            )
            joined = jnp.concatenate([output[:half], output[half:]], axis=1)
            buf[t, mine, 2 * g * HEAD : 2 * (g + 1) * HEAD] = joined.astype(buf.dtype)

    blocks = (1 - odd, odd)
    parts_of = [aligned(b * half, half) for b in blocks]

    def spread(h, k):
        piece = buf.at[t, parts_of[h]]
        return (
            go(piece, piece, gs.at[k], gr.at[k], x_dev),
            go(piece, piece, gs.at[k + 1], gr.at[k + 1], y_dev),
        )

    near_copy.wait_recv()
    attend(blocks[0])
    x_one, y_one = spread(0, 0)

    @pl.when(has_far)
    def _():
        far_copy.wait_recv()

    attend(blocks[1])
    x_two, y_two = spread(1, 2)
    for copy in meta_copies:
        copy.wait_recv()
    meta_z[z] = (meta[...] + meta_in[tx]) + (meta_in[ty] + meta_in[td])
    meta_z_copies = [
        go(meta_z.at[z], meta_z.at[z], ms.at[2 + m], mr.at[2 + m], z_devs[m]) for m in (1, 2, 3)
    ]
    loads[3].wait()
    for copy in res_copies:
        copy.wait_recv()

    def product(h, owner):
        weight = w[pl.ds(pl.multiple_of(owner * depth, depth), depth)]
        return jnp.dot(buf[owner, parts_of[h]], weight, preferred_element_type=jnp.float32)

    x_one.wait_recv()
    piece = buf.at[tx, parts_of[0]]
    d_one = go(piece, piece, gs.at[4], gr.at[4], y_dev)
    acc[0] = product(0, t)
    acc[0] += product(0, tx)
    y_one.wait_recv()
    acc[0] += product(0, ty)
    y_two.wait_recv()
    piece = buf.at[ty, parts_of[1]]
    d_two = go(piece, piece, gs.at[5], gr.at[5], x_dev)
    acc[1] = product(1, t)
    acc[1] += product(1, ty)
    gain = gain_ref[:, aligned(t * width, width)]

    def finish(h):
        projected = (acc[h] + product(h, td)).astype(proj.dtype)
        proj[parts_of[h]] = projected
        pair = res_in[pl.ds(2 * blocks[h], 2)].reshape(half, width)
        value = pair.astype(jnp.float32) + projected.astype(jnp.float32)
        tok[t, z, parts_of[h]] = (value * gain).astype(tok.dtype)
        return jnp.sum(value * value, axis=-1, keepdims=True)

    def record(h, sums):
        squares[blocks[h]] = jnp.broadcast_to(sums, (half, half)).T[: squares.shape[1]]

    def own_block(h):
        return tok.at[t, z, parts_of[h]]

    z_in = {
        (m, h): remote(
            own_block(h), tok.at[t, planes[m], parts_of[h]], zs.at[m, h], zr.at[m, h], z_devs[m]
        )
        for m in (1, 2, 3)
        for h in (0, 1)
    }

    out_one = [remote(own_block(h), own_block(h), zs.at[1, h], zr.at[1, h], z_devs[1]) for h in (0, 1)]
    out_three = [remote(own_block(h), own_block(h), zs.at[3, h], zr.at[3, h], z_devs[3]) for h in (0, 1)]

    def relay_copy(m, h):
        piece = tok.at[t, planes[m], parts_of[h]]
        lands, device = ((2, z_devs[3]), None, (3, z_devs[1]), (2, z_devs[1]))[
            {1: 0, 2: 2, 3: 3}[m]
        ]
        return remote(piece, piece, zs.at[3 + m, h], zr.at[lands, h], device)

    def depart(h):
        out_one[h].start()

        @pl.when(inner)
        def _():
            out_three[h].start()

    sent, forwarded, picks, parts, firsts, seconds, homes = {}, {}, {}, {}, {}, {}, {}

    def arrive(m, h):
        z_in[m, h].wait_recv()

    def relay(m, h, waited=True):
        @pl.when(inner)
        def _():
            if not waited:
                arrive(m, h)
            relay_copy(m, h).start()

    def send(m, h):
        piece = tok.at[t, planes[m], parts_of[h]]
        sent[m, h] = (
            go(piece, piece, ds_.at[m, 2 * h], dr.at[m, 2 * h], x_dev),
            go(piece, piece, ds_.at[m, 2 * h + 1], dr.at[m, 2 * h + 1], y_dev),
        )

    def forward(m, h):
        sent[m, h][0].wait_recv()
        piece = tok.at[tx, planes[m], aligned(blocks[h] * half, half // 2)]
        first = go(piece, piece, ds_.at[m, 4 + 2 * h], dr.at[m, 4 + 2 * h], y_dev)
        sent[m, h][1].wait_recv()
        piece = tok.at[ty, planes[m], aligned(blocks[h] * half + half // 2, half // 2)]
        second = go(piece, piece, ds_.at[m, 5 + 2 * h], dr.at[m, 5 + 2 * h], x_dev)
        forwarded[m, h] = (first, second)

    slots = xo.shape[1]
    capacity = slots // 4
    step = 256
    row = lax.broadcasted_iota(jnp.int32, (slots, lanes), 0).astype(jnp.float32)
    shift = (lax.broadcasted_iota(jnp.int32, (1, lanes), 1) // tokens * capacity).astype(
        jnp.float32
    )

    def place(source, m, which):
        ranks = source[planes[m], pl.ds(which, 1), :]
        target = jnp.where(ranks > 0.5, ranks + (shift - 1.0), -1.0)
        return row == target

    def scale(source, m, which):
        weights = source[planes[m], pl.ds(count + which, 1), :]
        return jnp.sum(
            jnp.where(place(source, m, which), weights, 0.0), axis=1, keepdims=True
        )

    def picking(m):
        return jnp.concatenate(
            [jnp.where(place(meta_z, m, which), 1.0, 0.0) for which in (s, near)], axis=0
        )

    def complete(m):
        for h in (0, 1):
            for copy in forwarded[m, h]:
                copy.wait_recv()

    def pick(m):
        chooser = picking(m)
        lengths = inverse[planes[m]]
        lengths = jnp.concatenate([lengths[0, 0:1], lengths[1, 0:1]], axis=1)
        factor = jnp.sum(chooser * lengths, axis=1, keepdims=True)
        chooser = chooser.astype(jnp.bfloat16)
        for owner in range(4):
            for k in range(width // step):
                rows_in = tok[owner, planes[m], :, k * step : (k + 1) * step]
                found = jnp.dot(chooser, rows_in, preferred_element_type=jnp.float32)
                found = (found * factor).astype(xs.dtype)
                columns = slice(owner * width + k * step, owner * width + (k + 1) * step)
                xs[m, 0:slots, columns] = found[:slots]
                xo[m, :, columns] = found[slots:]
        picks[m] = go(
            xo.at[m], xs.at[m, pl.ds(slots, slots)], xs_s.at[m], xs_r.at[m], n_dev
        )

    def rise(m, begin, end):
        @pl.loop(begin, end)
        def _(k):
            columns = pl.ds(pl.multiple_of(k * step, step), step)
            x = xs[m]
            g = jnp.dot(x, gate[:, columns], preferred_element_type=jnp.float32)
            u = jnp.dot(x, up[:, columns], preferred_element_type=jnp.float32)
            hidden[:, columns] = (jax.nn.silu(g) * u).astype(hidden.dtype)

    total_steps = gate.shape[1] // step
    first_steps = (total_steps + 1) // 2

    def fall(m):
        factor_mine = scale(meta_z, m, s)
        factor_near = scale(meta_p, m, s)
        wide = 512

        @pl.loop(0, model // wide)
        def _(k):
            columns = pl.ds(pl.multiple_of(k * wide, wide), wide)
            share = jnp.dot(hidden[...], down[:, columns], preferred_element_type=jnp.float32)
            po[m, 0:slots, columns] = (share[:slots] * factor_mine).astype(po.dtype)
            ps[m, :, columns] = (share[slots:] * factor_near).astype(ps.dtype)

        parts[m] = go(
            ps.at[m], po.at[m, pl.ds(slots, slots)], ps_s.at[m], ps_r.at[m], n_dev
        )

    def expand(m):
        parts[m].wait_recv()
        spreader = picking(m).T.astype(jnp.bfloat16)
        for owner in range(4):
            holds = jnp.where(t == owner, 1.0, 0.0)
            for k in range(width // step):
                columns = slice(owner * width + k * step, owner * width + (k + 1) * step)
                found = jnp.dot(spreader, po[m, :, columns], preferred_element_type=jnp.float32)
                if m == 0:
                    found += holds * proj[:, k * step : (k + 1) * step].astype(jnp.float32)
                rt[m, :, :, columns] = found.astype(rt.dtype).reshape(4, tokens, step)

    low, high = pl.ds(0, own // 2), pl.ds(own // 2, own // 2)

    def reduce_one(m):
        firsts[m] = (
            go(rt.at[m, td, low], bx1.at[m, 1], rs.at[m, 0], rr.at[m, 0], x_dev),
            go(rt.at[m, td, high], by1.at[m, 1], rs.at[m, 1], rr.at[m, 1], y_dev),
            go(rt.at[m, tx, low], bx1.at[m, 0], rs.at[m, 2], rr.at[m, 2], x_dev),
            go(rt.at[m, ty, high], by1.at[m, 0], rs.at[m, 3], rr.at[m, 3], y_dev),
        )

    def wide_sum(*pieces):
        result = pieces[0].astype(jnp.float32)
        for piece in pieces[1:]:
            result = result + piece.astype(jnp.float32)
        return result

    def reduce_two(m):
        firsts[m][0].wait_recv()
        mid[m, 0] = wide_sum(rt[m, ty, low], bx1[m, 1]).astype(mid.dtype)
        to_side = go(mid.at[m, 0], by2.at[m], rs.at[m, 4], rr.at[m, 4], y_dev)
        firsts[m][1].wait_recv()
        mid[m, 1] = wide_sum(rt[m, tx, high], by1[m, 1]).astype(mid.dtype)
        seconds[m] = (
            to_side,
            go(mid.at[m, 1], bx2.at[m], rs.at[m, 5], rr.at[m, 5], x_dev),
        )

    def reduce_three(m):
        firsts[m][2].wait_recv()
        seconds[m][0].wait_recv()
        lower = wide_sum(rt[m, t, low], bx1[m, 0], by2[m])
        if m:
            sz[m, low] = lower.astype(sz.dtype)
            lower_home = go(sz.at[m, low], zin.at[m, low], zbs.at[m, 0], zbr.at[m, 0], z_devs[m])
        else:
            home_sum[low] = lower
        firsts[m][3].wait_recv()
        seconds[m][1].wait_recv()
        upper = wide_sum(rt[m, t, high], by1[m, 0], bx2[m])
        if m:
            sz[m, high] = upper.astype(sz.dtype)
            homes[m] = (
                lower_home,
                go(sz.at[m, high], zin.at[m, high], zbs.at[m, 1], zbr.at[m, 1], z_devs[m]),
            )
        else:
            home_sum[high] = upper

    def share_squares():
        return [
            go(squares, squares_in.at[t], qs.at[k], qr.at[k], device)
            for k, device in enumerate((x_dev, y_dev, d_dev))
        ]

    def invert(square_copies):
        for copy in square_copies:
            copy.wait_recv()
        total = (squares[...] + squares_in[tx]) + (squares_in[ty] + squares_in[td])
        inverse[z] = lax.rsqrt(total * (1.0 / model) + EPS)
        return {
            m: go(inverse.at[z], inverse.at[z], qs.at[2 + m], qr.at[2 + m], z_devs[m])
            for m in (1, 2, 3)
        }

    d_one.wait_recv()
    sums = finish(0)
    send(0, 0)
    depart(0)
    record(0, sums)
    x_two.wait_recv()
    acc[1] += product(1, tx)
    d_two.wait_recv()
    sums = finish(1)
    send(0, 1)
    depart(1)
    record(1, sums)
    square_copies = share_squares()
    for copy in meta_z_copies:
        copy.wait_recv()
    meta_near = go(meta_z, meta_p, ms.at[6], mr.at[6], n_dev)
    forward(0, 0)
    arrive(1, 0)
    relay(1, 0)
    forward(0, 1)
    arrive(1, 1)
    relay(1, 1)
    relay(3, 0, False)
    relay(3, 1, False)
    send(1, 0)
    send(1, 1)
    inverse_copies = invert(square_copies)
    complete(0)
    pick(0)
    arrive(2, 0)
    relay(2, 0)
    send(2, 0)
    picks[0].wait_recv()
    for copy in loads[5:]:
        copy.wait()
    rise(0, 0, first_steps)
    arrive(2, 1)
    relay(2, 1)
    send(2, 1)
    rise(0, first_steps, total_steps)
    meta_near.wait_recv()
    fall(0)
    forward(2, 0)
    expand(0)
    forward(2, 1)

    @pl.when(outer)
    def _():
        arrive(3, 0)

    send(3, 0)

    @pl.when(outer)
    def _():
        arrive(3, 1)

    send(3, 1)
    complete(2)
    inverse_copies[2].wait_recv()
    pick(2)
    forward(3, 0)
    picks[2].wait_recv()
    rise(2, 0, first_steps)
    forward(3, 1)
    forward(1, 0)
    forward(1, 1)
    rise(2, first_steps, total_steps)
    fall(2)
    complete(3)
    inverse_copies[3].wait_recv()
    pick(3)
    expand(2)
    reduce_one(2)
    complete(1)
    inverse_copies[1].wait_recv()
    pick(1)
    picks[3].wait_recv()
    rise(3, 0, first_steps)
    rise(3, first_steps, total_steps)
    reduce_two(2)
    fall(3)
    picks[1].wait_recv()
    rise(1, 0, first_steps)
    expand(3)
    reduce_one(3)
    rise(1, first_steps, total_steps)
    reduce_three(2)
    fall(1)
    reduce_two(3)
    expand(1)
    reduce_one(1)
    reduce_three(3)
    reduce_two(1)
    reduce_one(0)
    reduce_three(1)
    reduce_two(0)
    reduce_three(0)
    for m in (2, 3, 1):
        homes[m][0].wait_recv()
        homes[m][1].wait_recv()
    out_ref[...] = (
        res[...].astype(jnp.float32) + (home_sum[...] + wide_sum(zin[1], zin[2], zin[3]))
    ).astype(out_ref.dtype)
    for copy in copies:
        copy.wait_send()
    near_copy.wait_send()
    for h in (0, 1):
        out_one[h].wait_send()

    @pl.when(inner)
    def _():
        for h in (0, 1):
            out_three[h].wait_send()
            for m in (1, 2, 3):
                relay_copy(m, h).wait_send()

    @pl.when(has_far)
    def _():
        far_copy.wait_send()


def layer(
    queries, keys, values, sink_logit, out_weight, residual, norm_gain, routes, route_weights,
    gate_weight, up_weight, down_weight, capacity,
):
    rows, depth = queries.shape
    kind = queries.dtype
    width = out_weight.shape[1]
    tokens, model = residual.shape
    count = lax.axis_size("sp")
    slots = 4 * capacity
    anywhere = pl.BlockSpec(memory_space=pl.ANY)
    vmem = pl.BlockSpec(memory_space=pltpu.VMEM)
    dma = pltpu.SemaphoreType.DMA
    one, six = dma((4,)), dma((4, 6))
    lanes = 4 * tokens
    return pl.pallas_call(
        layer_kernel,
        out_shape=jax.ShapeDtypeStruct(residual.shape, kind),
        in_specs=[anywhere] * 3
        + [pl.BlockSpec(memory_space=pltpu.SMEM), anywhere, anywhere, vmem, vmem, vmem]
        + [anywhere] * 3,
        out_specs=vmem,
        scratch_shapes=[
            pltpu.VMEM(queries.shape, kind),
            pltpu.VMEM((2 * rows, 2 * keys.shape[1]), kind),
            pltpu.VMEM(out_weight.shape, kind),
            pltpu.VMEM(residual.shape, kind),
            pltpu.VMEM((4, tokens, width), kind),
            pltpu.VMEM((4, rows, depth), kind),
            pltpu.VMEM((2, rows // 2, width), jnp.float32),
            pltpu.VMEM((rows, width), kind),
            pltpu.VMEM(gate_weight.shape, kind),
            pltpu.VMEM(up_weight.shape, kind),
            pltpu.VMEM(down_weight.shape, kind),
            pltpu.VMEM((2 * count, lanes), jnp.float32),
            pltpu.VMEM((4, 2 * count, lanes), jnp.float32),
            pltpu.VMEM((4, 2 * count, lanes), jnp.float32),
            pltpu.VMEM((4, 2 * count, lanes), jnp.float32),
            pltpu.VMEM((2, 8, rows // 2), jnp.float32),
            pltpu.VMEM((4, 2, 8, rows // 2), jnp.float32),
            pltpu.VMEM((4, 2, 8, rows // 2), jnp.float32),
            pltpu.VMEM((4, 4, rows, width), kind),
            pltpu.VMEM((4, 2 * slots, model), kind),
            pltpu.VMEM((4, slots, model), kind),
            pltpu.VMEM((2 * slots, gate_weight.shape[1]), kind),
            pltpu.VMEM((4, 2 * slots, model), kind),
            pltpu.VMEM((4, slots, model), kind),
            pltpu.VMEM((4, 4, tokens, model), kind),
            pltpu.VMEM((4, 2, tokens // 2, model), kind),
            pltpu.VMEM((4, 2, tokens // 2, model), kind),
            pltpu.VMEM((4, tokens // 2, model), kind),
            pltpu.VMEM((4, tokens // 2, model), kind),
            pltpu.VMEM((4, 2, tokens // 2, model), kind),
            pltpu.VMEM((4, tokens, model), kind),
            pltpu.VMEM((4, tokens, model), kind),
            pltpu.VMEM(residual.shape, jnp.float32),
            dma((8,)),
            dma((2,)), dma((2,)),
            dma((6,)), dma((6,)),
            dma((3,)), dma((3,)),
            dma((7,)), dma((7,)),
            dma((6,)), dma((6,)),
            dma((7, 2)), dma((4, 2)),
            dma((4, 8)), dma((4, 8)), one, one, one, one, six, six,
            dma((4, 2)), dma((4, 2)),
        ],
        compiler_params=pltpu.CompilerParams(
            collective_id=0, has_side_effects=True, vmem_limit_bytes=60 * 1024 * 1024
        ),
    )(
        queries, keys, values, sink_logit, out_weight, residual, norm_gain.reshape(1, -1),
        routes.T, route_weights.T,
        gate_weight, up_weight, down_weight,
    )


def with_halo(block, sides, width):
    for axis, dim in sides:
        count = lax.axis_size(axis)
        forward = [(i, i + 1) for i in range(count - 1)]
        backward = [(target, source) for source, target in forward]
        low = lax.ppermute(
            lax.slice_in_dim(block, block.shape[dim] - width, None, axis=dim), axis, forward
        )
        high = lax.ppermute(lax.slice_in_dim(block, 0, width, axis=dim), axis, backward)
        block = jnp.concatenate([low, block, high], axis=dim)
    return block


def make_band(extended, length):
    blocks = length // WINDOW
    pieces = [
        lax.slice_in_dim(extended, offset * WINDOW, offset * WINDOW + length, axis=0).reshape(
            blocks, WINDOW, -1
        )
        for offset in range(3)
    ]
    return jnp.concatenate(pieces, axis=1)


def attend_local(queries, keys, values, sink_logit):
    length = queries.shape[0]
    groups = keys.shape[1] // HEAD
    repeat = HEADS // KV_HEADS
    blocks = length // WINDOW
    joined = jnp.concatenate([keys, values], axis=1)
    extended = with_halo(joined, (("sp", 0),), WINDOW)
    banded = make_band(extended, length)
    key_band = banded[..., : groups * HEAD].reshape(blocks, 3 * WINDOW, groups, HEAD)
    value_band = banded[..., groups * HEAD :].reshape(blocks, 3 * WINDOW, groups, HEAD)
    query_blocks = queries.reshape(blocks, WINDOW, groups, repeat, HEAD)
    scores = jnp.einsum(
        "nqgrd,nkgd->ngrqk", query_blocks, key_band, preferred_element_type=jnp.float32
    ) * HEAD ** (-0.5)
    near = jnp.abs(jnp.arange(WINDOW)[:, None] + WINDOW - jnp.arange(3 * WINDOW)[None, :]) <= WINDOW
    first_token = lax.axis_index("sp") * length
    key_pos = (
        first_token + (jnp.arange(blocks)[:, None] - 1) * WINDOW + jnp.arange(3 * WINDOW)[None, :]
    )
    inside = (key_pos >= 0) & (key_pos < length * lax.axis_size("sp"))
    valid = near[None, None, None, :, :] & inside[:, None, None, None, :]
    sinks = sink_logit.reshape(1, groups, repeat, 1, 1)
    masked = jnp.where(valid, scores, NEGATIVE)
    top = jnp.maximum(jnp.max(masked, axis=-1, keepdims=True), sinks)
    probs = jnp.exp(masked - top)
    denom = jnp.sum(probs, axis=-1, keepdims=True) + jnp.exp(sinks - top)
    weights = (probs / denom).astype(jnp.bfloat16)
    output = jnp.einsum(
        "ngrqk,nkgd->nqgrd", weights, value_band, preferred_element_type=jnp.float32
    )
    return output.astype(jnp.bfloat16).reshape(length, groups * repeat * HEAD)


def local(
    queries,
    keys,
    values,
    sink_logit,
    out_weight,
    residual,
    norm_gain,
    routes,
    route_weights,
    gate_weight,
    up_weight,
    down_weight,
):
    capacity = max(2, 4 * residual.shape[0] // lax.axis_size("sp"))
    in_plane = (
        lax.axis_size("tp") == 4
        and lax.axis_size("sp") == 8
        and capacity % 32 == 0
        and gate_weight.shape[2] % 256 == 0
        and queries.shape[0] == 2 * WINDOW
        and residual.shape[0] == 64
    )
    if in_plane:
        return layer(
            queries, keys, values, sink_logit, out_weight, residual, norm_gain, routes,
            route_weights, gate_weight[0], up_weight[0], down_weight[0], capacity,
        )
    attention = attend_local(queries, keys, values, sink_logit)
    columns = jnp.dot(
        lax.all_gather(attention, "tp", axis=1, tiled=True),
        out_weight,
        preferred_element_type=jnp.float32,
    )
    projected = lax.all_to_all(
        columns.astype(jnp.bfloat16), "tp", split_axis=0, concat_axis=1, tiled=True
    )
    hidden_state = residual.astype(jnp.float32) + projected.astype(jnp.float32)
    inverse = lax.rsqrt(jnp.mean(hidden_state * hidden_state, axis=-1, keepdims=True) + EPS)
    normed = (hidden_state * inverse * norm_gain).astype(jnp.bfloat16)
    sp_count = lax.axis_size("sp")
    tok_rows = residual.shape[0]
    width = residual.shape[1]
    slot_total = sp_count * capacity
    expert_ids = routes.reshape(-1)
    onehot = (expert_ids[:, None] == jnp.arange(sp_count, dtype=jnp.int32)[None, :]).astype(
        jnp.int32
    )
    earlier = jnp.cumsum(onehot, axis=0) - onehot
    rank = jnp.sum(earlier * onehot, axis=1)
    slots = expert_ids * capacity + rank
    placing = (slots[:, None] == jnp.arange(slot_total, dtype=jnp.int32)[None, :]).astype(
        jnp.bfloat16
    )
    placing = placing.reshape(tok_rows, 2, slot_total)
    first_place = placing[:, 0]
    second_place = placing[:, 1]
    sending = jnp.einsum(
        "ts,td->sd", first_place + second_place, normed, preferred_element_type=jnp.float32
    )
    sending = sending.astype(jnp.bfloat16).reshape(sp_count, capacity, width)
    piece = lax.all_gather(
        lax.all_to_all(sending, "sp", split_axis=0, concat_axis=0, tiled=True),
        "tp",
        axis=0,
        tiled=True,
    )
    flat = piece.reshape(-1, piece.shape[-1])
    gate = jnp.dot(flat, gate_weight[0], preferred_element_type=jnp.float32)
    upward = jnp.dot(flat, up_weight[0], preferred_element_type=jnp.float32)
    hidden = (jax.nn.silu(gate) * upward).astype(jnp.bfloat16)
    partial_value = jnp.dot(hidden, down_weight[0], preferred_element_type=jnp.float32)
    partial_value = partial_value.reshape(piece.shape[:-1] + (down_weight.shape[-1],))
    returned = lax.all_to_all(
        lax.psum_scatter(
            partial_value.astype(jnp.bfloat16), "tp", scatter_dimension=0, tiled=True
        ),
        "sp",
        split_axis=0,
        concat_axis=0,
        tiled=True,
    )
    gathered_back = returned.reshape(slot_total, width)
    first_pick = jnp.dot(first_place, gathered_back, preferred_element_type=jnp.float32)
    second_pick = jnp.dot(second_place, gathered_back, preferred_element_type=jnp.float32)
    mixture = route_weights[:, 0:1] * first_pick + route_weights[:, 1:2] * second_pick
    return (hidden_state + mixture).astype(jnp.bfloat16)


def solution(mesh):
    in_specs = (
        P("sp", "tp"),
        P("sp", "tp"),
        P("sp", "tp"),
        P("tp"),
        P(None, "tp"),
        P(("sp", "tp"), None),
        P(),
        P(("sp", "tp"), None),
        P(("sp", "tp"), None),
        P("sp", None, "tp"),
        P("sp", None, "tp"),
        P("sp", "tp", None),
    )
    out_specs = P(("sp", "tp"), None)
    return jax.shard_map(local, mesh=mesh, in_specs=in_specs, out_specs=out_specs, check_vma=False)
```

```python
import functools

import jax
import jax.numpy as jnp
from jax import lax
from jax.experimental import pallas as pl
from jax.experimental.pallas import tpu as pltpu
from jax.sharding import PartitionSpec as P

HEADS = 32
KV_HEADS = 16
HEAD = 64
WINDOW = 128


EPS = 1e-06
NEGATIVE = -1e30
MESH = pl.DeviceIdType.MESH


def plane():
    t = lax.axis_index("tp")
    tx = t + 1 - 2 * lax.rem(t, 2)
    ty = lax.rem(t + 2, 4)
    return t, tx, ty, 3 - t


def remote(src, dst, send, recv, device):
    return pltpu.make_async_remote_copy(
        src_ref=src,
        dst_ref=dst,
        send_sem=send,
        recv_sem=recv,
        device_id=device,
        device_id_type=MESH,
    )


def flipped(index, mask):
    result = index
    bit = 1
    while bit <= mask:
        if mask & bit:
            result = result + bit * (1 - 2 * lax.rem(index // bit, 2))
        bit *= 2
    return result


def layer_kernel(
    q_hbm, k_hbm, v_hbm, sink_ref, w_hbm, res_hbm, gain_ref, routes_ref, route_weights_ref,
    gate_hbm, up_hbm, down_hbm, out_ref,
    q, kv, w, res, res_in, buf, acc, proj, gate, up, down,
    meta, meta_in, meta_z, meta_p, squares, squares_in, inverse, tok, xs, xo, hidden, po, ps, rt,
    bx1, by1, bx2, by2, mid, sz, zin, home_sum,
    load, hs, hr, gs, gr, as_, ar, ms, mr, qs, qr, zs, zr, ds_, dr, xs_s, xs_r, ps_s, ps_r,
    rs, rr, zbs, zbr, hos, hor,
):
    s = lax.axis_index("sp")
    t, tx, ty, td = plane()
    last = lax.axis_size("sp") - 1
    rows, depth = q.shape
    half = rows // 2
    groups = k_hbm.shape[1] // HEAD
    kept = groups * HEAD
    odd = lax.rem(s, 2)
    near = s + 1 - 2 * odd
    has_far = jnp.logical_and(s != 0, s != last)
    far = jnp.where(has_far, s - 1 + 2 * odd, near)
    x_dev, y_dev, d_dev, n_dev, f_dev = (s, tx), (s, ty), (s, td), (near, t), (far, t)
    z = s // 2
    planes = [flipped(z, m) for m in range(4)]
    z_devs = [(2 * planes[m] + odd, t) for m in range(4)]
    inner = jnp.logical_or(z == 1, z == 2)
    outer = jnp.logical_not(inner)
    middle = pl.ds(half, rows)
    loads = [
        pltpu.make_async_copy(source, target, load.at[k])
        for k, (source, target) in enumerate(
            (
                (k_hbm, kv.at[middle, pl.ds(0, kept)]),
                (v_hbm, kv.at[middle, pl.ds(kept, kept)]),
                (q_hbm, q),
                (w_hbm, w),
                (res_hbm, res),
                (gate_hbm, gate),
                (up_hbm, up),
                (down_hbm, down),
            )
        )
    ]
    for copy in loads[:5]:
        copy.start()
    barrier = pltpu.get_barrier_semaphore()
    for device in [x_dev, y_dev, d_dev, n_dev] + z_devs[1:]:
        pl.semaphore_signal(barrier, inc=1, device_id=device, device_id_type=MESH)

    @pl.when(has_far)
    def _():
        pl.semaphore_signal(barrier, inc=1, device_id=f_dev, device_id_type=MESH)
        pl.semaphore_wait(barrier, 8)

    @pl.when(jnp.logical_not(has_far))
    def _():
        pl.semaphore_wait(barrier, 7)

    def aligned(value, size):
        return pl.ds(pl.multiple_of(value, size), size)

    near_src = aligned(2 * half - half * odd, half)
    near_dst = aligned(3 * half * odd, half)
    far_src = aligned(half + half * odd, half)
    far_dst = aligned(3 * half * (1 - odd), half)
    near_copy = remote(kv.at[near_src], kv.at[near_dst], hs.at[0], hr.at[0], n_dev)
    far_copy = remote(kv.at[far_src], kv.at[far_dst], hs.at[1], hr.at[1], f_dev)
    loads[0].wait()
    loads[1].wait()

    @pl.when(has_far)
    def _():
        far_copy.start()

    near_copy.start()
    copies = []

    def go(*args):
        copy = remote(*args)
        copy.start()
        copies.append(copy)
        return copy

    own, model = res.shape
    width = w.shape[1]
    loads[4].wait()
    res_copies = [
        go(
            res.at[:, aligned(owner * width, width)],
            res_in.at[t],
            as_.at[k],
            ar.at[k],
            device,
        )
        for k, (owner, device) in enumerate(((tx, x_dev), (ty, y_dev), (td, d_dev)))
    ]
    res_in[t] = res[:, aligned(t * width, width)]
    count, lanes = meta.shape[0] // 2, meta.shape[1]
    tokens = lanes // 4
    expert = lax.broadcasted_iota(jnp.int32, (count, lanes), 0)
    lane = lax.broadcasted_iota(jnp.int32, (count, lanes), 1)
    mine_lane = jnp.logical_and(lane >= t * tokens, lane < (t + 1) * tokens)
    routes = jnp.concatenate([routes_ref[...]] * 4, axis=1)
    route_weights = jnp.concatenate([route_weights_ref[...]] * 4, axis=1)
    hit_one = routes[0:1, :] == expert
    hit = jnp.logical_and(mine_lane, jnp.logical_or(hit_one, routes[1:2, :] == expert))
    chosen = jnp.where(hit, 1.0, 0.0)
    before = lax.broadcasted_iota(jnp.int32, (lanes, lanes), 0) <= lax.broadcasted_iota(
        jnp.int32, (lanes, lanes), 1
    )
    rank = jnp.dot(
        chosen.astype(jnp.bfloat16),
        jnp.where(before, 1.0, 0.0).astype(jnp.bfloat16),
        preferred_element_type=jnp.float32,
    )
    meta[0:count] = chosen * rank
    meta[count : 2 * count] = chosen * jnp.where(
        hit_one, route_weights[0:1, :], route_weights[1:2, :]
    )
    meta_copies = [
        go(meta, meta_in.at[t], ms.at[k], mr.at[k], device)
        for k, device in enumerate((x_dev, y_dev, d_dev))
    ]

    for copy in loads[5:]:
        copy.start()

    @pl.when(jnp.logical_not(has_far))
    def _():
        kv[aligned(3 * half * odd, half)] = jnp.zeros((half, kv.shape[1]), kv.dtype)

    loads[2].wait()
    span = 3 * half
    query = lax.broadcasted_iota(jnp.int32, (2 * half, span), 0)
    query = jnp.where(query >= half, query - half, query)
    key = lax.broadcasted_iota(jnp.int32, (2 * half, span), 1)
    band = jnp.abs(query + half - key) <= WINDOW
    upper = lax.broadcasted_iota(jnp.int32, (2 * half, 1), 0) < half

    def attend(b, first, end):
        valid = jnp.logical_and(
            band,
            jnp.logical_and(
                key >= jnp.where(2 * s + b == 0, half, 0),
                key < jnp.where(2 * s + b == 2 * last + 1, 2 * half, span),
            ),
        )
        keys_at = pl.ds(pl.multiple_of(b * half, half), span)
        mine = aligned(b * half, half)
        for g in range(first, end):
            pair = q[mine, 2 * g * HEAD : 2 * (g + 1) * HEAD]
            stacked = jnp.concatenate([pair[:, :HEAD], pair[:, HEAD:]], axis=0)
            scores = lax.dot_general(
                stacked,
                kv[keys_at, g * HEAD : (g + 1) * HEAD],
                (((1,), (1,)), ((), ())),
                preferred_element_type=jnp.float32,
            ) * HEAD ** (-0.5)
            sink = jnp.where(upper, sink_ref[2 * g], sink_ref[2 * g + 1])
            masked = jnp.where(valid, scores, NEGATIVE)
            top = jnp.maximum(jnp.max(masked, axis=-1, keepdims=True), sink)
            probs = jnp.exp(masked - top)
            denom = jnp.sum(probs, axis=-1, keepdims=True) + jnp.exp(sink - top)
            weights = (probs * (1.0 / denom)).astype(jnp.bfloat16)
            output = jnp.dot(
                weights,
                kv[keys_at, kept + g * HEAD : kept + (g + 1) * HEAD],
                preferred_element_type=jnp.float32,
            )
            joined = jnp.concatenate([output[:half], output[half:]], axis=1)
            buf[t, mine, 2 * g * HEAD : 2 * (g + 1) * HEAD] = joined.astype(buf.dtype)

    blocks = (1 - odd, odd)
    parts_of = [aligned(b * half, half) for b in blocks]

    wide_piece = depth // 2

    def part(owner, h, j):
        return buf.at[owner, parts_of[h], pl.ds(j * wide_piece, wide_piece)]

    spreads, passes = {}, {}

    def spread(h, j):
        piece = part(t, h, j)
        k = 4 * h + 2 * j
        spreads[h, j] = (
            go(piece, piece, gs.at[k], gr.at[k], x_dev),
            go(piece, piece, gs.at[k + 1], gr.at[k + 1], y_dev),
        )

    def hand_on(h, j):
        spreads[h, j][j].wait_recv()
        piece = part(ty if j else tx, h, j)
        k = 8 + 2 * h + j
        passes[h, j] = go(piece, piece, gs.at[k], gr.at[k], x_dev if j else y_dev)

    near_copy.wait_recv()
    attend(blocks[0], 0, groups // 2)
    spread(0, 0)
    attend(blocks[0], groups // 2, groups)
    spread(0, 1)

    @pl.when(has_far)
    def _():
        far_copy.wait_recv()

    attend(blocks[1], 0, groups // 2)
    spread(1, 0)
    attend(blocks[1], groups // 2, groups)
    spread(1, 1)
    for copy in meta_copies:
        copy.wait_recv()
    meta_z[z] = (meta[...] + meta_in[tx]) + (meta_in[ty] + meta_in[td])
    meta_z_copies = [
        go(meta_z.at[z], meta_z.at[z], ms.at[2 + m], mr.at[2 + m], z_devs[m]) for m in (1, 2, 3)
    ]
    loads[3].wait()

    def product(h, owner):
        weight = w[pl.ds(pl.multiple_of(owner * depth, depth), depth)]
        return jnp.dot(buf[owner, parts_of[h]], weight, preferred_element_type=jnp.float32)

    def gather(h):
        hand_on(h, 0)
        acc[h] = product(h, t)
        hand_on(h, 1)
        spreads[h, 1][0].wait_recv()
        acc[h] += product(h, tx)
        spreads[h, 0][1].wait_recv()
        acc[h] += product(h, ty)

    gather(0)
    for copy in res_copies:
        copy.wait_recv()
    gather(1)
    gain = gain_ref[:, aligned(t * width, width)]

    def finish(h):
        projected = (acc[h] + product(h, td)).astype(proj.dtype)
        proj[parts_of[h]] = projected
        pair = res_in[pl.ds(2 * blocks[h], 2)].reshape(half, width)
        value = pair.astype(jnp.float32) + projected.astype(jnp.float32)
        tok[t, z, parts_of[h]] = (value * gain).astype(tok.dtype)
        return jnp.sum(value * value, axis=-1, keepdims=True)

    def record(h, sums):
        squares[blocks[h]] = jnp.broadcast_to(sums, (half, half)).T[: squares.shape[1]]

    def own_block(h):
        return tok.at[t, z, parts_of[h]]

    z_in = {
        (m, h): remote(
            own_block(h), tok.at[t, planes[m], parts_of[h]], zs.at[m, h], zr.at[m, h], z_devs[m]
        )
        for m in (1, 2, 3)
        for h in (0, 1)
    }

    out_one = [remote(own_block(h), own_block(h), zs.at[1, h], zr.at[1, h], z_devs[1]) for h in (0, 1)]
    out_three = [remote(own_block(h), own_block(h), zs.at[3, h], zr.at[3, h], z_devs[3]) for h in (0, 1)]

    def relay_copy(m, h):
        piece = tok.at[t, planes[m], parts_of[h]]
        lands, device = ((2, z_devs[3]), None, (3, z_devs[1]), (2, z_devs[1]))[
            {1: 0, 2: 2, 3: 3}[m]
        ]
        return remote(piece, piece, zs.at[3 + m, h], zr.at[lands, h], device)

    def depart(h):
        out_one[h].start()

        @pl.when(inner)
        def _():
            out_three[h].start()

    sent, forwarded, picks, parts, firsts, seconds, homes = {}, {}, {}, {}, {}, {}, {}

    def arrive(m, h):
        z_in[m, h].wait_recv()

    def relay(m, h, waited=True):
        @pl.when(inner)
        def _():
            if not waited:
                arrive(m, h)
            relay_copy(m, h).start()

    def send(m, h):
        piece = tok.at[t, planes[m], parts_of[h]]
        sent[m, h] = (
            go(piece, piece, ds_.at[m, 2 * h], dr.at[m, 2 * h], x_dev),
            go(piece, piece, ds_.at[m, 2 * h + 1], dr.at[m, 2 * h + 1], y_dev),
        )

    def forward(m, h):
        sent[m, h][0].wait_recv()
        piece = tok.at[tx, planes[m], aligned(blocks[h] * half, half // 2)]
        first = go(piece, piece, ds_.at[m, 4 + 2 * h], dr.at[m, 4 + 2 * h], y_dev)
        sent[m, h][1].wait_recv()
        piece = tok.at[ty, planes[m], aligned(blocks[h] * half + half // 2, half // 2)]
        second = go(piece, piece, ds_.at[m, 5 + 2 * h], dr.at[m, 5 + 2 * h], x_dev)
        forwarded[m, h] = (first, second)

    slots = xo.shape[1]
    capacity = slots // 4
    step = 256
    row = lax.broadcasted_iota(jnp.int32, (slots, lanes), 0).astype(jnp.float32)
    shift = (lax.broadcasted_iota(jnp.int32, (1, lanes), 1) // tokens * capacity).astype(
        jnp.float32
    )

    def place(source, m, which):
        ranks = source[planes[m], pl.ds(which, 1), :]
        target = jnp.where(ranks > 0.5, ranks + (shift - 1.0), -1.0)
        return row == target

    def scale(source, m, which):
        weights = source[planes[m], pl.ds(count + which, 1), :]
        return jnp.sum(
            jnp.where(place(source, m, which), weights, 0.0), axis=1, keepdims=True
        )

    def picking(m):
        return jnp.concatenate(
            [jnp.where(place(meta_z, m, which), 1.0, 0.0) for which in (s, near)], axis=0
        )

    handed = []

    def hand_over():
        for k, owner in enumerate((tx, ty, td)):
            piece = tok.at[owner, z]
            handed.append(go(piece, piece, hos.at[k], hor.at[k], z_devs[1]))

    def complete(m):
        if m == 1:
            for copy in handed:
                copy.wait_recv()
        else:
            for h in (0, 1):
                for copy in forwarded[m, h]:
                    copy.wait_recv()

    def pick(m):
        chooser = picking(m)
        lengths = inverse[planes[m]]
        lengths = jnp.concatenate([lengths[0, 0:1], lengths[1, 0:1]], axis=1)
        factor = jnp.sum(chooser * lengths, axis=1, keepdims=True)
        chooser = chooser.astype(jnp.bfloat16)
        for owner in range(4):
            for k in range(width // step):
                rows_in = tok[owner, planes[m], :, k * step : (k + 1) * step]
                found = jnp.dot(chooser, rows_in, preferred_element_type=jnp.float32)
                found = (found * factor).astype(xs.dtype)
                columns = slice(owner * width + k * step, owner * width + (k + 1) * step)
                xs[m, 0:slots, columns] = found[:slots]
                xo[m, :, columns] = found[slots:]
        picks[m] = go(
            xo.at[m], xs.at[m, pl.ds(slots, slots)], xs_s.at[m], xs_r.at[m], n_dev
        )

    def rise(m, begin, end):
        @pl.loop(begin, end)
        def _(k):
            columns = pl.ds(pl.multiple_of(k * step, step), step)
            x = xs[m]
            g = jnp.dot(x, gate[:, columns], preferred_element_type=jnp.float32)
            u = jnp.dot(x, up[:, columns], preferred_element_type=jnp.float32)
            hidden[:, columns] = (jax.nn.silu(g) * u).astype(hidden.dtype)

    total_steps = gate.shape[1] // step

    def fall(m):
        factor_mine = scale(meta_z, m, s)
        factor_near = scale(meta_p, m, s)
        wide = 512

        @pl.loop(0, model // wide)
        def _(k):
            columns = pl.ds(pl.multiple_of(k * wide, wide), wide)
            share = jnp.dot(hidden[...], down[:, columns], preferred_element_type=jnp.float32)
            po[m, 0:slots, columns] = (share[:slots] * factor_mine).astype(po.dtype)
            ps[m, :, columns] = (share[slots:] * factor_near).astype(ps.dtype)

        parts[m] = go(
            ps.at[m], po.at[m, pl.ds(slots, slots)], ps_s.at[m], ps_r.at[m], n_dev
        )

    def expand(m):
        parts[m].wait_recv()
        spreader = picking(m).T.astype(jnp.bfloat16)
        for owner in range(4):
            holds = jnp.where(t == owner, 1.0, 0.0)
            for k in range(width // step):
                columns = slice(owner * width + k * step, owner * width + (k + 1) * step)
                found = jnp.dot(spreader, po[m, :, columns], preferred_element_type=jnp.float32)
                if m == 0:
                    found += holds * proj[:, k * step : (k + 1) * step].astype(jnp.float32)
                rt[m, :, :, columns] = found.astype(rt.dtype).reshape(4, tokens, step)

    low, high = pl.ds(0, own // 2), pl.ds(own // 2, own // 2)

    def reduce_far(m):
        firsts[m] = (
            go(rt.at[m, td, low], bx1.at[m, 1], rs.at[m, 0], rr.at[m, 0], x_dev),
            go(rt.at[m, td, high], by1.at[m, 1], rs.at[m, 1], rr.at[m, 1], y_dev),
        )

    def reduce_side(m):
        firsts[m] += (
            go(rt.at[m, tx, low], bx1.at[m, 0], rs.at[m, 2], rr.at[m, 2], x_dev),
            go(rt.at[m, ty, high], by1.at[m, 0], rs.at[m, 3], rr.at[m, 3], y_dev),
        )

    def reduce_one(m):
        reduce_far(m)
        reduce_side(m)

    def wide_sum(*pieces):
        result = pieces[0].astype(jnp.float32)
        for piece in pieces[1:]:
            result = result + piece.astype(jnp.float32)
        return result

    def reduce_two(m):
        firsts[m][0].wait_recv()
        mid[m, 0] = wide_sum(rt[m, ty, low], bx1[m, 1]).astype(mid.dtype)
        to_side = go(mid.at[m, 0], by2.at[m], rs.at[m, 4], rr.at[m, 4], y_dev)
        firsts[m][1].wait_recv()
        mid[m, 1] = wide_sum(rt[m, tx, high], by1[m, 1]).astype(mid.dtype)
        seconds[m] = (
            to_side,
            go(mid.at[m, 1], bx2.at[m], rs.at[m, 5], rr.at[m, 5], x_dev),
        )

    def reduce_three(m):
        firsts[m][2].wait_recv()
        seconds[m][0].wait_recv()
        lower = wide_sum(rt[m, t, low], bx1[m, 0], by2[m])
        if m:
            sz[m, low] = lower.astype(sz.dtype)
            lower_home = go(sz.at[m, low], zin.at[m, low], zbs.at[m, 0], zbr.at[m, 0], z_devs[m])
        else:
            home_sum[low] = lower
        firsts[m][3].wait_recv()
        seconds[m][1].wait_recv()
        upper = wide_sum(rt[m, t, high], by1[m, 0], bx2[m])
        if m:
            sz[m, high] = upper.astype(sz.dtype)
            homes[m] = (
                lower_home,
                go(sz.at[m, high], zin.at[m, high], zbs.at[m, 1], zbr.at[m, 1], z_devs[m]),
            )
        else:
            home_sum[high] = upper

    def share_squares():
        return [
            go(squares, squares_in.at[t], qs.at[k], qr.at[k], device)
            for k, device in enumerate((x_dev, y_dev, d_dev))
        ]

    def invert(square_copies):
        for copy in square_copies:
            copy.wait_recv()
        total = (squares[...] + squares_in[tx]) + (squares_in[ty] + squares_in[td])
        inverse[z] = lax.rsqrt(total * (1.0 / model) + EPS)
        return {
            m: go(inverse.at[z], inverse.at[z], qs.at[2 + m], qr.at[2 + m], z_devs[m])
            for m in (1, 2, 3)
        }

    passes[0, 0].wait_recv()
    passes[0, 1].wait_recv()
    sums = finish(0)
    send(0, 0)
    depart(0)
    record(0, sums)
    passes[1, 0].wait_recv()
    passes[1, 1].wait_recv()
    sums = finish(1)
    send(0, 1)
    depart(1)
    record(1, sums)
    square_copies = share_squares()
    for copy in meta_z_copies:
        copy.wait_recv()
    meta_near = go(meta_z, meta_p, ms.at[6], mr.at[6], n_dev)
    forward(0, 0)
    arrive(1, 0)
    relay(1, 0)
    forward(0, 1)
    arrive(1, 1)
    relay(1, 1)
    relay(3, 0, False)
    relay(3, 1, False)
    inverse_copies = invert(square_copies)
    complete(0)
    pick(0)
    arrive(2, 0)
    relay(2, 0)
    send(2, 0)
    picks[0].wait_recv()
    for copy in loads[5:]:
        copy.wait()
    rise(0, 0, 2)
    arrive(2, 1)
    relay(2, 1)
    send(2, 1)
    hand_over()
    rise(0, 2, total_steps)
    forward(2, 0)
    meta_near.wait_recv()
    fall(0)
    forward(2, 1)

    @pl.when(outer)
    def _():
        arrive(3, 0)

    send(3, 0)
    expand(0)

    @pl.when(outer)
    def _():
        arrive(3, 1)

    send(3, 1)
    complete(2)
    inverse_copies[2].wait_recv()
    pick(2)
    forward(3, 0)
    picks[2].wait_recv()
    rise(2, 0, total_steps - 1)
    forward(3, 1)
    reduce_far(0)
    rise(2, total_steps - 1, total_steps)
    fall(2)
    complete(3)
    inverse_copies[3].wait_recv()
    pick(3)
    expand(2)
    reduce_one(2)
    picks[3].wait_recv()
    rise(3, 0, total_steps)
    fall(3)
    reduce_two(2)
    complete(1)
    inverse_copies[1].wait_recv()
    pick(1)
    expand(3)
    reduce_one(3)
    picks[1].wait_recv()
    rise(1, 0, total_steps)
    reduce_three(2)
    fall(1)
    reduce_two(3)
    expand(1)
    reduce_one(1)
    reduce_three(3)
    reduce_two(1)
    reduce_side(0)
    reduce_two(0)
    reduce_three(1)
    reduce_three(0)
    for m in (2, 3, 1):
        homes[m][0].wait_recv()
        homes[m][1].wait_recv()
    out_ref[...] = (
        res[...].astype(jnp.float32) + (home_sum[...] + wide_sum(zin[1], zin[2], zin[3]))
    ).astype(out_ref.dtype)
    for copy in copies:
        copy.wait_send()
    near_copy.wait_send()
    for h in (0, 1):
        out_one[h].wait_send()

    @pl.when(inner)
    def _():
        for h in (0, 1):
            out_three[h].wait_send()
            for m in (1, 2, 3):
                relay_copy(m, h).wait_send()

    @pl.when(has_far)
    def _():
        far_copy.wait_send()


def layer(
    queries, keys, values, sink_logit, out_weight, residual, norm_gain, routes, route_weights,
    gate_weight, up_weight, down_weight, capacity,
):
    rows, depth = queries.shape
    kind = queries.dtype
    width = out_weight.shape[1]
    tokens, model = residual.shape
    count = lax.axis_size("sp")
    slots = 4 * capacity
    anywhere = pl.BlockSpec(memory_space=pl.ANY)
    vmem = pl.BlockSpec(memory_space=pltpu.VMEM)
    dma = pltpu.SemaphoreType.DMA
    one, six = dma((4,)), dma((4, 6))
    lanes = 4 * tokens
    return pl.pallas_call(
        layer_kernel,
        out_shape=pltpu.VMEM(residual.shape, kind),
        in_specs=[anywhere] * 3
        + [pl.BlockSpec(memory_space=pltpu.SMEM), anywhere, anywhere, vmem, vmem, vmem]
        + [anywhere] * 3,
        out_specs=vmem,
        scratch_shapes=[
            pltpu.VMEM(queries.shape, kind),
            pltpu.VMEM((2 * rows, 2 * keys.shape[1]), kind),
            pltpu.VMEM(out_weight.shape, kind),
            pltpu.VMEM(residual.shape, kind),
            pltpu.VMEM((4, tokens, width), kind),
            pltpu.VMEM((4, rows, depth), kind),
            pltpu.VMEM((2, rows // 2, width), jnp.float32),
            pltpu.VMEM((rows, width), kind),
            pltpu.VMEM(gate_weight.shape, kind),
            pltpu.VMEM(up_weight.shape, kind),
            pltpu.VMEM(down_weight.shape, kind),
            pltpu.VMEM((2 * count, lanes), jnp.float32),
            pltpu.VMEM((4, 2 * count, lanes), jnp.float32),
            pltpu.VMEM((4, 2 * count, lanes), jnp.float32),
            pltpu.VMEM((4, 2 * count, lanes), jnp.float32),
            pltpu.VMEM((2, 8, rows // 2), jnp.float32),
            pltpu.VMEM((4, 2, 8, rows // 2), jnp.float32),
            pltpu.VMEM((4, 2, 8, rows // 2), jnp.float32),
            pltpu.VMEM((4, 4, rows, width), kind),
            pltpu.VMEM((4, 2 * slots, model), kind),
            pltpu.VMEM((4, slots, model), kind),
            pltpu.VMEM((2 * slots, gate_weight.shape[1]), kind),
            pltpu.VMEM((4, 2 * slots, model), kind),
            pltpu.VMEM((4, slots, model), kind),
            pltpu.VMEM((4, 4, tokens, model), kind),
            pltpu.VMEM((4, 2, tokens // 2, model), kind),
            pltpu.VMEM((4, 2, tokens // 2, model), kind),
            pltpu.VMEM((4, tokens // 2, model), kind),
            pltpu.VMEM((4, tokens // 2, model), kind),
            pltpu.VMEM((4, 2, tokens // 2, model), kind),
            pltpu.VMEM((4, tokens, model), kind),
            pltpu.VMEM((4, tokens, model), kind),
            pltpu.VMEM(residual.shape, jnp.float32),
            dma((8,)),
            dma((2,)), dma((2,)),
            dma((12,)), dma((12,)),
            dma((3,)), dma((3,)),
            dma((7,)), dma((7,)),
            dma((6,)), dma((6,)),
            dma((7, 2)), dma((4, 2)),
            dma((4, 8)), dma((4, 8)), one, one, one, one, six, six,
            dma((4, 2)), dma((4, 2)), dma((3,)), dma((3,)),
        ],
        compiler_params=pltpu.CompilerParams(
            collective_id=0, has_side_effects=True, vmem_limit_bytes=60 * 1024 * 1024
        ),
    )(
        queries, keys, values, sink_logit, out_weight, residual, norm_gain.reshape(1, -1),
        routes.T, route_weights.T,
        gate_weight, up_weight, down_weight,
    )


def with_halo(block, sides, width):
    for axis, dim in sides:
        count = lax.axis_size(axis)
        forward = [(i, i + 1) for i in range(count - 1)]
        backward = [(target, source) for source, target in forward]
        low = lax.ppermute(
            lax.slice_in_dim(block, block.shape[dim] - width, None, axis=dim), axis, forward
        )
        high = lax.ppermute(lax.slice_in_dim(block, 0, width, axis=dim), axis, backward)
        block = jnp.concatenate([low, block, high], axis=dim)
    return block


def make_band(extended, length):
    blocks = length // WINDOW
    pieces = [
        lax.slice_in_dim(extended, offset * WINDOW, offset * WINDOW + length, axis=0).reshape(
            blocks, WINDOW, -1
        )
        for offset in range(3)
    ]
    return jnp.concatenate(pieces, axis=1)


def attend_local(queries, keys, values, sink_logit):
    length = queries.shape[0]
    groups = keys.shape[1] // HEAD
    repeat = HEADS // KV_HEADS
    blocks = length // WINDOW
    joined = jnp.concatenate([keys, values], axis=1)
    extended = with_halo(joined, (("sp", 0),), WINDOW)
    banded = make_band(extended, length)
    key_band = banded[..., : groups * HEAD].reshape(blocks, 3 * WINDOW, groups, HEAD)
    value_band = banded[..., groups * HEAD :].reshape(blocks, 3 * WINDOW, groups, HEAD)
    query_blocks = queries.reshape(blocks, WINDOW, groups, repeat, HEAD)
    scores = jnp.einsum(
        "nqgrd,nkgd->ngrqk", query_blocks, key_band, preferred_element_type=jnp.float32
    ) * HEAD ** (-0.5)
    near = jnp.abs(jnp.arange(WINDOW)[:, None] + WINDOW - jnp.arange(3 * WINDOW)[None, :]) <= WINDOW
    first_token = lax.axis_index("sp") * length
    key_pos = (
        first_token + (jnp.arange(blocks)[:, None] - 1) * WINDOW + jnp.arange(3 * WINDOW)[None, :]
    )
    inside = (key_pos >= 0) & (key_pos < length * lax.axis_size("sp"))
    valid = near[None, None, None, :, :] & inside[:, None, None, None, :]
    sinks = sink_logit.reshape(1, groups, repeat, 1, 1)
    masked = jnp.where(valid, scores, NEGATIVE)
    top = jnp.maximum(jnp.max(masked, axis=-1, keepdims=True), sinks)
    probs = jnp.exp(masked - top)
    denom = jnp.sum(probs, axis=-1, keepdims=True) + jnp.exp(sinks - top)
    weights = (probs / denom).astype(jnp.bfloat16)
    output = jnp.einsum(
        "ngrqk,nkgd->nqgrd", weights, value_band, preferred_element_type=jnp.float32
    )
    return output.astype(jnp.bfloat16).reshape(length, groups * repeat * HEAD)


def local(
    queries,
    keys,
    values,
    sink_logit,
    out_weight,
    residual,
    norm_gain,
    routes,
    route_weights,
    gate_weight,
    up_weight,
    down_weight,
):
    capacity = max(2, 4 * residual.shape[0] // lax.axis_size("sp"))
    in_plane = (
        lax.axis_size("tp") == 4
        and lax.axis_size("sp") == 8
        and capacity % 32 == 0
        and gate_weight.shape[2] % 256 == 0
        and queries.shape[0] == 2 * WINDOW
        and residual.shape[0] == 64
    )
    if in_plane:
        return layer(
            queries, keys, values, sink_logit, out_weight, residual, norm_gain, routes,
            route_weights, gate_weight[0], up_weight[0], down_weight[0], capacity,
        )
    attention = attend_local(queries, keys, values, sink_logit)
    columns = jnp.dot(
        lax.all_gather(attention, "tp", axis=1, tiled=True),
        out_weight,
        preferred_element_type=jnp.float32,
    )
    projected = lax.all_to_all(
        columns.astype(jnp.bfloat16), "tp", split_axis=0, concat_axis=1, tiled=True
    )
    hidden_state = residual.astype(jnp.float32) + projected.astype(jnp.float32)
    inverse = lax.rsqrt(jnp.mean(hidden_state * hidden_state, axis=-1, keepdims=True) + EPS)
    normed = (hidden_state * inverse * norm_gain).astype(jnp.bfloat16)
    sp_count = lax.axis_size("sp")
    tok_rows = residual.shape[0]
    width = residual.shape[1]
    slot_total = sp_count * capacity
    expert_ids = routes.reshape(-1)
    onehot = (expert_ids[:, None] == jnp.arange(sp_count, dtype=jnp.int32)[None, :]).astype(
        jnp.int32
    )
    earlier = jnp.cumsum(onehot, axis=0) - onehot
    rank = jnp.sum(earlier * onehot, axis=1)
    slots = expert_ids * capacity + rank
    placing = (slots[:, None] == jnp.arange(slot_total, dtype=jnp.int32)[None, :]).astype(
        jnp.bfloat16
    )
    placing = placing.reshape(tok_rows, 2, slot_total)
    first_place = placing[:, 0]
    second_place = placing[:, 1]
    sending = jnp.einsum(
        "ts,td->sd", first_place + second_place, normed, preferred_element_type=jnp.float32
    )
    sending = sending.astype(jnp.bfloat16).reshape(sp_count, capacity, width)
    piece = lax.all_gather(
        lax.all_to_all(sending, "sp", split_axis=0, concat_axis=0, tiled=True),
        "tp",
        axis=0,
        tiled=True,
    )
    flat = piece.reshape(-1, piece.shape[-1])
    gate = jnp.dot(flat, gate_weight[0], preferred_element_type=jnp.float32)
    upward = jnp.dot(flat, up_weight[0], preferred_element_type=jnp.float32)
    hidden = (jax.nn.silu(gate) * upward).astype(jnp.bfloat16)
    partial_value = jnp.dot(hidden, down_weight[0], preferred_element_type=jnp.float32)
    partial_value = partial_value.reshape(piece.shape[:-1] + (down_weight.shape[-1],))
    returned = lax.all_to_all(
        lax.psum_scatter(
            partial_value.astype(jnp.bfloat16), "tp", scatter_dimension=0, tiled=True
        ),
        "sp",
        split_axis=0,
        concat_axis=0,
        tiled=True,
    )
    gathered_back = returned.reshape(slot_total, width)
    first_pick = jnp.dot(first_place, gathered_back, preferred_element_type=jnp.float32)
    second_pick = jnp.dot(second_place, gathered_back, preferred_element_type=jnp.float32)
    mixture = route_weights[:, 0:1] * first_pick + route_weights[:, 1:2] * second_pick
    return (hidden_state + mixture).astype(jnp.bfloat16)


def solution(mesh):
    in_specs = (
        P("sp", "tp"),
        P("sp", "tp"),
        P("sp", "tp"),
        P("tp"),
        P(None, "tp"),
        P(("sp", "tp"), None),
        P(),
        P(("sp", "tp"), None),
        P(("sp", "tp"), None),
        P("sp", None, "tp"),
        P("sp", None, "tp"),
        P("sp", "tp", None),
    )
    out_specs = P(("sp", "tp"), None)
    return jax.shard_map(local, mesh=mesh, in_specs=in_specs, out_specs=out_specs, check_vma=False)
```

```python
import functools

import jax
import jax.numpy as jnp
from jax import lax
from jax.experimental import pallas as pl
from jax.experimental.pallas import tpu as pltpu
from jax.sharding import PartitionSpec as P

HEADS = 32
KV_HEADS = 16
HEAD = 64
WINDOW = 128


EPS = 1e-06
NEGATIVE = -1e30
MESH = pl.DeviceIdType.MESH


def plane():
    t = lax.axis_index("tp")
    tx = t + 1 - 2 * lax.rem(t, 2)
    ty = lax.rem(t + 2, 4)
    return t, tx, ty, 3 - t


def remote(src, dst, send, recv, device):
    return pltpu.make_async_remote_copy(
        src_ref=src,
        dst_ref=dst,
        send_sem=send,
        recv_sem=recv,
        device_id=device,
        device_id_type=MESH,
    )


def flipped(index, mask):
    result = index
    bit = 1
    while bit <= mask:
        if mask & bit:
            result = result + bit * (1 - 2 * lax.rem(index // bit, 2))
        bit *= 2
    return result


def layer_kernel(
    q_hbm, k_hbm, v_hbm, sink_hbm, w_hbm, res_hbm, gain_hbm, routes_hbm, route_weights_hbm,
    gate_hbm, up_hbm, down_hbm, out_ref,
    sink_ref, gain_ref, routes_ref, route_weights_ref, q, kv, w, res, res_in, buf, acc, proj, gate, up, down,
    meta, meta_in, meta_z, meta_p, squares, squares_in, inverse, tok, xs, xo, hidden, po, ps, rt,
    bx1, by1, bx2, by2, mid, sz, zin, home_sum,
    load, hs, hr, gs, gr, as_, ar, ms, mr, qs, qr, zs, zr, ds_, dr, xs_s, xs_r, ps_s, ps_r,
    rs, rr, zbs, zbr, hos, hor,
):
    s = lax.axis_index("sp")
    t, tx, ty, td = plane()
    last = lax.axis_size("sp") - 1
    rows, depth = q.shape
    half = rows // 2
    groups = k_hbm.shape[1] // HEAD
    kept = groups * HEAD
    odd = lax.rem(s, 2)
    near = s + 1 - 2 * odd
    has_far = jnp.logical_and(s != 0, s != last)
    far = jnp.where(has_far, s - 1 + 2 * odd, near)
    x_dev, y_dev, d_dev, n_dev, f_dev = (s, tx), (s, ty), (s, td), (near, t), (far, t)
    z = s // 2
    planes = [flipped(z, m) for m in range(4)]
    z_devs = [(2 * planes[m] + odd, t) for m in range(4)]
    inner = jnp.logical_or(z == 1, z == 2)
    outer = jnp.logical_not(inner)
    middle = pl.ds(half, rows)
    loads = [
        pltpu.make_async_copy(source, target, load.at[k])
        for k, (source, target) in enumerate(
            (
                (k_hbm, kv.at[middle, pl.ds(0, kept)]),
                (v_hbm, kv.at[middle, pl.ds(kept, kept)]),
                (q_hbm, q),
                (w_hbm, w),
                (res_hbm, res),
                (gate_hbm, gate),
                (up_hbm, up),
                (down_hbm, down),
                (sink_hbm, sink_ref),
                (routes_hbm, routes_ref),
                (route_weights_hbm, route_weights_ref),
                (gain_hbm, gain_ref),
            )
        )
    ]
    barrier = pltpu.get_barrier_semaphore()
    for device in [x_dev, y_dev, d_dev, n_dev] + z_devs[1:]:
        pl.semaphore_signal(barrier, inc=1, device_id=device, device_id_type=MESH)

    @pl.when(has_far)
    def _():
        pl.semaphore_signal(barrier, inc=1, device_id=f_dev, device_id_type=MESH)

    for copy in loads[:5] + loads[8:]:
        copy.start()

    @pl.when(has_far)
    def _():
        pl.semaphore_wait(barrier, 8)

    @pl.when(jnp.logical_not(has_far))
    def _():
        pl.semaphore_wait(barrier, 7)

    def aligned(value, size):
        return pl.ds(pl.multiple_of(value, size), size)

    near_src = aligned(2 * half - half * odd, half)
    near_dst = aligned(3 * half * odd, half)
    far_src = aligned(half + half * odd, half)
    far_dst = aligned(3 * half * (1 - odd), half)
    near_copy = remote(kv.at[near_src], kv.at[near_dst], hs.at[0], hr.at[0], n_dev)
    far_copy = remote(kv.at[far_src], kv.at[far_dst], hs.at[1], hr.at[1], f_dev)
    loads[0].wait()
    loads[1].wait()

    @pl.when(has_far)
    def _():
        far_copy.start()

    near_copy.start()
    copies = []

    def go(*args):
        copy = remote(*args)
        copy.start()
        copies.append(copy)
        return copy

    own, model = res.shape
    width = w.shape[1]
    loads[4].wait()
    res_copies = [
        go(
            res.at[:, aligned(owner * width, width)],
            res_in.at[t],
            as_.at[k],
            ar.at[k],
            device,
        )
        for k, (owner, device) in enumerate(((tx, x_dev), (ty, y_dev), (td, d_dev)))
    ]
    res_in[t] = res[:, aligned(t * width, width)]
    count, lanes = meta.shape[0] // 2, meta.shape[1]
    tokens = lanes // 4
    expert = lax.broadcasted_iota(jnp.int32, (count, lanes), 0)
    lane = lax.broadcasted_iota(jnp.int32, (count, lanes), 1)
    mine_lane = jnp.logical_and(lane >= t * tokens, lane < (t + 1) * tokens)
    for copy in loads[8:]:
        copy.wait()
    routes = jnp.concatenate([routes_ref[...]] * 4, axis=1)
    route_weights = jnp.concatenate([route_weights_ref[...]] * 4, axis=1)
    hit_one = routes[0:1, :] == expert
    hit = jnp.logical_and(mine_lane, jnp.logical_or(hit_one, routes[1:2, :] == expert))
    chosen = jnp.where(hit, 1.0, 0.0)
    before = lax.broadcasted_iota(jnp.int32, (lanes, lanes), 0) <= lax.broadcasted_iota(
        jnp.int32, (lanes, lanes), 1
    )
    rank = jnp.dot(
        chosen.astype(jnp.bfloat16),
        jnp.where(before, 1.0, 0.0).astype(jnp.bfloat16),
        preferred_element_type=jnp.float32,
    )
    meta[0:count] = chosen * rank
    meta[count : 2 * count] = chosen * jnp.where(
        hit_one, route_weights[0:1, :], route_weights[1:2, :]
    )
    meta_copies = [
        go(meta, meta_in.at[t], ms.at[k], mr.at[k], device)
        for k, device in enumerate((x_dev, y_dev, d_dev))
    ]

    for copy in loads[5:8]:
        copy.start()

    @pl.when(jnp.logical_not(has_far))
    def _():
        kv[aligned(3 * half * odd, half)] = jnp.zeros((half, kv.shape[1]), kv.dtype)

    loads[2].wait()
    span = 3 * half
    query = lax.broadcasted_iota(jnp.int32, (2 * half, span), 0)
    query = jnp.where(query >= half, query - half, query)
    key = lax.broadcasted_iota(jnp.int32, (2 * half, span), 1)
    band = jnp.abs(query + half - key) <= WINDOW
    upper = lax.broadcasted_iota(jnp.int32, (2 * half, 1), 0) < half

    def attend(b, first, end):
        valid = jnp.logical_and(
            band,
            jnp.logical_and(
                key >= jnp.where(2 * s + b == 0, half, 0),
                key < jnp.where(2 * s + b == 2 * last + 1, 2 * half, span),
            ),
        )
        keys_at = pl.ds(pl.multiple_of(b * half, half), span)
        mine = aligned(b * half, half)
        for g in range(first, end):
            pair = q[mine, 2 * g * HEAD : 2 * (g + 1) * HEAD]
            stacked = jnp.concatenate([pair[:, :HEAD], pair[:, HEAD:]], axis=0)
            scores = lax.dot_general(
                stacked,
                kv[keys_at, g * HEAD : (g + 1) * HEAD],
                (((1,), (1,)), ((), ())),
                preferred_element_type=jnp.float32,
            ) * HEAD ** (-0.5)
            sink = jnp.where(upper, sink_ref[2 * g], sink_ref[2 * g + 1])
            masked = jnp.where(valid, scores, NEGATIVE)
            top = jnp.maximum(jnp.max(masked, axis=-1, keepdims=True), sink)
            probs = jnp.exp(masked - top)
            denom = jnp.sum(probs, axis=-1, keepdims=True) + jnp.exp(sink - top)
            weights = (probs * (1.0 / denom)).astype(jnp.bfloat16)
            output = jnp.dot(
                weights,
                kv[keys_at, kept + g * HEAD : kept + (g + 1) * HEAD],
                preferred_element_type=jnp.float32,
            )
            joined = jnp.concatenate([output[:half], output[half:]], axis=1)
            buf[t, mine, 2 * g * HEAD : 2 * (g + 1) * HEAD] = joined.astype(buf.dtype)

    blocks = (1 - odd, odd)
    parts_of = [aligned(b * half, half) for b in blocks]

    wide_piece = depth // 2

    def part(owner, h, j):
        return buf.at[owner, parts_of[h], pl.ds(j * wide_piece, wide_piece)]

    spreads, passes = {}, {}

    def spread(h, j):
        piece = part(t, h, j)
        k = 4 * h + 2 * j
        spreads[h, j] = (
            go(piece, piece, gs.at[k], gr.at[k], x_dev),
            go(piece, piece, gs.at[k + 1], gr.at[k + 1], y_dev),
        )

    def hand_on(h, j):
        spreads[h, j][j].wait_recv()
        piece = part(ty if j else tx, h, j)
        k = 8 + 2 * h + j
        passes[h, j] = go(piece, piece, gs.at[k], gr.at[k], x_dev if j else y_dev)

    near_copy.wait_recv()
    attend(blocks[0], 0, groups // 2)
    spread(0, 0)
    attend(blocks[0], groups // 2, groups)
    spread(0, 1)

    @pl.when(has_far)
    def _():
        far_copy.wait_recv()

    attend(blocks[1], 0, groups // 2)
    spread(1, 0)
    attend(blocks[1], groups // 2, groups)
    spread(1, 1)
    for copy in meta_copies:
        copy.wait_recv()
    meta_z[z] = (meta[...] + meta_in[tx]) + (meta_in[ty] + meta_in[td])
    meta_z_copies = [
        go(meta_z.at[z], meta_z.at[z], ms.at[2 + m], mr.at[2 + m], z_devs[m]) for m in (1, 2, 3)
    ]
    loads[3].wait()

    def product(h, owner):
        weight = w[pl.ds(pl.multiple_of(owner * depth, depth), depth)]
        return jnp.dot(buf[owner, parts_of[h]], weight, preferred_element_type=jnp.float32)

    def gather(h):
        hand_on(h, 0)
        acc[h] = product(h, t)
        hand_on(h, 1)
        spreads[h, 1][0].wait_recv()
        acc[h] += product(h, tx)
        spreads[h, 0][1].wait_recv()
        acc[h] += product(h, ty)

    gather(0)
    for copy in res_copies:
        copy.wait_recv()
    gather(1)
    gain = gain_ref[:, aligned(t * width, width)]

    def finish(h):
        projected = (acc[h] + product(h, td)).astype(proj.dtype)
        proj[parts_of[h]] = projected
        pair = res_in[pl.ds(2 * blocks[h], 2)].reshape(half, width)
        value = pair.astype(jnp.float32) + projected.astype(jnp.float32)
        tok[t, z, parts_of[h]] = (value * gain).astype(tok.dtype)
        return jnp.sum(value * value, axis=-1, keepdims=True)

    def record(h, sums):
        squares[blocks[h]] = jnp.broadcast_to(sums, (half, half)).T[: squares.shape[1]]

    def own_block(h):
        return tok.at[t, z, parts_of[h]]

    z_in = {
        (m, h): remote(
            own_block(h), tok.at[t, planes[m], parts_of[h]], zs.at[m, h], zr.at[m, h], z_devs[m]
        )
        for m in (1, 2, 3)
        for h in (0, 1)
    }

    out_one = [remote(own_block(h), own_block(h), zs.at[1, h], zr.at[1, h], z_devs[1]) for h in (0, 1)]
    out_three = [remote(own_block(h), own_block(h), zs.at[3, h], zr.at[3, h], z_devs[3]) for h in (0, 1)]

    def relay_copy(m, h):
        piece = tok.at[t, planes[m], parts_of[h]]
        lands, device = ((2, z_devs[3]), None, (3, z_devs[1]), (2, z_devs[1]))[
            {1: 0, 2: 2, 3: 3}[m]
        ]
        return remote(piece, piece, zs.at[3 + m, h], zr.at[lands, h], device)

    def depart(h):
        out_one[h].start()

        @pl.when(inner)
        def _():
            out_three[h].start()

    sent, forwarded, picks, parts, firsts, seconds, homes = {}, {}, {}, {}, {}, {}, {}

    def arrive(m, h):
        z_in[m, h].wait_recv()

    def relay(m, h, waited=True):
        @pl.when(inner)
        def _():
            if not waited:
                arrive(m, h)
            relay_copy(m, h).start()

    def send(m, h):
        piece = tok.at[t, planes[m], parts_of[h]]
        sent[m, h] = (
            go(piece, piece, ds_.at[m, 2 * h], dr.at[m, 2 * h], x_dev),
            go(piece, piece, ds_.at[m, 2 * h + 1], dr.at[m, 2 * h + 1], y_dev),
        )

    def forward(m, h):
        sent[m, h][0].wait_recv()
        piece = tok.at[tx, planes[m], aligned(blocks[h] * half, half // 2)]
        first = go(piece, piece, ds_.at[m, 4 + 2 * h], dr.at[m, 4 + 2 * h], y_dev)
        sent[m, h][1].wait_recv()
        piece = tok.at[ty, planes[m], aligned(blocks[h] * half + half // 2, half // 2)]
        second = go(piece, piece, ds_.at[m, 5 + 2 * h], dr.at[m, 5 + 2 * h], x_dev)
        forwarded[m, h] = (first, second)

    slots = xo.shape[1]
    capacity = slots // 4
    step = 256
    row = lax.broadcasted_iota(jnp.int32, (slots, lanes), 0).astype(jnp.float32)
    shift = (lax.broadcasted_iota(jnp.int32, (1, lanes), 1) // tokens * capacity).astype(
        jnp.float32
    )

    def place(source, m, which):
        ranks = source[planes[m], pl.ds(which, 1), :]
        target = jnp.where(ranks > 0.5, ranks + (shift - 1.0), -1.0)
        return row == target

    def scale(source, m, which):
        weights = source[planes[m], pl.ds(count + which, 1), :]
        return jnp.sum(
            jnp.where(place(source, m, which), weights, 0.0), axis=1, keepdims=True
        )

    def picking(m):
        return jnp.concatenate(
            [jnp.where(place(meta_z, m, which), 1.0, 0.0) for which in (s, near)], axis=0
        )

    handed = []

    def hand_over():
        for k, owner in enumerate((tx, ty, td)):
            piece = tok.at[owner, z]
            handed.append(go(piece, piece, hos.at[k], hor.at[k], z_devs[1]))

    def complete(m):
        if m == 1:
            for copy in handed:
                copy.wait_recv()
        else:
            for h in (0, 1):
                for copy in forwarded[m, h]:
                    copy.wait_recv()

    def pick(m):
        chooser = picking(m)
        lengths = inverse[planes[m]]
        lengths = jnp.concatenate([lengths[0, 0:1], lengths[1, 0:1]], axis=1)
        factor = jnp.sum(chooser * lengths, axis=1, keepdims=True)
        chooser = chooser.astype(jnp.bfloat16)
        for owner in range(4):
            for k in range(width // step):
                rows_in = tok[owner, planes[m], :, k * step : (k + 1) * step]
                found = jnp.dot(chooser, rows_in, preferred_element_type=jnp.float32)
                found = (found * factor).astype(xs.dtype)
                columns = slice(owner * width + k * step, owner * width + (k + 1) * step)
                xs[m, 0:slots, columns] = found[:slots]
                xo[m, :, columns] = found[slots:]
            if owner % 2:
                columns = pl.ds((owner - 1) * width, 2 * width)
                picks[m, owner // 2] = go(
                    xo.at[m, :, columns],
                    xs.at[m, pl.ds(slots, slots), columns],
                    xs_s.at[m, owner // 2],
                    xs_r.at[m, owner // 2],
                    n_dev,
                )

    def picked(m):
        for k in (0, 1):
            picks[m, k].wait_recv()

    def rise(m, begin, end):
        @pl.loop(begin, end)
        def _(k):
            columns = pl.ds(pl.multiple_of(k * step, step), step)
            x = xs[m]
            g = jnp.dot(x, gate[:, columns], preferred_element_type=jnp.float32)
            u = jnp.dot(x, up[:, columns], preferred_element_type=jnp.float32)
            hidden[:, columns] = (jax.nn.silu(g) * u).astype(hidden.dtype)

    total_steps = gate.shape[1] // step

    def fall(m):
        factor_mine = scale(meta_z, m, s)
        factor_near = scale(meta_p, m, s)
        wide = 512

        for side in (0, 1):

            @pl.loop(side * model // (2 * wide), (side + 1) * model // (2 * wide))
            def _(k):
                columns = pl.ds(pl.multiple_of(k * wide, wide), wide)
                share = jnp.dot(hidden[...], down[:, columns], preferred_element_type=jnp.float32)
                po[m, 0:slots, columns] = (share[:slots] * factor_mine).astype(po.dtype)
                ps[m, :, columns] = (share[slots:] * factor_near).astype(ps.dtype)

            columns = pl.ds(side * (model // 2), model // 2)
            parts[m, side] = go(
                ps.at[m, :, columns],
                po.at[m, pl.ds(slots, slots), columns],
                ps_s.at[m, side],
                ps_r.at[m, side],
                n_dev,
            )

    def expand(m):
        spreader = picking(m).T.astype(jnp.bfloat16)
        for owner in range(4):
            if owner % 2 == 0:
                parts[m, owner // 2].wait_recv()
            holds = jnp.where(t == owner, 1.0, 0.0)
            for k in range(width // step):
                columns = slice(owner * width + k * step, owner * width + (k + 1) * step)
                found = jnp.dot(spreader, po[m, :, columns], preferred_element_type=jnp.float32)
                if m == 0:
                    found += holds * proj[:, k * step : (k + 1) * step].astype(jnp.float32)
                rt[m, :, :, columns] = found.astype(rt.dtype).reshape(4, tokens, step)

    low, high = pl.ds(0, own // 2), pl.ds(own // 2, own // 2)

    def side_of(m, c):
        if c is None:
            return m, pl.ds(0, model)
        return m if c == 0 else {1: 4, 0: 5, 3: 6}[m], pl.ds(c * (model // 2), model // 2)

    def reduce_far(m, c=None):
        k, columns = side_of(m, c)
        firsts[m, c] = (
            go(
                rt.at[m, td, low, columns], bx1.at[m, 1, :, columns],
                rs.at[k, 0], rr.at[k, 0], x_dev,
            ),
            go(
                rt.at[m, td, high, columns], by1.at[m, 1, :, columns],
                rs.at[k, 1], rr.at[k, 1], y_dev,
            ),
        )

    def reduce_side(m, c=None):
        k, columns = side_of(m, c)
        firsts[m, c] += (
            go(
                rt.at[m, tx, low, columns], bx1.at[m, 0, :, columns],
                rs.at[k, 2], rr.at[k, 2], x_dev,
            ),
            go(
                rt.at[m, ty, high, columns], by1.at[m, 0, :, columns],
                rs.at[k, 3], rr.at[k, 3], y_dev,
            ),
        )

    def reduce_one(m):
        reduce_far(m)
        reduce_side(m)

    def wide_sum(*pieces):
        result = pieces[0].astype(jnp.float32)
        for piece in pieces[1:]:
            result = result + piece.astype(jnp.float32)
        return result

    def reduce_two(m, c=None):
        k, columns = side_of(m, c)
        firsts[m, c][0].wait_recv()
        mid[m, 0, :, columns] = wide_sum(
            rt[m, ty, low, columns], bx1[m, 1, :, columns]
        ).astype(mid.dtype)
        to_side = go(
            mid.at[m, 0, :, columns], by2.at[m, :, columns], rs.at[k, 4], rr.at[k, 4], y_dev
        )
        firsts[m, c][1].wait_recv()
        mid[m, 1, :, columns] = wide_sum(
            rt[m, tx, high, columns], by1[m, 1, :, columns]
        ).astype(mid.dtype)
        seconds[m, c] = (
            to_side,
            go(mid.at[m, 1, :, columns], bx2.at[m, :, columns], rs.at[k, 5], rr.at[k, 5], x_dev),
        )

    home_two = (jnp.where(inner, z_devs[2][0], z_devs[1][0]), t)

    def reduce_three(m, c=None):
        k, columns = side_of(m, c)

        def home(rows_at, value, h):
            if m == 0:
                home_sum[rows_at, columns] += value
                return None
            if m == 3:

                @pl.when(inner)
                def _():
                    if not c:
                        homes[2, None][h].wait_recv()
                    joint = value + zin[2, rows_at, columns].astype(jnp.float32)
                    sz[m, rows_at, columns] = joint.astype(sz.dtype)

                @pl.when(outer)
                def _():
                    sz[m, rows_at, columns] = value.astype(sz.dtype)

            else:
                sz[m, rows_at, columns] = value.astype(sz.dtype)
            return go(
                sz.at[m, rows_at, columns], zin.at[m, rows_at, columns],
                zbs.at[k, h], zbr.at[k, h], home_two if m == 2 else z_devs[m],
            )

        firsts[m, c][2].wait_recv()
        seconds[m, c][0].wait_recv()
        lower = home(
            low,
            wide_sum(rt[m, t, low, columns], bx1[m, 0, :, columns], by2[m, :, columns]),
            0,
        )
        firsts[m, c][3].wait_recv()
        seconds[m, c][1].wait_recv()
        upper = home(
            high,
            wide_sum(rt[m, t, high, columns], by1[m, 0, :, columns], bx2[m, :, columns]),
            1,
        )
        homes[m, c] = (lower, upper)

    def share_squares():
        return [
            go(squares, squares_in.at[t], qs.at[k], qr.at[k], device)
            for k, device in enumerate((x_dev, y_dev, d_dev))
        ]

    def invert(square_copies):
        for copy in square_copies:
            copy.wait_recv()
        total = (squares[...] + squares_in[tx]) + (squares_in[ty] + squares_in[td])
        inverse[z] = lax.rsqrt(total * (1.0 / model) + EPS)
        return {
            m: go(inverse.at[z], inverse.at[z], qs.at[2 + m], qr.at[2 + m], z_devs[m])
            for m in (1, 2, 3)
        }

    passes[0, 0].wait_recv()
    passes[0, 1].wait_recv()
    sums = finish(0)
    send(0, 0)
    depart(0)
    record(0, sums)
    passes[1, 0].wait_recv()
    passes[1, 1].wait_recv()
    sums = finish(1)
    send(0, 1)
    depart(1)
    record(1, sums)
    square_copies = share_squares()
    for copy in meta_z_copies:
        copy.wait_recv()
    meta_near = go(meta_z, meta_p, ms.at[6], mr.at[6], n_dev)
    forward(0, 0)
    arrive(1, 0)
    relay(1, 0)
    relay(3, 0, False)
    forward(0, 1)
    arrive(1, 1)
    relay(1, 1)
    relay(3, 1, False)
    inverse_copies = invert(square_copies)
    arrive(2, 0)
    relay(2, 0)
    send(2, 0)
    complete(0)
    pick(0)
    arrive(2, 1)
    relay(2, 1)
    send(2, 1)
    hand_over()
    picked(0)
    for copy in loads[5:8]:
        copy.wait()
    rise(0, 0, 2)
    forward(2, 0)
    rise(0, 2, total_steps)
    forward(2, 1)

    @pl.when(outer)
    def _():
        arrive(3, 0)

    send(3, 0)
    meta_near.wait_recv()
    fall(0)

    @pl.when(outer)
    def _():
        arrive(3, 1)

    send(3, 1)
    expand(0)
    complete(2)
    inverse_copies[2].wait_recv()
    pick(2)
    picked(2)
    rise(2, 0, 2)
    forward(3, 0)
    rise(2, 2, total_steps)
    forward(3, 1)
    reduce_far(0, 0)
    reduce_far(0, 1)
    fall(2)
    complete(3)
    inverse_copies[3].wait_recv()
    pick(3)
    expand(2)
    reduce_one(2)
    picked(3)
    rise(3, 0, total_steps)
    reduce_two(2)
    reduce_side(0, 0)
    fall(3)
    complete(1)
    inverse_copies[1].wait_recv()
    pick(1)
    expand(3)
    reduce_far(3, 0)
    reduce_side(3, 0)
    reduce_far(3, 1)
    picked(1)
    rise(1, 0, 1)
    reduce_three(2)
    rise(1, 1, total_steps - 1)
    reduce_two(3, 0)
    reduce_side(3, 1)
    rise(1, total_steps - 1, total_steps)
    fall(1)
    reduce_two(3, 1)
    drained = len(copies)
    expand(1)
    reduce_far(1, 0)
    reduce_side(1, 0)
    reduce_far(1, 1)
    reduce_three(3, 0)
    reduce_three(3, 1)
    reduce_two(1, 0)
    reduce_side(1, 1)
    reduce_two(1, 1)
    reduce_side(0, 1)
    reduce_two(0, 0)
    reduce_two(0, 1)
    reduce_three(1, 0)
    for copy in copies[: drained - 8]:
        copy.wait_send()
    near_copy.wait_send()
    for h in (0, 1):
        out_one[h].wait_send()

    @pl.when(inner)
    def _():
        for h in (0, 1):
            out_three[h].wait_send()
            for m in (1, 2, 3):
                relay_copy(m, h).wait_send()

    @pl.when(has_far)
    def _():
        far_copy.wait_send()

    reduce_three(1, 1)
    @pl.when(outer)
    def _():
        for copy in homes[2, None]:
            copy.wait_recv()

    for copy in homes[3, 0] + homes[3, 1]:
        copy.wait_recv()
    home_sum[...] = (
        res[...].astype(jnp.float32)
        + jnp.where(outer, zin[2].astype(jnp.float32), 0.0)
        + zin[3].astype(jnp.float32)
    )
    reduce_three(0, 0)
    reduce_three(0, 1)
    for c in (0, 1):
        for copy in homes[1, c]:
            copy.wait_recv()
    out_ref[...] = (home_sum[...] + zin[1].astype(jnp.float32)).astype(out_ref.dtype)
    for copy in copies[drained - 8 :]:
        copy.wait_send()


def layer(
    queries, keys, values, sink_logit, out_weight, residual, norm_gain, routes, route_weights,
    gate_weight, up_weight, down_weight, capacity,
):
    rows, depth = queries.shape
    kind = queries.dtype
    width = out_weight.shape[1]
    tokens, model = residual.shape
    count = lax.axis_size("sp")
    slots = 4 * capacity
    anywhere = pl.BlockSpec(memory_space=pl.ANY)
    vmem = pl.BlockSpec(memory_space=pltpu.VMEM)
    dma = pltpu.SemaphoreType.DMA
    two = dma((4, 2))
    lanes = 4 * tokens
    return pl.pallas_call(
        layer_kernel,
        out_shape=pltpu.VMEM(residual.shape, kind),
        in_specs=[anywhere] * 12,
        out_specs=vmem,
        scratch_shapes=[
            pltpu.SMEM(sink_logit.shape, jnp.float32),
            pltpu.VMEM((1, model), jnp.float32),
            pltpu.VMEM((2, tokens), jnp.int32),
            pltpu.VMEM((2, tokens), jnp.float32),
            pltpu.VMEM(queries.shape, kind),
            pltpu.VMEM((2 * rows, 2 * keys.shape[1]), kind),
            pltpu.VMEM(out_weight.shape, kind),
            pltpu.VMEM(residual.shape, kind),
            pltpu.VMEM((4, tokens, width), kind),
            pltpu.VMEM((4, rows, depth), kind),
            pltpu.VMEM((2, rows // 2, width), jnp.float32),
            pltpu.VMEM((rows, width), kind),
            pltpu.VMEM(gate_weight.shape, kind),
            pltpu.VMEM(up_weight.shape, kind),
            pltpu.VMEM(down_weight.shape, kind),
            pltpu.VMEM((2 * count, lanes), jnp.float32),
            pltpu.VMEM((4, 2 * count, lanes), jnp.float32),
            pltpu.VMEM((4, 2 * count, lanes), jnp.float32),
            pltpu.VMEM((4, 2 * count, lanes), jnp.float32),
            pltpu.VMEM((2, 8, rows // 2), jnp.float32),
            pltpu.VMEM((4, 2, 8, rows // 2), jnp.float32),
            pltpu.VMEM((4, 2, 8, rows // 2), jnp.float32),
            pltpu.VMEM((4, 4, rows, width), kind),
            pltpu.VMEM((4, 2 * slots, model), kind),
            pltpu.VMEM((4, slots, model), kind),
            pltpu.VMEM((2 * slots, gate_weight.shape[1]), kind),
            pltpu.VMEM((4, 2 * slots, model), kind),
            pltpu.VMEM((4, slots, model), kind),
            pltpu.VMEM((4, 4, tokens, model), kind),
            pltpu.VMEM((4, 2, tokens // 2, model), kind),
            pltpu.VMEM((4, 2, tokens // 2, model), kind),
            pltpu.VMEM((4, tokens // 2, model), kind),
            pltpu.VMEM((4, tokens // 2, model), kind),
            pltpu.VMEM((4, 2, tokens // 2, model), kind),
            pltpu.VMEM((4, tokens, model), kind),
            pltpu.VMEM((4, tokens, model), kind),
            pltpu.VMEM(residual.shape, jnp.float32),
            dma((12,)),
            dma((2,)), dma((2,)),
            dma((12,)), dma((12,)),
            dma((3,)), dma((3,)),
            dma((7,)), dma((7,)),
            dma((6,)), dma((6,)),
            dma((7, 2)), dma((4, 2)),
            dma((4, 8)), dma((4, 8)), two, two, two, two, dma((7, 6)), dma((7, 6)),
            dma((7, 2)), dma((7, 2)), dma((3,)), dma((3,)),
        ],
        compiler_params=pltpu.CompilerParams(
            collective_id=0, has_side_effects=True, vmem_limit_bytes=60 * 1024 * 1024
        ),
    )(
        queries, keys, values, sink_logit, out_weight, residual, norm_gain.reshape(1, -1),
        routes.T, route_weights.T,
        gate_weight, up_weight, down_weight,
    )


def with_halo(block, sides, width):
    for axis, dim in sides:
        count = lax.axis_size(axis)
        forward = [(i, i + 1) for i in range(count - 1)]
        backward = [(target, source) for source, target in forward]
        low = lax.ppermute(
            lax.slice_in_dim(block, block.shape[dim] - width, None, axis=dim), axis, forward
        )
        high = lax.ppermute(lax.slice_in_dim(block, 0, width, axis=dim), axis, backward)
        block = jnp.concatenate([low, block, high], axis=dim)
    return block


def make_band(extended, length):
    blocks = length // WINDOW
    pieces = [
        lax.slice_in_dim(extended, offset * WINDOW, offset * WINDOW + length, axis=0).reshape(
            blocks, WINDOW, -1
        )
        for offset in range(3)
    ]
    return jnp.concatenate(pieces, axis=1)


def attend_local(queries, keys, values, sink_logit):
    length = queries.shape[0]
    groups = keys.shape[1] // HEAD
    repeat = HEADS // KV_HEADS
    blocks = length // WINDOW
    joined = jnp.concatenate([keys, values], axis=1)
    extended = with_halo(joined, (("sp", 0),), WINDOW)
    banded = make_band(extended, length)
    key_band = banded[..., : groups * HEAD].reshape(blocks, 3 * WINDOW, groups, HEAD)
    value_band = banded[..., groups * HEAD :].reshape(blocks, 3 * WINDOW, groups, HEAD)
    query_blocks = queries.reshape(blocks, WINDOW, groups, repeat, HEAD)
    scores = jnp.einsum(
        "nqgrd,nkgd->ngrqk", query_blocks, key_band, preferred_element_type=jnp.float32
    ) * HEAD ** (-0.5)
    near = jnp.abs(jnp.arange(WINDOW)[:, None] + WINDOW - jnp.arange(3 * WINDOW)[None, :]) <= WINDOW
    first_token = lax.axis_index("sp") * length
    key_pos = (
        first_token + (jnp.arange(blocks)[:, None] - 1) * WINDOW + jnp.arange(3 * WINDOW)[None, :]
    )
    inside = (key_pos >= 0) & (key_pos < length * lax.axis_size("sp"))
    valid = near[None, None, None, :, :] & inside[:, None, None, None, :]
    sinks = sink_logit.reshape(1, groups, repeat, 1, 1)
    masked = jnp.where(valid, scores, NEGATIVE)
    top = jnp.maximum(jnp.max(masked, axis=-1, keepdims=True), sinks)
    probs = jnp.exp(masked - top)
    denom = jnp.sum(probs, axis=-1, keepdims=True) + jnp.exp(sinks - top)
    weights = (probs / denom).astype(jnp.bfloat16)
    output = jnp.einsum(
        "ngrqk,nkgd->nqgrd", weights, value_band, preferred_element_type=jnp.float32
    )
    return output.astype(jnp.bfloat16).reshape(length, groups * repeat * HEAD)


def local(
    queries,
    keys,
    values,
    sink_logit,
    out_weight,
    residual,
    norm_gain,
    routes,
    route_weights,
    gate_weight,
    up_weight,
    down_weight,
):
    capacity = max(2, 4 * residual.shape[0] // lax.axis_size("sp"))
    in_plane = (
        lax.axis_size("tp") == 4
        and lax.axis_size("sp") == 8
        and capacity % 32 == 0
        and gate_weight.shape[2] % 256 == 0
        and queries.shape[0] == 2 * WINDOW
        and residual.shape[0] == 64
    )
    if in_plane:
        return layer(
            queries, keys, values, sink_logit, out_weight, residual, norm_gain, routes,
            route_weights, gate_weight[0], up_weight[0], down_weight[0], capacity,
        )
    attention = attend_local(queries, keys, values, sink_logit)
    columns = jnp.dot(
        lax.all_gather(attention, "tp", axis=1, tiled=True),
        out_weight,
        preferred_element_type=jnp.float32,
    )
    projected = lax.all_to_all(
        columns.astype(jnp.bfloat16), "tp", split_axis=0, concat_axis=1, tiled=True
    )
    hidden_state = residual.astype(jnp.float32) + projected.astype(jnp.float32)
    inverse = lax.rsqrt(jnp.mean(hidden_state * hidden_state, axis=-1, keepdims=True) + EPS)
    normed = (hidden_state * inverse * norm_gain).astype(jnp.bfloat16)
    sp_count = lax.axis_size("sp")
    tok_rows = residual.shape[0]
    width = residual.shape[1]
    slot_total = sp_count * capacity
    expert_ids = routes.reshape(-1)
    onehot = (expert_ids[:, None] == jnp.arange(sp_count, dtype=jnp.int32)[None, :]).astype(
        jnp.int32
    )
    earlier = jnp.cumsum(onehot, axis=0) - onehot
    rank = jnp.sum(earlier * onehot, axis=1)
    slots = expert_ids * capacity + rank
    placing = (slots[:, None] == jnp.arange(slot_total, dtype=jnp.int32)[None, :]).astype(
        jnp.bfloat16
    )
    placing = placing.reshape(tok_rows, 2, slot_total)
    first_place = placing[:, 0]
    second_place = placing[:, 1]
    sending = jnp.einsum(
        "ts,td->sd", first_place + second_place, normed, preferred_element_type=jnp.float32
    )
    sending = sending.astype(jnp.bfloat16).reshape(sp_count, capacity, width)
    piece = lax.all_gather(
        lax.all_to_all(sending, "sp", split_axis=0, concat_axis=0, tiled=True),
        "tp",
        axis=0,
        tiled=True,
    )
    flat = piece.reshape(-1, piece.shape[-1])
    gate = jnp.dot(flat, gate_weight[0], preferred_element_type=jnp.float32)
    upward = jnp.dot(flat, up_weight[0], preferred_element_type=jnp.float32)
    hidden = (jax.nn.silu(gate) * upward).astype(jnp.bfloat16)
    partial_value = jnp.dot(hidden, down_weight[0], preferred_element_type=jnp.float32)
    partial_value = partial_value.reshape(piece.shape[:-1] + (down_weight.shape[-1],))
    returned = lax.all_to_all(
        lax.psum_scatter(
            partial_value.astype(jnp.bfloat16), "tp", scatter_dimension=0, tiled=True
        ),
        "sp",
        split_axis=0,
        concat_axis=0,
        tiled=True,
    )
    gathered_back = returned.reshape(slot_total, width)
    first_pick = jnp.dot(first_place, gathered_back, preferred_element_type=jnp.float32)
    second_pick = jnp.dot(second_place, gathered_back, preferred_element_type=jnp.float32)
    mixture = route_weights[:, 0:1] * first_pick + route_weights[:, 1:2] * second_pick
    return (hidden_state + mixture).astype(jnp.bfloat16)


def solution(mesh):
    in_specs = (
        P("sp", "tp"),
        P("sp", "tp"),
        P("sp", "tp"),
        P("tp"),
        P(None, "tp"),
        P(("sp", "tp"), None),
        P(),
        P(("sp", "tp"), None),
        P(("sp", "tp"), None),
        P("sp", None, "tp"),
        P("sp", None, "tp"),
        P("sp", "tp", None),
    )
    out_specs = P(("sp", "tp"), None)
    return jax.shard_map(local, mesh=mesh, in_specs=in_specs, out_specs=out_specs, check_vma=False)
```

```python
import math

import jax
import jax.numpy as jnp
from jax import lax
from jax.experimental import pallas as pl
from jax.experimental.pallas import tpu as pltpu
from jax.sharding import PartitionSpec as P

HEADS = 32
KV_HEADS = 16
HEAD = 64
WINDOW = 128


EPS = 1e-06
NEGATIVE = -1e30
MESH = pl.DeviceIdType.MESH


def plane():
    t = lax.axis_index("tp")
    tx = t + 1 - 2 * lax.rem(t, 2)
    ty = lax.rem(t + 2, 4)
    return t, tx, ty, 3 - t


def remote(src, dst, send, recv, device):
    return pltpu.make_async_remote_copy(
        src_ref=src,
        dst_ref=dst,
        send_sem=send,
        recv_sem=recv,
        device_id=device,
        device_id_type=MESH,
    )


def flipped(index, mask):
    result = index
    bit = 1
    while bit <= mask:
        if mask & bit:
            result = result + bit * (1 - 2 * lax.rem(index // bit, 2))
        bit *= 2
    return result


def layer_kernel(
    q_hbm, k_hbm, v_hbm, sink_hbm, w_hbm, res_hbm, gain_hbm, routes_hbm, route_weights_hbm,
    gate_hbm, up_hbm, down_hbm, out_ref,
    sink_ref, gain_ref, routes_ref, route_weights_ref, q, kv, w, res, res_in, buf, acc, proj, gate, up, down,
    meta, meta_in, meta_z, meta_p, squares, squares_in, inverse, tok, xs, xo, hidden, po, ps, rt,
    bx1, by1, bx2, by2, mid, sz, zin, home_sum,
    load, sends, hs, hr, gr, ar, mr, qr, zs, zr, dr, xs_r, ps_r, rr, zbr, hor,
):
    s = lax.axis_index("sp")
    t, tx, ty, td = plane()
    last = lax.axis_size("sp") - 1
    rows, depth = q.shape
    half = rows // 2
    groups = k_hbm.shape[1] // HEAD
    kept = groups * HEAD
    odd = lax.rem(s, 2)
    near = s + 1 - 2 * odd
    has_far = jnp.logical_and(s != 0, s != last)
    far = jnp.where(has_far, s - 1 + 2 * odd, near)
    x_dev, y_dev, d_dev, n_dev, f_dev = (s, tx), (s, ty), (s, td), (near, t), (far, t)
    z = s // 2
    planes = [flipped(z, m) for m in range(4)]
    z_devs = [(2 * planes[m] + odd, t) for m in range(4)]
    inner = jnp.logical_or(z == 1, z == 2)
    outer = jnp.logical_not(inner)
    middle = pl.ds(half, rows)
    loads = [
        pltpu.make_async_copy(source, target, load.at[k])
        for k, (source, target) in enumerate(
            (
                (k_hbm, kv.at[middle, pl.ds(0, kept)]),
                (v_hbm, kv.at[middle, pl.ds(kept, kept)]),
                (q_hbm, q),
                (w_hbm, w),
                (res_hbm, res),
                (gate_hbm, gate),
                (up_hbm, up),
                (down_hbm, down),
                (sink_hbm, sink_ref),
                (routes_hbm, routes_ref),
                (route_weights_hbm, route_weights_ref),
                (gain_hbm, gain_ref),
            )
        )
    ]
    barrier = pltpu.get_barrier_semaphore()
    for device in [x_dev, y_dev, d_dev, n_dev] + z_devs[1:]:
        pl.semaphore_signal(barrier, inc=1, device_id=device, device_id_type=MESH)

    @pl.when(has_far)
    def _():
        pl.semaphore_signal(barrier, inc=1, device_id=f_dev, device_id_type=MESH)

    for copy in loads[:5] + loads[8:]:
        copy.start()

    @pl.when(has_far)
    def _():
        pl.semaphore_wait(barrier, 8)

    @pl.when(jnp.logical_not(has_far))
    def _():
        pl.semaphore_wait(barrier, 7)

    def aligned(value, size):
        return pl.ds(pl.multiple_of(value, size), size)

    near_src = aligned(2 * half - half * odd, half)
    near_dst = aligned(3 * half * odd, half)
    far_src = aligned(half + half * odd, half)
    far_dst = aligned(3 * half * (1 - odd), half)
    near_copy = remote(kv.at[near_src], kv.at[near_dst], hs.at[0], hr.at[0], n_dev)
    far_copy = remote(kv.at[far_src], kv.at[far_dst], hs.at[1], hr.at[1], f_dev)
    loads[0].wait()
    loads[1].wait()

    @pl.when(has_far)
    def _():
        far_copy.start()

    near_copy.start()
    amounts = [0] * sends.shape[0]

    def go(source, target, group, recv, device):
        copy = remote(source, target, sends.at[group], recv, device)
        copy.start()
        amounts[group] += math.prod(source.shape) * source.dtype.itemsize
        return copy

    def settle(group):
        line = tok.shape[3] * tok.dtype.itemsize
        lines = amounts[group] // line
        if lines <= tok.shape[2]:
            whole = tok.at[0, 0, pl.ds(0, lines)]
        else:
            whole = tok.at[0, pl.ds(0, lines // tok.shape[2])]
        remote(whole, whole, sends.at[group], hr.at[0], x_dev).wait_send()

    own, model = res.shape
    width = w.shape[1]
    loads[4].wait()
    res_copies = [
        go(
            res.at[:, aligned(owner * width, width)],
            res_in.at[t],
            1,
            ar.at[k],
            device,
        )
        for k, (owner, device) in enumerate(((tx, x_dev), (ty, y_dev), (td, d_dev)))
    ]
    res_in[t] = res[:, aligned(t * width, width)]
    count, lanes = meta.shape[0] // 2, meta.shape[1]
    tokens = lanes // 4
    expert = lax.broadcasted_iota(jnp.int32, (count, lanes), 0)
    lane = lax.broadcasted_iota(jnp.int32, (count, lanes), 1)
    mine_lane = jnp.logical_and(lane >= t * tokens, lane < (t + 1) * tokens)
    for copy in loads[8:]:
        copy.wait()
    routes = jnp.concatenate([routes_ref[...]] * 4, axis=1)
    route_weights = jnp.concatenate([route_weights_ref[...]] * 4, axis=1)
    hit_one = routes[0:1, :] == expert
    hit = jnp.logical_and(mine_lane, jnp.logical_or(hit_one, routes[1:2, :] == expert))
    chosen = jnp.where(hit, 1.0, 0.0)
    before = lax.broadcasted_iota(jnp.int32, (lanes, lanes), 0) <= lax.broadcasted_iota(
        jnp.int32, (lanes, lanes), 1
    )
    rank = jnp.dot(
        chosen.astype(jnp.bfloat16),
        jnp.where(before, 1.0, 0.0).astype(jnp.bfloat16),
        preferred_element_type=jnp.float32,
    )
    meta[0:count] = chosen * rank
    meta[count : 2 * count] = chosen * jnp.where(
        hit_one, route_weights[0:1, :], route_weights[1:2, :]
    )
    meta_copies = [
        go(meta, meta_in.at[t], 2, mr.at[k], device)
        for k, device in enumerate((x_dev, y_dev, d_dev))
    ]

    for copy in loads[5:8]:
        copy.start()

    @pl.when(jnp.logical_not(has_far))
    def _():
        kv[aligned(3 * half * odd, half)] = jnp.zeros((half, kv.shape[1]), kv.dtype)

    loads[2].wait()
    span = 3 * half
    query = lax.broadcasted_iota(jnp.int32, (2 * half, span), 0)
    query = jnp.where(query >= half, query - half, query)
    key = lax.broadcasted_iota(jnp.int32, (2 * half, span), 1)
    band = jnp.abs(query + half - key) <= WINDOW
    upper = lax.broadcasted_iota(jnp.int32, (2 * half, 1), 0) < half

    def attend(b, first, end):
        valid = jnp.logical_and(
            band,
            jnp.logical_and(
                key >= jnp.where(2 * s + b == 0, half, 0),
                key < jnp.where(2 * s + b == 2 * last + 1, 2 * half, span),
            ),
        )
        keys_at = pl.ds(pl.multiple_of(b * half, half), span)
        mine = aligned(b * half, half)
        for g in range(first, end):
            pair = q[mine, 2 * g * HEAD : 2 * (g + 1) * HEAD]
            stacked = jnp.concatenate([pair[:, :HEAD], pair[:, HEAD:]], axis=0)
            scores = lax.dot_general(
                stacked,
                kv[keys_at, g * HEAD : (g + 1) * HEAD],
                (((1,), (1,)), ((), ())),
                preferred_element_type=jnp.float32,
            ) * HEAD ** (-0.5)
            sink = jnp.where(upper, sink_ref[2 * g], sink_ref[2 * g + 1])
            masked = jnp.where(valid, scores, NEGATIVE)
            top = jnp.maximum(jnp.max(masked, axis=-1, keepdims=True), sink)
            probs = jnp.exp(masked - top)
            denom = jnp.sum(probs, axis=-1, keepdims=True) + jnp.exp(sink - top)
            weights = (probs * (1.0 / denom)).astype(jnp.bfloat16)
            output = jnp.dot(
                weights,
                kv[keys_at, kept + g * HEAD : kept + (g + 1) * HEAD],
                preferred_element_type=jnp.float32,
            )
            joined = jnp.concatenate([output[:half], output[half:]], axis=1)
            buf[t, mine, 2 * g * HEAD : 2 * (g + 1) * HEAD] = joined.astype(buf.dtype)

    blocks = (1 - odd, odd)
    parts_of = [aligned(b * half, half) for b in blocks]

    wide_piece = depth // 2

    def part(owner, h, j):
        return buf.at[owner, parts_of[h], pl.ds(j * wide_piece, wide_piece)]

    spreads, passes = {}, {}

    def spread(h, j):
        piece = part(t, h, j)
        k = 4 * h + 2 * j
        spreads[h, j] = (
            go(piece, piece, 0, gr.at[k], x_dev),
            go(piece, piece, 0, gr.at[k + 1], y_dev),
        )

    def hand_on(h, j):
        spreads[h, j][j].wait_recv()
        piece = part(ty if j else tx, h, j)
        k = 8 + 2 * h + j
        passes[h, j] = go(piece, piece, 0, gr.at[k], x_dev if j else y_dev)

    near_copy.wait_recv()
    attend(blocks[0], 0, groups // 2)
    spread(0, 0)
    attend(blocks[0], groups // 2, groups)
    spread(0, 1)

    @pl.when(has_far)
    def _():
        far_copy.wait_recv()

    attend(blocks[1], 0, groups // 2)
    spread(1, 0)
    attend(blocks[1], groups // 2, groups)
    spread(1, 1)
    for copy in meta_copies:
        copy.wait_recv()
    meta_z[z] = (meta[...] + meta_in[tx]) + (meta_in[ty] + meta_in[td])
    meta_z_copies = [
        go(meta_z.at[z], meta_z.at[z], 2, mr.at[2 + m], z_devs[m]) for m in (1, 2, 3)
    ]
    loads[3].wait()

    def product(h, owner):
        weight = w[pl.ds(pl.multiple_of(owner * depth, depth), depth)]
        return jnp.dot(buf[owner, parts_of[h]], weight, preferred_element_type=jnp.float32)

    def gather(h):
        hand_on(h, 0)
        acc[h] = product(h, t)
        hand_on(h, 1)
        spreads[h, 1][0].wait_recv()
        acc[h] += product(h, tx)
        spreads[h, 0][1].wait_recv()
        acc[h] += product(h, ty)

    gather(0)
    for copy in res_copies:
        copy.wait_recv()
    gather(1)
    gain = gain_ref[:, aligned(t * width, width)]

    def finish(h):
        projected = (acc[h] + product(h, td)).astype(proj.dtype)
        proj[parts_of[h]] = projected
        pair = res_in[pl.ds(2 * blocks[h], 2)].reshape(half, width)
        value = pair.astype(jnp.float32) + projected.astype(jnp.float32)
        tok[t, z, parts_of[h]] = (value * gain).astype(tok.dtype)
        return jnp.sum(value * value, axis=-1, keepdims=True)

    def record(h, sums):
        squares[blocks[h]] = jnp.broadcast_to(sums, (half, half)).T[: squares.shape[1]]

    def own_block(h):
        return tok.at[t, z, parts_of[h]]

    z_in = {
        (m, h): remote(
            own_block(h), tok.at[t, planes[m], parts_of[h]], zs.at[m, h], zr.at[m, h], z_devs[m]
        )
        for m in (1, 2, 3)
        for h in (0, 1)
    }

    out_one = [remote(own_block(h), own_block(h), zs.at[1, h], zr.at[1, h], z_devs[1]) for h in (0, 1)]
    out_three = [remote(own_block(h), own_block(h), zs.at[3, h], zr.at[3, h], z_devs[3]) for h in (0, 1)]

    def relay_copy(m, h):
        piece = tok.at[t, planes[m], parts_of[h]]
        lands, device = ((2, z_devs[3]), None, (3, z_devs[1]), (2, z_devs[1]))[
            {1: 0, 2: 2, 3: 3}[m]
        ]
        return remote(piece, piece, zs.at[3 + m, h], zr.at[lands, h], device)

    def depart(h):
        out_one[h].start()

        @pl.when(inner)
        def _():
            out_three[h].start()

    sent, parts, firsts, seconds, homes = {}, {}, {}, {}, {}

    def arrive(m, h):
        z_in[m, h].wait_recv()

    def relay(m, h, waited=True):
        @pl.when(inner)
        def _():
            if not waited:
                arrive(m, h)
            relay_copy(m, h).start()

    def send(m, h):
        piece = tok.at[t, planes[m], parts_of[h]]
        k = max(m - 1, 0)
        sent[m, h] = (
            go(piece, piece, 5 + k, dr.at[k, 2 * h], x_dev),
            go(piece, piece, 5 + k, dr.at[k, 2 * h + 1], y_dev),
        )

    def forward(m, h):
        k = max(m - 1, 0)
        sent[m, h][0].wait_recv()
        piece = tok.at[tx, planes[m], aligned(blocks[h] * half, half // 2)]
        go(piece, piece, 5 + k, dr.at[k, 4], y_dev)
        sent[m, h][1].wait_recv()
        piece = tok.at[ty, planes[m], aligned(blocks[h] * half + half // 2, half // 2)]
        go(piece, piece, 5 + k, dr.at[k, 4], x_dev)

    slots = xo.shape[1]
    capacity = slots // 4
    step = 256
    row = lax.broadcasted_iota(jnp.int32, (slots, lanes), 0).astype(jnp.float32)
    shift = (lax.broadcasted_iota(jnp.int32, (1, lanes), 1) // tokens * capacity).astype(
        jnp.float32
    )

    def place(source, m, which):
        ranks = source[planes[m], pl.ds(which, 1), :]
        target = jnp.where(ranks > 0.5, ranks + (shift - 1.0), -1.0)
        return row == target

    def scale(source, m, which):
        weights = source[planes[m], pl.ds(count + which, 1), :]
        return jnp.sum(
            jnp.where(place(source, m, which), weights, 0.0), axis=1, keepdims=True
        )

    def picking(m):
        return jnp.concatenate(
            [jnp.where(place(meta_z, m, which), 1.0, 0.0) for which in (s, near)], axis=0
        )

    def hand_over():
        for k, owner in enumerate((tx, ty, td)):
            piece = tok.at[owner, z]
            go(piece, piece, 4, hor, z_devs[1])

    def complete(m):
        if m == 1:
            whole, recv = tok.at[0, pl.ds(0, 3)], hor
        else:
            whole, recv = tok.at[0, 0], dr.at[max(m - 1, 0), 4]
        remote(whole, whole, sends.at[4], recv, x_dev).wait_recv()

    def pick(m):
        chooser = picking(m)
        lengths = inverse[planes[m]]
        lengths = jnp.concatenate([lengths[0, 0:1], lengths[1, 0:1]], axis=1)
        factor = jnp.sum(chooser * lengths, axis=1, keepdims=True)
        chooser = chooser.astype(jnp.bfloat16)
        for owner in range(4):
            for k in range(width // step):
                rows_in = tok[owner, planes[m], :, k * step : (k + 1) * step]
                found = jnp.dot(chooser, rows_in, preferred_element_type=jnp.float32)
                found = (found * factor).astype(xs.dtype)
                columns = slice(owner * width + k * step, owner * width + (k + 1) * step)
                xs[m, 0:slots, columns] = found[:slots]
                xo[m, :, columns] = found[slots:]
            if owner % 2:
                columns = pl.ds((owner - 1) * width, 2 * width)
                go(
                    xo.at[m, :, columns],
                    xs.at[m, pl.ds(slots, slots), columns],
                    8 + m,
                    xs_r.at[m],
                    n_dev,
                )

    def picked(m):
        whole = xo.at[m]
        remote(whole, whole, sends.at[8 + m], xs_r.at[m], n_dev).wait_recv()

    def rise(m, begin, end):
        @pl.loop(begin, end)
        def _(k):
            columns = pl.ds(pl.multiple_of(k * step, step), step)
            x = xs[m]
            g = jnp.dot(x, gate[:, columns], preferred_element_type=jnp.float32)
            u = jnp.dot(x, up[:, columns], preferred_element_type=jnp.float32)
            hidden[:, columns] = (jax.nn.silu(g) * u).astype(hidden.dtype)

    total_steps = gate.shape[1] // step

    def fall(m):
        factor_mine = scale(meta_z, m, s)
        factor_near = scale(meta_p, m, s)
        wide = 512

        for side in (0, 1):

            @pl.loop(side * model // (2 * wide), (side + 1) * model // (2 * wide))
            def _(k):
                columns = pl.ds(pl.multiple_of(k * wide, wide), wide)
                share = jnp.dot(hidden[...], down[:, columns], preferred_element_type=jnp.float32)
                po[m, 0:slots, columns] = (share[:slots] * factor_mine).astype(po.dtype)
                ps[m, :, columns] = (share[slots:] * factor_near).astype(ps.dtype)

            columns = pl.ds(side * (model // 2), model // 2)
            parts[m, side] = go(
                ps.at[m, :, columns],
                po.at[m, pl.ds(slots, slots), columns],
                12 + m,
                ps_r.at[m, side],
                n_dev,
            )

    def expand(m):
        spreader = picking(m).T.astype(jnp.bfloat16)
        for owner in range(4):
            if owner % 2 == 0:
                parts[m, owner // 2].wait_recv()
            holds = jnp.where(t == owner, 1.0, 0.0)
            for k in range(width // step):
                columns = slice(owner * width + k * step, owner * width + (k + 1) * step)
                found = jnp.dot(spreader, po[m, :, columns], preferred_element_type=jnp.float32)
                if m == 0:
                    found += holds * proj[:, k * step : (k + 1) * step].astype(jnp.float32)
                rt[m, :, :, columns] = found.astype(rt.dtype).reshape(4, tokens, step)

    low, high = pl.ds(0, own // 2), pl.ds(own // 2, own // 2)

    def side_of(m, c):
        if c is None:
            return m, pl.ds(0, model)
        return m if c == 0 else {1: 4, 0: 5, 3: 6}[m], pl.ds(c * (model // 2), model // 2)

    def reduce_far(m, c=None):
        k, columns = side_of(m, c)
        firsts[m, c] = (
            go(
                rt.at[m, td, low, columns], bx1.at[m, 1, :, columns],
                16 + m, rr.at[k, 0], x_dev,
            ),
            go(
                rt.at[m, td, high, columns], by1.at[m, 1, :, columns],
                16 + m, rr.at[k, 1], y_dev,
            ),
        )

    def reduce_side(m, c=None):
        k, columns = side_of(m, c)
        firsts[m, c] += (
            go(
                rt.at[m, tx, low, columns], bx1.at[m, 0, :, columns],
                16 + m, rr.at[k, 2], x_dev,
            ),
            go(
                rt.at[m, ty, high, columns], by1.at[m, 0, :, columns],
                16 + m, rr.at[k, 3], y_dev,
            ),
        )

    def reduce_one(m):
        reduce_far(m)
        reduce_side(m)

    def wide_sum(*pieces):
        result = pieces[0].astype(jnp.float32)
        for piece in pieces[1:]:
            result = result + piece.astype(jnp.float32)
        return result

    def reduce_two(m, c=None):
        k, columns = side_of(m, c)
        firsts[m, c][0].wait_recv()
        mid[m, 0, :, columns] = wide_sum(
            rt[m, ty, low, columns], bx1[m, 1, :, columns]
        ).astype(mid.dtype)
        to_side = go(
            mid.at[m, 0, :, columns], by2.at[m, :, columns], 16 + m, rr.at[k, 4], y_dev
        )
        firsts[m, c][1].wait_recv()
        mid[m, 1, :, columns] = wide_sum(
            rt[m, tx, high, columns], by1[m, 1, :, columns]
        ).astype(mid.dtype)
        seconds[m, c] = (
            to_side,
            go(mid.at[m, 1, :, columns], bx2.at[m, :, columns], 16 + m, rr.at[k, 5], x_dev),
        )

    home_two = (jnp.where(inner, z_devs[2][0], z_devs[1][0]), t)

    def reduce_three(m, c=None):
        k, columns = side_of(m, c)

        def home(rows_at, value, h):
            if m == 0:
                home_sum[rows_at, columns] += value
                return None
            if m == 3:

                @pl.when(inner)
                def _():
                    if not c:
                        homes[2, None][h].wait_recv()
                    joint = value + zin[2, rows_at, columns].astype(jnp.float32)
                    sz[m, rows_at, columns] = joint.astype(sz.dtype)

                @pl.when(outer)
                def _():
                    sz[m, rows_at, columns] = value.astype(sz.dtype)

            else:
                sz[m, rows_at, columns] = value.astype(sz.dtype)
            return go(
                sz.at[m, rows_at, columns], zin.at[m, rows_at, columns],
                20 + m, zbr.at[k, h], home_two if m == 2 else z_devs[m],
            )

        firsts[m, c][2].wait_recv()
        seconds[m, c][0].wait_recv()
        lower = home(
            low,
            wide_sum(rt[m, t, low, columns], bx1[m, 0, :, columns], by2[m, :, columns]),
            0,
        )
        firsts[m, c][3].wait_recv()
        seconds[m, c][1].wait_recv()
        upper = home(
            high,
            wide_sum(rt[m, t, high, columns], by1[m, 0, :, columns], bx2[m, :, columns]),
            1,
        )
        homes[m, c] = (lower, upper)

    def share_squares():
        return [
            go(squares, squares_in.at[t], 3, qr.at[k], device)
            for k, device in enumerate((x_dev, y_dev, d_dev))
        ]

    def invert(square_copies):
        for copy in square_copies:
            copy.wait_recv()
        total = (squares[...] + squares_in[tx]) + (squares_in[ty] + squares_in[td])
        inverse[z] = lax.rsqrt(total * (1.0 / model) + EPS)
        return {
            m: go(inverse.at[z], inverse.at[z], 3, qr.at[2 + m], z_devs[m])
            for m in (1, 2, 3)
        }

    passes[0, 0].wait_recv()
    passes[0, 1].wait_recv()
    sums = finish(0)
    send(0, 0)
    depart(0)
    record(0, sums)
    passes[1, 0].wait_recv()
    passes[1, 1].wait_recv()
    sums = finish(1)
    send(0, 1)
    depart(1)
    record(1, sums)
    square_copies = share_squares()
    for copy in meta_z_copies:
        copy.wait_recv()
    meta_near = go(meta_z, meta_p, 2, mr.at[6], n_dev)
    forward(0, 0)
    arrive(1, 0)
    relay(1, 0)
    relay(3, 0, False)
    forward(0, 1)
    arrive(1, 1)
    relay(1, 1)
    relay(3, 1, False)
    inverse_copies = invert(square_copies)
    arrive(2, 0)
    relay(2, 0)
    send(2, 0)
    complete(0)
    pick(0)
    arrive(2, 1)
    relay(2, 1)
    send(2, 1)
    hand_over()
    picked(0)
    for copy in loads[5:8]:
        copy.wait()
    rise(0, 0, 2)
    forward(2, 0)
    rise(0, 2, total_steps)
    forward(2, 1)

    @pl.when(outer)
    def _():
        arrive(3, 0)

    send(3, 0)
    meta_near.wait_recv()
    fall(0)

    @pl.when(outer)
    def _():
        arrive(3, 1)

    send(3, 1)
    expand(0)
    complete(2)
    inverse_copies[2].wait_recv()
    pick(2)
    picked(2)
    rise(2, 0, 2)
    forward(3, 0)
    rise(2, 2, total_steps)
    forward(3, 1)
    reduce_far(0, 0)
    reduce_far(0, 1)
    fall(2)
    complete(3)
    inverse_copies[3].wait_recv()
    pick(3)
    expand(2)
    reduce_one(2)
    picked(3)
    rise(3, 0, total_steps)
    reduce_two(2)
    reduce_side(0, 0)
    fall(3)
    complete(1)
    inverse_copies[1].wait_recv()
    pick(1)
    expand(3)
    reduce_far(3, 0)
    reduce_side(3, 0)
    reduce_far(3, 1)
    picked(1)
    rise(1, 0, 1)
    reduce_three(2)
    rise(1, 1, total_steps - 1)
    reduce_two(3, 0)
    reduce_side(3, 1)
    rise(1, total_steps - 1, total_steps)
    fall(1)
    reduce_two(3, 1)
    expand(1)
    reduce_far(1, 0)
    reduce_side(1, 0)
    reduce_far(1, 1)
    reduce_three(3, 0)
    reduce_three(3, 1)
    reduce_two(1, 0)
    reduce_side(1, 1)
    reduce_two(1, 1)
    reduce_side(0, 1)
    reduce_two(0, 0)
    reduce_two(0, 1)
    reduce_three(1, 0)
    for group in range(24):
        if group not in (16, 17, 19, 20, 21, 23):
            settle(group)
    near_copy.wait_send()
    for h in (0, 1):
        out_one[h].wait_send()

    @pl.when(inner)
    def _():
        for h in (0, 1):
            out_three[h].wait_send()
            for m in (1, 2, 3):
                relay_copy(m, h).wait_send()

    @pl.when(has_far)
    def _():
        far_copy.wait_send()

    reduce_three(1, 1)
    @pl.when(outer)
    def _():
        for copy in homes[2, None]:
            copy.wait_recv()

    for copy in homes[3, 0] + homes[3, 1]:
        copy.wait_recv()
    home_sum[...] = (
        res[...].astype(jnp.float32)
        + jnp.where(outer, zin[2].astype(jnp.float32), 0.0)
        + zin[3].astype(jnp.float32)
    )
    reduce_three(0, 0)
    reduce_three(0, 1)
    for c in (0, 1):
        for copy in homes[1, c]:
            copy.wait_recv()
    out_ref[...] = (home_sum[...] + zin[1].astype(jnp.float32)).astype(out_ref.dtype)
    for group in (16, 17, 19, 21, 23):
        settle(group)


def layer(
    queries, keys, values, sink_logit, out_weight, residual, norm_gain, routes, route_weights,
    gate_weight, up_weight, down_weight, capacity,
):
    rows, depth = queries.shape
    kind = queries.dtype
    width = out_weight.shape[1]
    tokens, model = residual.shape
    count = lax.axis_size("sp")
    slots = 4 * capacity
    anywhere = pl.BlockSpec(memory_space=pl.ANY)
    vmem = pl.BlockSpec(memory_space=pltpu.VMEM)
    dma = pltpu.SemaphoreType.DMA
    lanes = 4 * tokens
    return pl.pallas_call(
        layer_kernel,
        out_shape=pltpu.VMEM(residual.shape, kind),
        in_specs=[anywhere] * 12,
        out_specs=vmem,
        scratch_shapes=[
            pltpu.SMEM(sink_logit.shape, jnp.float32),
            pltpu.VMEM((1, model), jnp.float32),
            pltpu.VMEM((2, tokens), jnp.int32),
            pltpu.VMEM((2, tokens), jnp.float32),
            pltpu.VMEM(queries.shape, kind),
            pltpu.VMEM((2 * rows, 2 * keys.shape[1]), kind),
            pltpu.VMEM(out_weight.shape, kind),
            pltpu.VMEM(residual.shape, kind),
            pltpu.VMEM((4, tokens, width), kind),
            pltpu.VMEM((4, rows, depth), kind),
            pltpu.VMEM((2, rows // 2, width), jnp.float32),
            pltpu.VMEM((rows, width), kind),
            pltpu.VMEM(gate_weight.shape, kind),
            pltpu.VMEM(up_weight.shape, kind),
            pltpu.VMEM(down_weight.shape, kind),
            pltpu.VMEM((2 * count, lanes), jnp.float32),
            pltpu.VMEM((4, 2 * count, lanes), jnp.float32),
            pltpu.VMEM((4, 2 * count, lanes), jnp.float32),
            pltpu.VMEM((4, 2 * count, lanes), jnp.float32),
            pltpu.VMEM((2, 8, rows // 2), jnp.float32),
            pltpu.VMEM((4, 2, 8, rows // 2), jnp.float32),
            pltpu.VMEM((4, 2, 8, rows // 2), jnp.float32),
            pltpu.VMEM((4, 4, rows, width), kind),
            pltpu.VMEM((4, 2 * slots, model), kind),
            pltpu.VMEM((4, slots, model), kind),
            pltpu.VMEM((2 * slots, gate_weight.shape[1]), kind),
            pltpu.VMEM((4, 2 * slots, model), kind),
            pltpu.VMEM((4, slots, model), kind),
            pltpu.VMEM((4, 4, tokens, model), kind),
            pltpu.VMEM((4, 2, tokens // 2, model), kind),
            pltpu.VMEM((4, 2, tokens // 2, model), kind),
            pltpu.VMEM((4, tokens // 2, model), kind),
            pltpu.VMEM((4, tokens // 2, model), kind),
            pltpu.VMEM((4, 2, tokens // 2, model), kind),
            pltpu.VMEM((4, tokens, model), kind),
            pltpu.VMEM((4, tokens, model), kind),
            pltpu.VMEM(residual.shape, jnp.float32),
            dma((12,)), dma((24,)),
            dma((2,)), dma((2,)), dma((12,)), dma((3,)), dma((7,)), dma((6,)),
            dma((7, 2)), dma((4, 2)), dma((3, 5)), dma((4,)), dma((4, 2)),
            dma((7, 6)), dma((7, 2)), dma(()),
        ],
        compiler_params=pltpu.CompilerParams(
            collective_id=0, has_side_effects=True, vmem_limit_bytes=60 * 1024 * 1024
        ),
    )(
        queries, keys, values, sink_logit, out_weight, residual, norm_gain.reshape(1, -1),
        routes.T, route_weights.T,
        gate_weight, up_weight, down_weight,
    )


def with_halo(block, sides, width):
    for axis, dim in sides:
        count = lax.axis_size(axis)
        forward = [(i, i + 1) for i in range(count - 1)]
        backward = [(target, source) for source, target in forward]
        low = lax.ppermute(
            lax.slice_in_dim(block, block.shape[dim] - width, None, axis=dim), axis, forward
        )
        high = lax.ppermute(lax.slice_in_dim(block, 0, width, axis=dim), axis, backward)
        block = jnp.concatenate([low, block, high], axis=dim)
    return block


def make_band(extended, length):
    blocks = length // WINDOW
    pieces = [
        lax.slice_in_dim(extended, offset * WINDOW, offset * WINDOW + length, axis=0).reshape(
            blocks, WINDOW, -1
        )
        for offset in range(3)
    ]
    return jnp.concatenate(pieces, axis=1)


def attend_local(queries, keys, values, sink_logit):
    length = queries.shape[0]
    groups = keys.shape[1] // HEAD
    repeat = HEADS // KV_HEADS
    blocks = length // WINDOW
    joined = jnp.concatenate([keys, values], axis=1)
    extended = with_halo(joined, (("sp", 0),), WINDOW)
    banded = make_band(extended, length)
    key_band = banded[..., : groups * HEAD].reshape(blocks, 3 * WINDOW, groups, HEAD)
    value_band = banded[..., groups * HEAD :].reshape(blocks, 3 * WINDOW, groups, HEAD)
    query_blocks = queries.reshape(blocks, WINDOW, groups, repeat, HEAD)
    scores = jnp.einsum(
        "nqgrd,nkgd->ngrqk", query_blocks, key_band, preferred_element_type=jnp.float32
    ) * HEAD ** (-0.5)
    near = jnp.abs(jnp.arange(WINDOW)[:, None] + WINDOW - jnp.arange(3 * WINDOW)[None, :]) <= WINDOW
    first_token = lax.axis_index("sp") * length
    key_pos = (
        first_token + (jnp.arange(blocks)[:, None] - 1) * WINDOW + jnp.arange(3 * WINDOW)[None, :]
    )
    inside = (key_pos >= 0) & (key_pos < length * lax.axis_size("sp"))
    valid = near[None, None, None, :, :] & inside[:, None, None, None, :]
    sinks = sink_logit.reshape(1, groups, repeat, 1, 1)
    masked = jnp.where(valid, scores, NEGATIVE)
    top = jnp.maximum(jnp.max(masked, axis=-1, keepdims=True), sinks)
    probs = jnp.exp(masked - top)
    denom = jnp.sum(probs, axis=-1, keepdims=True) + jnp.exp(sinks - top)
    weights = (probs / denom).astype(jnp.bfloat16)
    output = jnp.einsum(
        "ngrqk,nkgd->nqgrd", weights, value_band, preferred_element_type=jnp.float32
    )
    return output.astype(jnp.bfloat16).reshape(length, groups * repeat * HEAD)


def local(
    queries,
    keys,
    values,
    sink_logit,
    out_weight,
    residual,
    norm_gain,
    routes,
    route_weights,
    gate_weight,
    up_weight,
    down_weight,
):
    capacity = max(2, 4 * residual.shape[0] // lax.axis_size("sp"))
    in_plane = (
        lax.axis_size("tp") == 4
        and lax.axis_size("sp") == 8
        and capacity % 32 == 0
        and gate_weight.shape[2] % 256 == 0
        and queries.shape[0] == 2 * WINDOW
        and residual.shape[0] == 64
    )
    if in_plane:
        return layer(
            queries, keys, values, sink_logit, out_weight, residual, norm_gain, routes,
            route_weights, gate_weight[0], up_weight[0], down_weight[0], capacity,
        )
    attention = attend_local(queries, keys, values, sink_logit)
    columns = jnp.dot(
        lax.all_gather(attention, "tp", axis=1, tiled=True),
        out_weight,
        preferred_element_type=jnp.float32,
    )
    projected = lax.all_to_all(
        columns.astype(jnp.bfloat16), "tp", split_axis=0, concat_axis=1, tiled=True
    )
    hidden_state = residual.astype(jnp.float32) + projected.astype(jnp.float32)
    inverse = lax.rsqrt(jnp.mean(hidden_state * hidden_state, axis=-1, keepdims=True) + EPS)
    normed = (hidden_state * inverse * norm_gain).astype(jnp.bfloat16)
    sp_count = lax.axis_size("sp")
    tok_rows = residual.shape[0]
    width = residual.shape[1]
    slot_total = sp_count * capacity
    expert_ids = routes.reshape(-1)
    onehot = (expert_ids[:, None] == jnp.arange(sp_count, dtype=jnp.int32)[None, :]).astype(
        jnp.int32
    )
    earlier = jnp.cumsum(onehot, axis=0) - onehot
    rank = jnp.sum(earlier * onehot, axis=1)
    slots = expert_ids * capacity + rank
    placing = (slots[:, None] == jnp.arange(slot_total, dtype=jnp.int32)[None, :]).astype(
        jnp.bfloat16
    )
    placing = placing.reshape(tok_rows, 2, slot_total)
    first_place = placing[:, 0]
    second_place = placing[:, 1]
    sending = jnp.einsum(
        "ts,td->sd", first_place + second_place, normed, preferred_element_type=jnp.float32
    )
    sending = sending.astype(jnp.bfloat16).reshape(sp_count, capacity, width)
    piece = lax.all_gather(
        lax.all_to_all(sending, "sp", split_axis=0, concat_axis=0, tiled=True),
        "tp",
        axis=0,
        tiled=True,
    )
    flat = piece.reshape(-1, piece.shape[-1])
    gate = jnp.dot(flat, gate_weight[0], preferred_element_type=jnp.float32)
    upward = jnp.dot(flat, up_weight[0], preferred_element_type=jnp.float32)
    hidden = (jax.nn.silu(gate) * upward).astype(jnp.bfloat16)
    partial_value = jnp.dot(hidden, down_weight[0], preferred_element_type=jnp.float32)
    partial_value = partial_value.reshape(piece.shape[:-1] + (down_weight.shape[-1],))
    returned = lax.all_to_all(
        lax.psum_scatter(
            partial_value.astype(jnp.bfloat16), "tp", scatter_dimension=0, tiled=True
        ),
        "sp",
        split_axis=0,
        concat_axis=0,
        tiled=True,
    )
    gathered_back = returned.reshape(slot_total, width)
    first_pick = jnp.dot(first_place, gathered_back, preferred_element_type=jnp.float32)
    second_pick = jnp.dot(second_place, gathered_back, preferred_element_type=jnp.float32)
    mixture = route_weights[:, 0:1] * first_pick + route_weights[:, 1:2] * second_pick
    return (hidden_state + mixture).astype(jnp.bfloat16)


def solution(mesh):
    in_specs = (
        P("sp", "tp"),
        P("sp", "tp"),
        P("sp", "tp"),
        P("tp"),
        P(None, "tp"),
        P(("sp", "tp"), None),
        P(),
        P(("sp", "tp"), None),
        P(("sp", "tp"), None),
        P("sp", None, "tp"),
        P("sp", None, "tp"),
        P("sp", "tp", None),
    )
    out_specs = P(("sp", "tp"), None)
    return jax.shard_map(local, mesh=mesh, in_specs=in_specs, out_specs=out_specs, check_vma=False)
```

```python
import math

import jax
import jax.numpy as jnp
from jax import lax
from jax.experimental import pallas as pl
from jax.experimental.pallas import tpu as pltpu
from jax.sharding import PartitionSpec as P

HEADS = 32
KV_HEADS = 16
HEAD = 64
WINDOW = 128


EPS = 1e-06
NEGATIVE = -1e30
MESH = pl.DeviceIdType.MESH


def plane():
    t = lax.axis_index("tp")
    tx = t + 1 - 2 * lax.rem(t, 2)
    ty = lax.rem(t + 2, 4)
    return t, tx, ty, 3 - t


def remote(src, dst, send, recv, device):
    return pltpu.make_async_remote_copy(
        src_ref=src,
        dst_ref=dst,
        send_sem=send,
        recv_sem=recv,
        device_id=device,
        device_id_type=MESH,
    )


def flipped(index, mask):
    result = index
    bit = 1
    while bit <= mask:
        if mask & bit:
            result = result + bit * (1 - 2 * lax.rem(index // bit, 2))
        bit *= 2
    return result


def layer_kernel(
    q_hbm, k_hbm, v_hbm, sink_hbm, w_hbm, res_hbm, gain_hbm, routes_hbm, route_weights_hbm,
    gate_hbm, up_hbm, down_hbm, out_ref,
    sink_ref, gain_ref, routes_ref, route_weights_ref, q, kv, w, res, res_in, buf, acc, proj, gate, up, down,
    meta, meta_in, meta_z, meta_p, squares, squares_in, inverse, tok, xs, xo, hidden, po, ps, rt,
    bx1, by1, bx2, by2, mid, sz, zin, home_sum,
    load, sends, hs, hr, gr, ar, mr, qr, zs, zr, dr, xs_r, ps_r, rr, zbr, hor,
):
    s = lax.axis_index("sp")
    t, tx, ty, td = plane()
    last = lax.axis_size("sp") - 1
    rows, depth = q.shape
    half = rows // 2
    groups = k_hbm.shape[1] // HEAD
    kept = groups * HEAD
    odd = lax.rem(s, 2)
    near = s + 1 - 2 * odd
    has_far = jnp.logical_and(s != 0, s != last)
    far = jnp.where(has_far, s - 1 + 2 * odd, near)
    x_dev, y_dev, d_dev, n_dev, f_dev = (s, tx), (s, ty), (s, td), (near, t), (far, t)
    z = s // 2
    planes = [flipped(z, m) for m in range(4)]
    z_devs = [(2 * planes[m] + odd, t) for m in range(4)]
    inner = jnp.logical_or(z == 1, z == 2)
    outer = jnp.logical_not(inner)
    middle = pl.ds(half, rows)
    loads = [
        pltpu.make_async_copy(source, target, load.at[k])
        for k, (source, target) in enumerate(
            (
                (k_hbm, kv.at[middle, pl.ds(0, kept)]),
                (v_hbm, kv.at[middle, pl.ds(kept, kept)]),
                (q_hbm, q),
                (w_hbm, w),
                (res_hbm, res),
                (gate_hbm, gate),
                (up_hbm, up),
                (down_hbm, down),
                (sink_hbm, sink_ref),
                (routes_hbm, routes_ref),
                (route_weights_hbm, route_weights_ref),
                (gain_hbm, gain_ref),
            )
        )
    ]
    barrier = pltpu.get_barrier_semaphore()
    for device in [x_dev, y_dev, d_dev, n_dev] + z_devs[1:]:
        pl.semaphore_signal(barrier, inc=1, device_id=device, device_id_type=MESH)

    @pl.when(has_far)
    def _():
        pl.semaphore_signal(barrier, inc=1, device_id=f_dev, device_id_type=MESH)

    for copy in loads[:5] + loads[8:]:
        copy.start()

    @pl.when(has_far)
    def _():
        pl.semaphore_wait(barrier, 8)

    @pl.when(jnp.logical_not(has_far))
    def _():
        pl.semaphore_wait(barrier, 7)

    def aligned(value, size):
        return pl.ds(pl.multiple_of(value, size), size)

    near_src = aligned(2 * half - half * odd, half)
    near_dst = aligned(3 * half * odd, half)
    far_src = aligned(half + half * odd, half)
    far_dst = aligned(3 * half * (1 - odd), half)
    near_copy = remote(kv.at[near_src], kv.at[near_dst], hs.at[0], hr.at[0], n_dev)
    far_copy = remote(kv.at[far_src], kv.at[far_dst], hs.at[1], hr.at[1], f_dev)
    loads[0].wait()
    loads[1].wait()

    @pl.when(has_far)
    def _():
        far_copy.start()

    near_copy.start()
    amounts = [0] * sends.shape[0]

    def go(source, target, group, recv, device):
        copy = remote(source, target, sends.at[group], recv, device)
        copy.start()
        amounts[group] += math.prod(source.shape) * source.dtype.itemsize
        return copy

    def settle(group):
        line = tok.shape[3] * tok.dtype.itemsize
        lines = amounts[group] // line
        if lines <= tok.shape[2]:
            whole = tok.at[0, 0, pl.ds(0, lines)]
        else:
            whole = tok.at[0, pl.ds(0, lines // tok.shape[2])]
        remote(whole, whole, sends.at[group], hr.at[0], x_dev).wait_send()

    own, model = res.shape
    width = w.shape[1]
    loads[4].wait()
    res_copies = [
        go(
            res.at[:, aligned(owner * width, width)],
            res_in.at[t],
            1,
            ar.at[k],
            device,
        )
        for k, (owner, device) in enumerate(((tx, x_dev), (ty, y_dev), (td, d_dev)))
    ]
    res_in[t] = res[:, aligned(t * width, width)]
    count, lanes = meta.shape[0] // 2, meta.shape[1]
    tokens = lanes // 4
    expert = lax.broadcasted_iota(jnp.int32, (count, lanes), 0)
    lane = lax.broadcasted_iota(jnp.int32, (count, lanes), 1)
    mine_lane = jnp.logical_and(lane >= t * tokens, lane < (t + 1) * tokens)
    for copy in loads[8:]:
        copy.wait()
    routes = jnp.concatenate([routes_ref[...]] * 4, axis=1)
    route_weights = jnp.concatenate([route_weights_ref[...]] * 4, axis=1)
    hit_one = routes[0:1, :] == expert
    hit = jnp.logical_and(mine_lane, jnp.logical_or(hit_one, routes[1:2, :] == expert))
    chosen = jnp.where(hit, 1.0, 0.0)
    before = lax.broadcasted_iota(jnp.int32, (lanes, lanes), 0) <= lax.broadcasted_iota(
        jnp.int32, (lanes, lanes), 1
    )
    rank = jnp.dot(
        chosen.astype(jnp.bfloat16),
        jnp.where(before, 1.0, 0.0).astype(jnp.bfloat16),
        preferred_element_type=jnp.float32,
    )
    meta[0:count] = chosen * rank
    meta[count : 2 * count] = chosen * jnp.where(
        hit_one, route_weights[0:1, :], route_weights[1:2, :]
    )
    meta_copies = [
        go(meta, meta_in.at[t], 2, mr.at[k], device)
        for k, device in enumerate((x_dev, y_dev, d_dev))
    ]

    for copy in loads[5:8]:
        copy.start()

    @pl.when(jnp.logical_not(has_far))
    def _():
        kv[aligned(3 * half * odd, half)] = jnp.zeros((half, kv.shape[1]), kv.dtype)

    loads[2].wait()
    span = 3 * half
    query = lax.broadcasted_iota(jnp.int32, (2 * half, span), 0)
    query = jnp.where(query >= half, query - half, query)
    key = lax.broadcasted_iota(jnp.int32, (2 * half, span), 1)
    band = jnp.abs(query + half - key) <= WINDOW
    upper = lax.broadcasted_iota(jnp.int32, (2 * half, 1), 0) < half

    def attend(b, first, end):
        valid = jnp.logical_and(
            band,
            jnp.logical_and(
                key >= jnp.where(2 * s + b == 0, half, 0),
                key < jnp.where(2 * s + b == 2 * last + 1, 2 * half, span),
            ),
        )
        keys_at = pl.ds(pl.multiple_of(b * half, half), span)
        mine = aligned(b * half, half)
        for g in range(first, end):
            pair = q[mine, 2 * g * HEAD : 2 * (g + 1) * HEAD]
            stacked = jnp.concatenate([pair[:, :HEAD], pair[:, HEAD:]], axis=0)
            scores = lax.dot_general(
                stacked,
                kv[keys_at, g * HEAD : (g + 1) * HEAD],
                (((1,), (1,)), ((), ())),
                preferred_element_type=jnp.float32,
            ) * HEAD ** (-0.5)
            sink = jnp.where(upper, sink_ref[2 * g], sink_ref[2 * g + 1])
            masked = jnp.where(valid, scores, NEGATIVE)
            top = jnp.maximum(jnp.max(masked, axis=-1, keepdims=True), sink)
            probs = jnp.exp(masked - top)
            denom = jnp.sum(probs, axis=-1, keepdims=True) + jnp.exp(sink - top)
            weights = (probs * (1.0 / denom)).astype(jnp.bfloat16)
            output = jnp.dot(
                weights,
                kv[keys_at, kept + g * HEAD : kept + (g + 1) * HEAD],
                preferred_element_type=jnp.float32,
            )
            joined = jnp.concatenate([output[:half], output[half:]], axis=1)
            buf[t, mine, 2 * g * HEAD : 2 * (g + 1) * HEAD] = joined.astype(buf.dtype)

    blocks = (1 - odd, odd)
    parts_of = [aligned(b * half, half) for b in blocks]

    wide_piece = depth // 2

    def part(owner, h, j):
        return buf.at[owner, parts_of[h], pl.ds(j * wide_piece, wide_piece)]

    spreads, passes = {}, {}

    def spread(h, j):
        piece = part(t, h, j)
        k = 4 * h + 2 * j
        spreads[h, j] = (
            go(piece, piece, 0, gr.at[k], x_dev),
            go(piece, piece, 0, gr.at[k + 1], y_dev),
        )

    def hand_on(h, j):
        spreads[h, j][j].wait_recv()
        piece = part(ty if j else tx, h, j)
        k = 8 + 2 * h + j
        passes[h, j] = go(piece, piece, 0, gr.at[k], x_dev if j else y_dev)

    near_copy.wait_recv()
    attend(blocks[0], 0, groups // 2)
    spread(0, 0)
    attend(blocks[0], groups // 2, groups)
    spread(0, 1)

    @pl.when(has_far)
    def _():
        far_copy.wait_recv()

    attend(blocks[1], 0, groups // 2)
    spread(1, 0)
    attend(blocks[1], groups // 2, groups)
    spread(1, 1)
    for copy in meta_copies:
        copy.wait_recv()
    meta_z[z] = (meta[...] + meta_in[tx]) + (meta_in[ty] + meta_in[td])
    meta_z_copies = [
        go(meta_z.at[z], meta_z.at[z], 2, mr.at[2 + m], z_devs[m]) for m in (1, 2, 3)
    ]
    loads[3].wait()

    def product(h, owner):
        weight = w[pl.ds(pl.multiple_of(owner * depth, depth), depth)]
        return jnp.dot(buf[owner, parts_of[h]], weight, preferred_element_type=jnp.float32)

    def gather(h):
        hand_on(h, 0)
        acc[h] = product(h, t)
        hand_on(h, 1)
        spreads[h, 1][0].wait_recv()
        acc[h] += product(h, tx)
        spreads[h, 0][1].wait_recv()
        acc[h] += product(h, ty)

    gather(0)
    for copy in res_copies:
        copy.wait_recv()
    gather(1)
    gain = gain_ref[:, aligned(t * width, width)]

    def finish(h):
        projected = (acc[h] + product(h, td)).astype(proj.dtype)
        proj[parts_of[h]] = projected
        pair = res_in[pl.ds(2 * blocks[h], 2)].reshape(half, width)
        value = pair.astype(jnp.float32) + projected.astype(jnp.float32)
        tok[t, z, parts_of[h]] = (value * gain).astype(tok.dtype)
        return jnp.sum(value * value, axis=-1, keepdims=True)

    def record(h, sums):
        squares[blocks[h]] = jnp.broadcast_to(sums, (half, half)).T[: squares.shape[1]]

    def own_block(h):
        return tok.at[t, z, parts_of[h]]

    z_in = {
        (m, h): remote(
            own_block(h), tok.at[t, planes[m], parts_of[h]], zs.at[m, h], zr.at[m, h], z_devs[m]
        )
        for m in (1, 2, 3)
        for h in (0, 1)
    }

    out_one = [remote(own_block(h), own_block(h), zs.at[1, h], zr.at[1, h], z_devs[1]) for h in (0, 1)]
    out_three = [remote(own_block(h), own_block(h), zs.at[3, h], zr.at[3, h], z_devs[3]) for h in (0, 1)]

    def relay_copy(m, h):
        piece = tok.at[t, planes[m], parts_of[h]]
        lands, device = ((2, z_devs[3]), None, (3, z_devs[1]), (2, z_devs[1]))[
            {1: 0, 2: 2, 3: 3}[m]
        ]
        return remote(piece, piece, zs.at[3 + m, h], zr.at[lands, h], device)

    def depart(h):
        out_one[h].start()

        @pl.when(inner)
        def _():
            out_three[h].start()

    sent, parts, firsts, seconds, homes = {}, {}, {}, {}, {}

    def arrive(m, h):
        z_in[m, h].wait_recv()

    def relay(m, h, waited=True):
        @pl.when(inner)
        def _():
            if not waited:
                arrive(m, h)
            relay_copy(m, h).start()

    def send(m, h):
        piece = tok.at[t, planes[m], parts_of[h]]
        k = max(m - 1, 0)
        sent[m, h] = (
            go(piece, piece, 5 + k, dr.at[k, 2 * h], x_dev),
            go(piece, piece, 5 + k, dr.at[k, 2 * h + 1], y_dev),
        )

    def forward(m, h):
        k = max(m - 1, 0)
        sent[m, h][0].wait_recv()
        piece = tok.at[tx, planes[m], aligned(blocks[h] * half, half // 2)]
        go(piece, piece, 5 + k, dr.at[k, 4], y_dev)
        sent[m, h][1].wait_recv()
        piece = tok.at[ty, planes[m], aligned(blocks[h] * half + half // 2, half // 2)]
        go(piece, piece, 5 + k, dr.at[k, 4], x_dev)

    slots = xo.shape[1]
    capacity = slots // 4
    step = 256
    row = lax.broadcasted_iota(jnp.int32, (slots, lanes), 0).astype(jnp.float32)
    shift = (lax.broadcasted_iota(jnp.int32, (1, lanes), 1) // tokens * capacity).astype(
        jnp.float32
    )

    def place(source, m, which):
        ranks = source[planes[m], pl.ds(which, 1), :]
        target = jnp.where(ranks > 0.5, ranks + (shift - 1.0), -1.0)
        return row == target

    def scale(source, m, which):
        weights = source[planes[m], pl.ds(count + which, 1), :]
        return jnp.sum(
            jnp.where(place(source, m, which), weights, 0.0), axis=1, keepdims=True
        )

    def picking(m):
        return jnp.concatenate(
            [jnp.where(place(meta_z, m, which), 1.0, 0.0) for which in (s, near)], axis=0
        )

    def hand_over():
        for k, owner in enumerate((tx, ty, td)):
            piece = tok.at[owner, z]
            go(piece, piece, 4, hor, z_devs[1])

    def complete(m):
        if m == 1:
            whole, recv = tok.at[0, pl.ds(0, 3)], hor
        else:
            whole, recv = tok.at[0, 0], dr.at[max(m - 1, 0), 4]
        remote(whole, whole, sends.at[4], recv, x_dev).wait_recv()

    def pick(m):
        chooser = picking(m)
        lengths = inverse[planes[m]]
        lengths = jnp.concatenate([lengths[0, 0:1], lengths[1, 0:1]], axis=1)
        factor = jnp.sum(chooser * lengths, axis=1, keepdims=True)
        chooser = chooser.astype(jnp.bfloat16)
        for owner in range(4):
            for k in range(width // step):
                rows_in = tok[owner, planes[m], :, k * step : (k + 1) * step]
                found = jnp.dot(chooser, rows_in, preferred_element_type=jnp.float32)
                found = (found * factor).astype(xs.dtype)
                columns = slice(owner * width + k * step, owner * width + (k + 1) * step)
                xs[m, 0:slots, columns] = found[:slots]
                xo[m, :, columns] = found[slots:]
            if owner % 2:
                columns = pl.ds((owner - 1) * width, 2 * width)
                go(
                    xo.at[m, :, columns],
                    xs.at[m, pl.ds(slots, slots), columns],
                    8 + m,
                    xs_r.at[m],
                    n_dev,
                )

    def picked(m):
        whole = xo.at[m]
        remote(whole, whole, sends.at[8 + m], xs_r.at[m], n_dev).wait_recv()

    def rise(m, begin, end):
        @pl.loop(begin, end)
        def _(k):
            columns = pl.ds(pl.multiple_of(k * step, step), step)
            x = xs[m]
            g = jnp.dot(x, gate[:, columns], preferred_element_type=jnp.float32)
            u = jnp.dot(x, up[:, columns], preferred_element_type=jnp.float32)
            hidden[:, columns] = (jax.nn.silu(g) * u).astype(hidden.dtype)

    total_steps = gate.shape[1] // step

    def fall(m):
        factor_mine = scale(meta_z, m, s)
        factor_near = scale(meta_p, m, s)
        wide = 512

        for side in (0, 1):

            @pl.loop(side * model // (2 * wide), (side + 1) * model // (2 * wide))
            def _(k):
                columns = pl.ds(pl.multiple_of(k * wide, wide), wide)
                share = jnp.dot(hidden[...], down[:, columns], preferred_element_type=jnp.float32)
                po[m, 0:slots, columns] = (share[:slots] * factor_mine).astype(po.dtype)
                ps[m, :, columns] = (share[slots:] * factor_near).astype(ps.dtype)

            columns = pl.ds(side * (model // 2), model // 2)
            parts[m, side] = go(
                ps.at[m, :, columns],
                po.at[m, pl.ds(slots, slots), columns],
                12 + m,
                ps_r.at[m, side],
                n_dev,
            )

    def expand(m):
        spreader = picking(m).T.astype(jnp.bfloat16)
        for owner in range(4):
            if owner % 2 == 0:
                parts[m, owner // 2].wait_recv()
            holds = jnp.where(t == owner, 1.0, 0.0)
            for k in range(width // step):
                columns = slice(owner * width + k * step, owner * width + (k + 1) * step)
                found = jnp.dot(spreader, po[m, :, columns], preferred_element_type=jnp.float32)
                if m == 0:
                    found += holds * proj[:, k * step : (k + 1) * step].astype(jnp.float32)
                rt[m, :, :, columns] = found.astype(rt.dtype).reshape(4, tokens, step)

    low, high = pl.ds(0, own // 2), pl.ds(own // 2, own // 2)

    def side_of(m, c):
        if c is None:
            return m, pl.ds(0, model)
        return m if c == 0 else {1: 4, 0: 5, 3: 6}[m], pl.ds(c * (model // 2), model // 2)

    def reduce_far(m, c=None):
        k, columns = side_of(m, c)
        firsts[m, c] = (
            go(
                rt.at[m, td, low, columns], bx1.at[m, 1, :, columns],
                16 + m, rr.at[k, 0], x_dev,
            ),
            go(
                rt.at[m, td, high, columns], by1.at[m, 1, :, columns],
                16 + m, rr.at[k, 1], y_dev,
            ),
        )

    def reduce_side(m, c=None):
        k, columns = side_of(m, c)
        firsts[m, c] += (
            go(
                rt.at[m, tx, low, columns], bx1.at[m, 0, :, columns],
                16 + m, rr.at[k, 2], x_dev,
            ),
            go(
                rt.at[m, ty, high, columns], by1.at[m, 0, :, columns],
                16 + m, rr.at[k, 3], y_dev,
            ),
        )

    def reduce_one(m):
        reduce_far(m)
        reduce_side(m)

    def wide_sum(*pieces):
        result = pieces[0].astype(jnp.float32)
        for piece in pieces[1:]:
            result = result + piece.astype(jnp.float32)
        return result

    def reduce_two(m, c=None):
        k, columns = side_of(m, c)
        firsts[m, c][0].wait_recv()
        mid[m, 0, :, columns] = wide_sum(
            rt[m, ty, low, columns], bx1[m, 1, :, columns]
        ).astype(mid.dtype)
        to_side = go(
            mid.at[m, 0, :, columns], by2.at[m, :, columns], 16 + m, rr.at[k, 2], y_dev
        )
        firsts[m, c][1].wait_recv()
        mid[m, 1, :, columns] = wide_sum(
            rt[m, tx, high, columns], by1[m, 1, :, columns]
        ).astype(mid.dtype)
        seconds[m, c] = (
            to_side,
            go(mid.at[m, 1, :, columns], bx2.at[m, :, columns], 16 + m, rr.at[k, 3], x_dev),
        )

    home_two = (jnp.where(inner, z_devs[2][0], z_devs[1][0]), t)

    def reduce_three(m, c=None):
        k, columns = side_of(m, c)

        def home(rows_at, value, h):
            if m == 0:
                home_sum[rows_at, columns] += value
                return None
            if m == 3:

                @pl.when(inner)
                def _():
                    if not c:
                        homes[2, None][h].wait_recv()
                    joint = value + zin[2, rows_at, columns].astype(jnp.float32)
                    sz[m, rows_at, columns] = joint.astype(sz.dtype)

                @pl.when(outer)
                def _():
                    sz[m, rows_at, columns] = value.astype(sz.dtype)

            else:
                sz[m, rows_at, columns] = value.astype(sz.dtype)
            return go(
                sz.at[m, rows_at, columns], zin.at[m, rows_at, columns],
                20 + m, zbr.at[k, h], home_two if m == 2 else z_devs[m],
            )

        whole = rt.at[m, t, :, columns]
        remote(whole, whole, sends.at[16 + m], rr.at[k, 2], x_dev).wait_recv()
        lower = home(
            low,
            wide_sum(rt[m, t, low, columns], bx1[m, 0, :, columns], by2[m, :, columns]),
            0,
        )
        remote(whole, whole, sends.at[16 + m], rr.at[k, 3], x_dev).wait_recv()
        upper = home(
            high,
            wide_sum(rt[m, t, high, columns], by1[m, 0, :, columns], bx2[m, :, columns]),
            1,
        )
        homes[m, c] = (lower, upper)

    def share_squares():
        return [
            go(squares, squares_in.at[t], 3, qr.at[k], device)
            for k, device in enumerate((x_dev, y_dev, d_dev))
        ]

    def invert(square_copies):
        for copy in square_copies:
            copy.wait_recv()
        total = (squares[...] + squares_in[tx]) + (squares_in[ty] + squares_in[td])
        inverse[z] = lax.rsqrt(total * (1.0 / model) + EPS)
        return {
            m: go(inverse.at[z], inverse.at[z], 3, qr.at[2 + m], z_devs[m])
            for m in (1, 2, 3)
        }

    passes[0, 0].wait_recv()
    passes[0, 1].wait_recv()
    sums = finish(0)
    send(0, 0)
    depart(0)
    record(0, sums)
    passes[1, 0].wait_recv()
    passes[1, 1].wait_recv()
    sums = finish(1)
    send(0, 1)
    depart(1)
    record(1, sums)
    square_copies = share_squares()
    for copy in meta_z_copies:
        copy.wait_recv()
    meta_near = go(meta_z, meta_p, 2, mr.at[6], n_dev)
    forward(0, 0)
    arrive(1, 0)
    relay(1, 0)
    relay(3, 0, False)
    forward(0, 1)
    arrive(1, 1)
    relay(1, 1)
    relay(3, 1, False)
    inverse_copies = invert(square_copies)
    arrive(2, 0)
    relay(2, 0)
    send(2, 0)
    complete(0)
    pick(0)
    arrive(2, 1)
    relay(2, 1)
    send(2, 1)
    hand_over()
    picked(0)
    for copy in loads[5:8]:
        copy.wait()
    rise(0, 0, 2)
    forward(2, 0)
    rise(0, 2, total_steps)
    forward(2, 1)

    @pl.when(outer)
    def _():
        arrive(3, 0)

    send(3, 0)
    meta_near.wait_recv()
    fall(0)

    @pl.when(outer)
    def _():
        arrive(3, 1)

    send(3, 1)
    expand(0)
    complete(2)
    inverse_copies[2].wait_recv()
    pick(2)
    picked(2)
    rise(2, 0, 2)
    forward(3, 0)
    rise(2, 2, total_steps - 1)
    forward(3, 1)
    reduce_far(0, 0)
    reduce_far(0, 1)
    rise(2, total_steps - 1, total_steps)
    fall(2)
    complete(3)
    inverse_copies[3].wait_recv()
    pick(3)
    expand(2)
    reduce_one(2)
    picked(3)
    rise(3, 0, total_steps)
    reduce_two(2)
    reduce_side(0, 0)
    fall(3)
    complete(1)
    inverse_copies[1].wait_recv()
    pick(1)
    expand(3)
    reduce_far(3, 0)
    reduce_side(3, 0)
    reduce_far(3, 1)
    picked(1)
    rise(1, 0, 1)
    reduce_three(2)
    rise(1, 1, total_steps - 1)
    reduce_two(3, 0)
    reduce_side(3, 1)
    rise(1, total_steps - 1, total_steps)
    fall(1)
    reduce_two(3, 1)
    expand(1)
    reduce_far(1, 0)
    reduce_side(1, 0)
    reduce_far(1, 1)
    reduce_three(3, 0)
    reduce_three(3, 1)
    reduce_two(1, 0)
    reduce_side(1, 1)
    reduce_two(1, 1)
    reduce_side(0, 1)
    reduce_two(0, 0)
    reduce_two(0, 1)
    reduce_three(1, 0)
    for group in range(24):
        if group not in (16, 17, 19, 20, 21, 23):
            settle(group)
    near_copy.wait_send()
    for h in (0, 1):
        out_one[h].wait_send()

    @pl.when(inner)
    def _():
        for h in (0, 1):
            out_three[h].wait_send()
            for m in (1, 2, 3):
                relay_copy(m, h).wait_send()

    @pl.when(has_far)
    def _():
        far_copy.wait_send()

    reduce_three(1, 1)
    @pl.when(outer)
    def _():
        for copy in homes[2, None]:
            copy.wait_recv()

    for copy in homes[3, 0] + homes[3, 1]:
        copy.wait_recv()
    home_sum[...] = (
        res[...].astype(jnp.float32)
        + jnp.where(outer, zin[2].astype(jnp.float32), 0.0)
        + zin[3].astype(jnp.float32)
    )
    reduce_three(0, 0)
    reduce_three(0, 1)
    for c in (0, 1):
        for copy in homes[1, c]:
            copy.wait_recv()
    out_ref[...] = (home_sum[...] + zin[1].astype(jnp.float32)).astype(out_ref.dtype)
    for group in (16, 17, 19, 21, 23):
        settle(group)


def layer(
    queries, keys, values, sink_logit, out_weight, residual, norm_gain, routes, route_weights,
    gate_weight, up_weight, down_weight, capacity,
):
    rows, depth = queries.shape
    kind = queries.dtype
    width = out_weight.shape[1]
    tokens, model = residual.shape
    count = lax.axis_size("sp")
    slots = 4 * capacity
    anywhere = pl.BlockSpec(memory_space=pl.ANY)
    vmem = pl.BlockSpec(memory_space=pltpu.VMEM)
    dma = pltpu.SemaphoreType.DMA
    lanes = 4 * tokens
    return pl.pallas_call(
        layer_kernel,
        out_shape=pltpu.VMEM(residual.shape, kind),
        in_specs=[anywhere] * 12,
        out_specs=vmem,
        scratch_shapes=[
            pltpu.SMEM(sink_logit.shape, jnp.float32),
            pltpu.VMEM((1, model), jnp.float32),
            pltpu.VMEM((2, tokens), jnp.int32),
            pltpu.VMEM((2, tokens), jnp.float32),
            pltpu.VMEM(queries.shape, kind),
            pltpu.VMEM((2 * rows, 2 * keys.shape[1]), kind),
            pltpu.VMEM(out_weight.shape, kind),
            pltpu.VMEM(residual.shape, kind),
            pltpu.VMEM((4, tokens, width), kind),
            pltpu.VMEM((4, rows, depth), kind),
            pltpu.VMEM((2, rows // 2, width), jnp.float32),
            pltpu.VMEM((rows, width), kind),
            pltpu.VMEM(gate_weight.shape, kind),
            pltpu.VMEM(up_weight.shape, kind),
            pltpu.VMEM(down_weight.shape, kind),
            pltpu.VMEM((2 * count, lanes), jnp.float32),
            pltpu.VMEM((4, 2 * count, lanes), jnp.float32),
            pltpu.VMEM((4, 2 * count, lanes), jnp.float32),
            pltpu.VMEM((4, 2 * count, lanes), jnp.float32),
            pltpu.VMEM((2, 8, rows // 2), jnp.float32),
            pltpu.VMEM((4, 2, 8, rows // 2), jnp.float32),
            pltpu.VMEM((4, 2, 8, rows // 2), jnp.float32),
            pltpu.VMEM((4, 4, rows, width), kind),
            pltpu.VMEM((4, 2 * slots, model), kind),
            pltpu.VMEM((4, slots, model), kind),
            pltpu.VMEM((2 * slots, gate_weight.shape[1]), kind),
            pltpu.VMEM((4, 2 * slots, model), kind),
            pltpu.VMEM((4, slots, model), kind),
            pltpu.VMEM((4, 4, tokens, model), kind),
            pltpu.VMEM((4, 2, tokens // 2, model), kind),
            pltpu.VMEM((4, 2, tokens // 2, model), kind),
            pltpu.VMEM((4, tokens // 2, model), kind),
            pltpu.VMEM((4, tokens // 2, model), kind),
            pltpu.VMEM((4, 2, tokens // 2, model), kind),
            pltpu.VMEM((4, tokens, model), kind),
            pltpu.VMEM((4, tokens, model), kind),
            pltpu.VMEM(residual.shape, jnp.float32),
            dma((12,)), dma((24,)),
            dma((2,)), dma((2,)), dma((12,)), dma((3,)), dma((7,)), dma((6,)),
            dma((7, 2)), dma((4, 2)), dma((3, 5)), dma((4,)), dma((4, 2)),
            dma((7, 4)), dma((7, 2)), dma(()),
        ],
        compiler_params=pltpu.CompilerParams(
            collective_id=0, has_side_effects=True, vmem_limit_bytes=60 * 1024 * 1024
        ),
    )(
        queries, keys, values, sink_logit, out_weight, residual, norm_gain.reshape(1, -1),
        routes.T, route_weights.T,
        gate_weight, up_weight, down_weight,
    )


def with_halo(block, sides, width):
    for axis, dim in sides:
        count = lax.axis_size(axis)
        forward = [(i, i + 1) for i in range(count - 1)]
        backward = [(target, source) for source, target in forward]
        low = lax.ppermute(
            lax.slice_in_dim(block, block.shape[dim] - width, None, axis=dim), axis, forward
        )
        high = lax.ppermute(lax.slice_in_dim(block, 0, width, axis=dim), axis, backward)
        block = jnp.concatenate([low, block, high], axis=dim)
    return block


def make_band(extended, length):
    blocks = length // WINDOW
    pieces = [
        lax.slice_in_dim(extended, offset * WINDOW, offset * WINDOW + length, axis=0).reshape(
            blocks, WINDOW, -1
        )
        for offset in range(3)
    ]
    return jnp.concatenate(pieces, axis=1)


def attend_local(queries, keys, values, sink_logit):
    length = queries.shape[0]
    groups = keys.shape[1] // HEAD
    repeat = HEADS // KV_HEADS
    blocks = length // WINDOW
    joined = jnp.concatenate([keys, values], axis=1)
    extended = with_halo(joined, (("sp", 0),), WINDOW)
    banded = make_band(extended, length)
    key_band = banded[..., : groups * HEAD].reshape(blocks, 3 * WINDOW, groups, HEAD)
    value_band = banded[..., groups * HEAD :].reshape(blocks, 3 * WINDOW, groups, HEAD)
    query_blocks = queries.reshape(blocks, WINDOW, groups, repeat, HEAD)
    scores = jnp.einsum(
        "nqgrd,nkgd->ngrqk", query_blocks, key_band, preferred_element_type=jnp.float32
    ) * HEAD ** (-0.5)
    near = jnp.abs(jnp.arange(WINDOW)[:, None] + WINDOW - jnp.arange(3 * WINDOW)[None, :]) <= WINDOW
    first_token = lax.axis_index("sp") * length
    key_pos = (
        first_token + (jnp.arange(blocks)[:, None] - 1) * WINDOW + jnp.arange(3 * WINDOW)[None, :]
    )
    inside = (key_pos >= 0) & (key_pos < length * lax.axis_size("sp"))
    valid = near[None, None, None, :, :] & inside[:, None, None, None, :]
    sinks = sink_logit.reshape(1, groups, repeat, 1, 1)
    masked = jnp.where(valid, scores, NEGATIVE)
    top = jnp.maximum(jnp.max(masked, axis=-1, keepdims=True), sinks)
    probs = jnp.exp(masked - top)
    denom = jnp.sum(probs, axis=-1, keepdims=True) + jnp.exp(sinks - top)
    weights = (probs / denom).astype(jnp.bfloat16)
    output = jnp.einsum(
        "ngrqk,nkgd->nqgrd", weights, value_band, preferred_element_type=jnp.float32
    )
    return output.astype(jnp.bfloat16).reshape(length, groups * repeat * HEAD)


def local(
    queries,
    keys,
    values,
    sink_logit,
    out_weight,
    residual,
    norm_gain,
    routes,
    route_weights,
    gate_weight,
    up_weight,
    down_weight,
):
    capacity = max(2, 4 * residual.shape[0] // lax.axis_size("sp"))
    in_plane = (
        lax.axis_size("tp") == 4
        and lax.axis_size("sp") == 8
        and capacity % 32 == 0
        and gate_weight.shape[2] % 256 == 0
        and queries.shape[0] == 2 * WINDOW
        and residual.shape[0] == 64
    )
    if in_plane:
        return layer(
            queries, keys, values, sink_logit, out_weight, residual, norm_gain, routes,
            route_weights, gate_weight[0], up_weight[0], down_weight[0], capacity,
        )
    attention = attend_local(queries, keys, values, sink_logit)
    columns = jnp.dot(
        lax.all_gather(attention, "tp", axis=1, tiled=True),
        out_weight,
        preferred_element_type=jnp.float32,
    )
    projected = lax.all_to_all(
        columns.astype(jnp.bfloat16), "tp", split_axis=0, concat_axis=1, tiled=True
    )
    hidden_state = residual.astype(jnp.float32) + projected.astype(jnp.float32)
    inverse = lax.rsqrt(jnp.mean(hidden_state * hidden_state, axis=-1, keepdims=True) + EPS)
    normed = (hidden_state * inverse * norm_gain).astype(jnp.bfloat16)
    sp_count = lax.axis_size("sp")
    tok_rows = residual.shape[0]
    width = residual.shape[1]
    slot_total = sp_count * capacity
    expert_ids = routes.reshape(-1)
    onehot = (expert_ids[:, None] == jnp.arange(sp_count, dtype=jnp.int32)[None, :]).astype(
        jnp.int32
    )
    earlier = jnp.cumsum(onehot, axis=0) - onehot
    rank = jnp.sum(earlier * onehot, axis=1)
    slots = expert_ids * capacity + rank
    placing = (slots[:, None] == jnp.arange(slot_total, dtype=jnp.int32)[None, :]).astype(
        jnp.bfloat16
    )
    placing = placing.reshape(tok_rows, 2, slot_total)
    first_place = placing[:, 0]
    second_place = placing[:, 1]
    sending = jnp.einsum(
        "ts,td->sd", first_place + second_place, normed, preferred_element_type=jnp.float32
    )
    sending = sending.astype(jnp.bfloat16).reshape(sp_count, capacity, width)
    piece = lax.all_gather(
        lax.all_to_all(sending, "sp", split_axis=0, concat_axis=0, tiled=True),
        "tp",
        axis=0,
        tiled=True,
    )
    flat = piece.reshape(-1, piece.shape[-1])
    gate = jnp.dot(flat, gate_weight[0], preferred_element_type=jnp.float32)
    upward = jnp.dot(flat, up_weight[0], preferred_element_type=jnp.float32)
    hidden = (jax.nn.silu(gate) * upward).astype(jnp.bfloat16)
    partial_value = jnp.dot(hidden, down_weight[0], preferred_element_type=jnp.float32)
    partial_value = partial_value.reshape(piece.shape[:-1] + (down_weight.shape[-1],))
    returned = lax.all_to_all(
        lax.psum_scatter(
            partial_value.astype(jnp.bfloat16), "tp", scatter_dimension=0, tiled=True
        ),
        "sp",
        split_axis=0,
        concat_axis=0,
        tiled=True,
    )
    gathered_back = returned.reshape(slot_total, width)
    first_pick = jnp.dot(first_place, gathered_back, preferred_element_type=jnp.float32)
    second_pick = jnp.dot(second_place, gathered_back, preferred_element_type=jnp.float32)
    mixture = route_weights[:, 0:1] * first_pick + route_weights[:, 1:2] * second_pick
    return (hidden_state + mixture).astype(jnp.bfloat16)


def solution(mesh):
    in_specs = (
        P("sp", "tp"),
        P("sp", "tp"),
        P("sp", "tp"),
        P("tp"),
        P(None, "tp"),
        P(("sp", "tp"), None),
        P(),
        P(("sp", "tp"), None),
        P(("sp", "tp"), None),
        P("sp", None, "tp"),
        P("sp", None, "tp"),
        P("sp", "tp", None),
    )
    out_specs = P(("sp", "tp"), None)
    return jax.shard_map(local, mesh=mesh, in_specs=in_specs, out_specs=out_specs, check_vma=False)
```
